256 devices in a mesh: grp: 4 (over y, x), ep: 64 (over z, core).
Axes of the slice: x: 2, y: 2, z: 32, core: 2. Of those that a mesh axis runs over, the one named last changes fastest.
The devices are a block of a 4x8x32 slice.
Arguments:
- tokens: bfloat16 [1024, 2048], P(('grp', 'ep')), parts along dimension 0, may hold values from -6 to 6
- prior_state: float32 [1024, 32, 64, 64], P(('grp', 'ep')), parts along dimension 0, may hold values from -3 to 3
- receptance_matrix: bfloat16 [2048, 2048], P('ep'), may hold values from -0.125 to 0.125
- key_matrix: bfloat16 [2048, 2048], P('ep'), may hold values from -0.125 to 0.125
- value_matrix: bfloat16 [2048, 2048], P('ep'), may hold values from -0.125 to 0.125
- decay_lowrank_first: bfloat16 [2048, 64], replicated, may hold values from -0.125 to 0.125
- decay_lowrank_second: bfloat16 [64, 2048], replicated, may hold values from -1.5 to 1.5
- decay_channel_offset: float32 [2048], replicated, may hold values from -6 to 0
- correction_lowrank_first: bfloat16 [2048, 64], replicated, may hold values from -0.125 to 0.125
- correction_lowrank_second: bfloat16 [64, 2048], replicated, may hold values from -1.5 to 1.5
- correction_offset: float32 [2048], replicated, may hold values from -4 to 4
- gate_lowrank_first: bfloat16 [2048, 128], replicated, may hold values from -0.25 to 0.25
- gate_lowrank_second: bfloat16 [128, 2048], replicated, may hold values from -0.5 to 0.5
- key_rate_blend: float32 [2048], replicated, may hold values from 0.1 to 1.9
- self_token_scale: float32 [32, 64], replicated, may hold values from -1.2 to 1.2
- per_head_gain: float32 [2048], replicated, may hold values from 0.1 to 1.9
- per_head_bias: float32 [2048], replicated, may hold values from -1.8 to 1.8
- mixer_output_weight: bfloat16 [2048, 2048], P('ep'), may hold values from -0.125 to 0.125
- mixer_norm_gain: float32 [2048], replicated, may hold values from 0.1 to 1.9
- mixer_norm_bias: float32 [2048], replicated, may hold values from -1.8 to 1.8
- expert_norm_gain: float32 [2048], replicated, may hold values from 0.1 to 1.9
- expert_norm_bias: float32 [2048], replicated, may hold values from -1.8 to 1.8
- routes: int32 [1024, 4], P(('grp', 'ep')), parts along dimension 0, may hold values from 0 to 63, all different within a row; in each aligned block of 4 rows (0 to 3, 4 to 7, ...) at most 2 rows name the same one
- routing_weight: float32 [1024, 4], P(('grp', 'ep')), parts along dimension 0, may hold values from 0.1 to 1
- expert_gate_weight: bfloat16 [64, 2048, 512], P('ep'), may hold values from -0.125 to 0.125
- expert_up_weight: bfloat16 [64, 2048, 512], P('ep'), may hold values from -0.125 to 0.125
- expert_down_weight: bfloat16 [64, 512, 2048], P('ep'), may hold values from -0.25 to 0.25
Outputs:
- result: bfloat16 [1024, 2048], P(('grp', 'ep')), parts along dimension 0
- next_state: float32 [1024, 32, 64, 64], P(('grp', 'ep')), parts along dimension 0
The draws below stay inside these ranges and needn't reach their ends.
There are 4 independent parts, one for each index of `grp`. The reference program is written for one: setup_inputs(seed, part) draws one part's arguments, and reference() takes and returns one part's arrays. A program takes and returns all parts, laid end to end along the dimension named above; an argument that names none is the same for every part. Nothing has to cross between parts.
Inputs may be any that keep to these rules, and one draw needn't show every extreme that they name: `routes`: A row names 4 different experts. Among the rows of one device no expert is named more than 2 times, and in some device one expert is named exactly 2 times; every expert is named somewhere.
All inputs are finite; a program needn't handle non-finite values.
Results may differ from the reference program's by a relative error of at most 0.0081.
Values may be sent and summed in bfloat16 or wider, within the bound.
A program may use at most 128 MiB of HBM per device.

```python
import math
import jax
import jax.numpy as jnp
import numpy as np
from jax import lax

D = 2048
MIXER_HEADS = 32
HEAD_CHANNELS = 64
W = 2048
DECAY_RANK = 64
LEARN_RANK = 64
GATE_RANK = 128
FF = 512
TOP = 4
SEQ_DEV = 4
TOKENS = 256
EXPERTS = 64
CAP = 2
N_EP = 64


def levels(own_key, extent, cuts, smallest, largest):
    factor_of, own = 1.0, jax.random.fold_in(own_key, 6)
    for axis_at, shards_of in cuts:
        heights = jnp.exp(jax.random.uniform(jax.random.fold_in(own, axis_at), (shards_of,), jnp.float32, smallest / len(cuts), largest / len(cuts)))
        factor_of = factor_of * jnp.repeat(heights, extent[axis_at] // shards_of).reshape([-1 if axis == axis_at else 1 for axis in range(len(extent))])
    return factor_of


def assign_block(rng, own, number, rows, number_of, top, reach, slope):
    order = jax.random.permutation(rng, number_of)
    heavy_load, usual = shares(number_of, rows * top, reach, slope, True), shares(number_of, rows * top, reach, slope, False)
    places = jnp.arange(number_of)

    def named(lengths, turn):
        used = int((lengths > 0).sum())
        fixed = max(1, used // 4)
        moved = fixed + (places - fixed + turn * (used - fixed)) % max(1, number_of - fixed)
        return jnp.zeros((number_of,), jnp.int32).at[order[jnp.where(places < fixed, places, moved)]].set(jnp.asarray(lengths, jnp.int32))

    lengths = jnp.where(number % 4 == 0, named(heavy_load, number // 4), named(usual, number - number // 4 - 1))
    mixed = jax.random.permutation(jax.random.fold_in(own, 3), number_of)
    source_of, receiver = mixed[0:number_of // 2 * 2:2], mixed[1:number_of // 2 * 2:2]
    room = jnp.minimum(lengths[source_of] - 1, reach - lengths[receiver]) // 2
    room = jnp.where((source_of == order[0]) | (receiver == order[0]) | (lengths[receiver] == 0), 0, jnp.maximum(room, 0))
    moved = jax.random.randint(jax.random.fold_in(own, 4), (number_of // 2,), 0, 1 << 20) % (room + 1)
    lengths = lengths.at[source_of].add(-moved).at[receiver].add(moved)
    labels = jnp.searchsorted(jnp.cumsum(lengths), jnp.arange(rows * top), side="right").astype(jnp.int32)
    listing = labels.reshape(top, rows).T
    listing = listing[jax.random.permutation(jax.random.fold_in(own, 1), rows)]
    turn = jax.random.randint(jax.random.fold_in(own, 2), (rows, 1), 0, top)
    return jnp.take_along_axis(listing, (jnp.arange(top)[None, :] + turn) % top, axis=1)


def shares(number_of, total, reach, lean, full):
    weights = [(1 << 20) // math.isqrt(standing ** lean) + 1 for standing in range(1, number_of + 1)]
    largest = reach if full else min(reach, max(-(-total // number_of), total * weights[0] // sum(weights)))
    least = 1 if total - largest >= number_of - 1 else 0
    given, spare = [largest] + [least] * (number_of - 1), total - largest - least * (number_of - 1)
    while spare > 0:
        free = [i for i in range(1, number_of) if given[i] < largest] or [i for i in range(1, number_of) if given[i] < reach]
        mass, remaining = sum([weights[i] for i in free]), spare
        for i in free:
            extra = min(reach - given[i], max(1, remaining * weights[i] // mass), spare)
            given[i] = given[i] + extra
            spare = spare - extra
    return np.array(given)


def noise(stream_key, extent, scale, limit, split=(), kind=jnp.bfloat16):
    factor_of = levels(stream_key, extent, split, -0.22, 0.18) if split else 1.0
    values = jax.random.normal(stream_key, extent, jnp.float32) * scale * factor_of
    return jnp.minimum(jnp.maximum(values, -limit), limit).astype(kind)


def setup_inputs(seed: int = 0, part: int = 0) -> dict:
    arg_keys = jax.random.split(jax.random.key(seed), 28)
    part_keys = jax.random.split(jax.random.fold_in(arg_keys[27], part), 28)
    tokens = noise(part_keys[0], (TOKENS, D), 1.0, 6.0, ((0, 64),))
    prior_state = noise(part_keys[1], (TOKENS, MIXER_HEADS, HEAD_CHANNELS, HEAD_CHANNELS), 0.3, 3.0, ((0, 64),), jnp.float32)
    receptance_matrix = noise(arg_keys[2], (D, W), D ** -0.5, 0.125, ((0, 64),))
    key_matrix = noise(arg_keys[3], (D, W), D ** -0.5, 0.125, ((0, 64),))
    value_matrix = noise(arg_keys[4], (D, W), D ** -0.5, 0.125, ((0, 64),))
    decay_lowrank_first = noise(arg_keys[5], (D, DECAY_RANK), D ** -0.5, 0.125)
    decay_lowrank_second = noise(arg_keys[6], (DECAY_RANK, W), (DECAY_RANK // 4) ** -0.5, 1.5)
    decay_channel_offset = jnp.clip(jax.random.uniform(arg_keys[7], (W,), jnp.float32, -6.0, 0.0), -6.0, 0.0)
    correction_lowrank_first = noise(arg_keys[8], (D, LEARN_RANK), D ** -0.5, 0.125)
    correction_lowrank_second = noise(arg_keys[9], (LEARN_RANK, W), (LEARN_RANK // 4) ** -0.5, 1.5)
    correction_offset = noise(arg_keys[10], (W,), 1.0, 4.0, (), jnp.float32)
    gate_lowrank_first = noise(arg_keys[11], (D, GATE_RANK), (D // 4) ** -0.5, 0.25)
    gate_lowrank_second = noise(arg_keys[12], (GATE_RANK, W), GATE_RANK ** -0.5, 0.5)
    key_rate_blend = jnp.clip(1.0 + 0.18 * jax.random.normal(arg_keys[13], (W,), jnp.float32), 0.1, 1.9)
    self_token_scale = noise(arg_keys[14], (MIXER_HEADS, HEAD_CHANNELS), 0.2, 1.2, (), jnp.float32)
    per_head_gain = jnp.clip(1.0 + 0.18 * jax.random.normal(arg_keys[15], (W,), jnp.float32), 0.1, 1.9)
    per_head_bias = noise(arg_keys[16], (W,), 0.3, 1.8, (), jnp.float32)
    mixer_output_weight = noise(arg_keys[17], (W, D), W ** -0.5, 0.125, ((0, 64),))
    mixer_norm_gain = jnp.clip(1.0 + 0.18 * jax.random.normal(arg_keys[18], (D,), jnp.float32), 0.1, 1.9)
    mixer_norm_bias = noise(arg_keys[19], (D,), 0.3, 1.8, (), jnp.float32)
    expert_norm_gain = jnp.clip(1.0 + 0.18 * jax.random.normal(arg_keys[20], (D,), jnp.float32), 0.1, 1.9)
    expert_norm_bias = noise(arg_keys[21], (D,), 0.3, 1.8, (), jnp.float32)
    routes_keys = jax.random.split(jax.random.fold_in(part_keys[22], 1), TOKENS // SEQ_DEV)
    routes_turns = jax.random.permutation(jax.random.fold_in(part_keys[22], 3), TOKENS // SEQ_DEV)
    routes = jax.vmap(lambda own, number: assign_block(jax.random.fold_in(part_keys[22], 2), own, number, SEQ_DEV, EXPERTS, TOP, CAP, 1))(routes_keys, routes_turns).reshape((TOKENS, TOP))
    routing_weight = jnp.clip(0.1 + 0.9 * jax.random.uniform(part_keys[23], (TOKENS, TOP), jnp.float32) ** levels(part_keys[23], (TOKENS, TOP), ((0, 64),), -0.2, 0.2), 0.1, 1.0)
    expert_gate_weight = noise(arg_keys[24], (EXPERTS, D, FF), D ** -0.5, 0.125, ((0, 64),))
    expert_up_weight = noise(arg_keys[25], (EXPERTS, D, FF), D ** -0.5, 0.125, ((0, 64),))
    expert_down_weight = noise(arg_keys[26], (EXPERTS, FF, D), FF ** -0.5, 0.25, ((0, 64),))
    return {"tokens": tokens, "prior_state": prior_state, "receptance_matrix": receptance_matrix, "key_matrix": key_matrix, "value_matrix": value_matrix, "decay_lowrank_first": decay_lowrank_first, "decay_lowrank_second": decay_lowrank_second, "decay_channel_offset": decay_channel_offset, "correction_lowrank_first": correction_lowrank_first, "correction_lowrank_second": correction_lowrank_second, "correction_offset": correction_offset, "gate_lowrank_first": gate_lowrank_first, "gate_lowrank_second": gate_lowrank_second, "key_rate_blend": key_rate_blend, "self_token_scale": self_token_scale, "per_head_gain": per_head_gain, "per_head_bias": per_head_bias, "mixer_output_weight": mixer_output_weight, "mixer_norm_gain": mixer_norm_gain, "mixer_norm_bias": mixer_norm_bias, "expert_norm_gain": expert_norm_gain, "expert_norm_bias": expert_norm_bias, "routes": routes, "routing_weight": routing_weight, "expert_gate_weight": expert_gate_weight, "expert_up_weight": expert_up_weight, "expert_down_weight": expert_down_weight}


def layer_norm(values_in, gain_vec, bias_vec):
    row_mean = lax.optimization_barrier(jnp.mean(values_in, -1, keepdims=True))
    centered = values_in - row_mean
    row_var = lax.optimization_barrier(jnp.mean(centered * centered, -1, keepdims=True))
    return centered * lax.rsqrt(row_var + 1e-05) * gain_vec + bias_vec

def recurrent_readout(tokens, prior_state, receptance_rows, key_rows, value_rows, decay_lowrank_first, decay_lowrank_second, decay_channel_offset, correction_lowrank_first, correction_lowrank_second, correction_offset, gate_lowrank_first, gate_lowrank_second, key_rate_blend, self_token_scale, per_head_gain, per_head_bias):
    row_count = tokens.shape[0]
    head_count = prior_state.shape[1]
    head_size = prior_state.shape[2]
    squash = jnp.tanh(jnp.dot(tokens, decay_lowrank_first, preferred_element_type=jnp.float32)).astype(jnp.bfloat16)
    pre_decay = decay_channel_offset + jnp.dot(squash, decay_lowrank_second, preferred_element_type=jnp.float32)
    decay_rate = jnp.exp(-jnp.exp(-jax.nn.softplus(-pre_decay) - 0.5))
    low_learn = jnp.dot(tokens, correction_lowrank_first, preferred_element_type=jnp.float32).astype(jnp.bfloat16)
    learn_rate = jax.nn.sigmoid(correction_offset + jnp.dot(low_learn, correction_lowrank_second, preferred_element_type=jnp.float32))
    opened = jax.nn.sigmoid(jnp.dot(tokens, gate_lowrank_first, preferred_element_type=jnp.float32)).astype(jnp.bfloat16)
    gating = jnp.dot(opened, gate_lowrank_second, preferred_element_type=jnp.float32)

    def by_head(flat_arr):
        return flat_arr.reshape(row_count, head_count, head_size)
    scaled = by_head(key_rows)
    unit_key = scaled * lax.rsqrt(lax.optimization_barrier(jnp.sum(scaled * scaled, -1, keepdims=True)) + 1e-06)
    written_key = by_head(key_rows * (1.0 + (learn_rate - 1.0) * key_rate_blend))
    receptance_by_head = by_head(receptance_rows)
    value_by_head = by_head(value_rows)
    removed = jnp.einsum('nhvk,nhk->nhv', prior_state, unit_key, precision=lax.Precision.HIGHEST)
    next_state = prior_state * by_head(decay_rate)[:, :, None, :] - removed[..., None] * (unit_key * by_head(learn_rate))[:, :, None, :] + value_by_head[..., None] * written_key[:, :, None, :]
    readout = jnp.einsum('nhvk,nhk->nhv', next_state, receptance_by_head, precision=lax.Precision.HIGHEST)
    head_mean = lax.optimization_barrier(jnp.mean(readout, -1, keepdims=True))
    head_dev = readout - head_mean
    head_var = lax.optimization_barrier(jnp.mean(head_dev * head_dev, -1, keepdims=True))
    normed = (head_dev * lax.rsqrt(head_var + 0.00064)).reshape(row_count, -1) * per_head_gain + per_head_bias
    self_token_term = lax.optimization_barrier(jnp.sum(receptance_by_head * written_key * self_token_scale, -1, keepdims=True)) * value_by_head
    mixer_result = ((normed + self_token_term.reshape(row_count, -1)) * gating).astype(jnp.bfloat16)
    return (mixer_result, next_state)

def reference(tokens, prior_state, receptance_matrix, key_matrix, value_matrix, decay_lowrank_first, decay_lowrank_second, decay_channel_offset, correction_lowrank_first, correction_lowrank_second, correction_offset, gate_lowrank_first, gate_lowrank_second, key_rate_blend, self_token_scale, per_head_gain, per_head_bias, mixer_output_weight, mixer_norm_gain, mixer_norm_bias, expert_norm_gain, expert_norm_bias, routes, routing_weight, expert_gate_weight, expert_up_weight, expert_down_weight):
    receptance_rows = jnp.dot(tokens, receptance_matrix, preferred_element_type=jnp.float32)
    key_rows = jnp.dot(tokens, key_matrix, preferred_element_type=jnp.float32)
    value_rows = jnp.dot(tokens, value_matrix, preferred_element_type=jnp.float32)
    mixer_result, next_state = recurrent_readout(tokens, prior_state, receptance_rows, key_rows, value_rows, decay_lowrank_first, decay_lowrank_second, decay_channel_offset, correction_lowrank_first, correction_lowrank_second, correction_offset, gate_lowrank_first, gate_lowrank_second, key_rate_blend, self_token_scale, per_head_gain, per_head_bias)
    mixed = jnp.dot(mixer_result, mixer_output_weight, preferred_element_type=jnp.float32)
    hidden = layer_norm(tokens.astype(jnp.float32) + mixed, mixer_norm_gain, mixer_norm_bias).astype(jnp.bfloat16)
    model_width = hidden.shape[1]
    flat_ids = routes.reshape(-1).astype(jnp.int32)
    slot_total = flat_ids.shape[0]
    sort_order = jnp.argsort(flat_ids, stable=True).astype(jnp.int32)
    sorted_ids = flat_ids[sort_order]
    expert_ids = jnp.arange(EXPERTS, dtype=jnp.int32)
    counts = lax.optimization_barrier(jnp.sum((flat_ids[None, :] == expert_ids[:, None]).astype(jnp.int32), 1))
    starts = jnp.cumsum(counts) - counts
    column = jnp.arange(N_EP * CAP, dtype=jnp.int32)

    def one_expert(expert_item):
        gate_mat, up_mat, down_mat, first_slot, slot_count = expert_item
        row_index = sort_order[jnp.minimum(first_slot + column, slot_total - 1)]
        live = (column < slot_count).astype(jnp.bfloat16)
        rows_in = hidden[row_index // TOP] * live[:, None]
        gate_val = jnp.dot(rows_in, gate_mat, preferred_element_type=jnp.float32)
        up_val = jnp.dot(rows_in, up_mat, preferred_element_type=jnp.float32)
        inner = (jax.nn.silu(gate_val) * up_val).astype(jnp.bfloat16)
        return jnp.dot(inner, down_mat, preferred_element_type=jnp.float32).astype(jnp.bfloat16)
    produced = lax.map(one_expert, (expert_gate_weight, expert_up_weight, expert_down_weight, starts, counts))
    position = jnp.arange(slot_total, dtype=jnp.int32) - starts[sorted_ids]
    sorted_out = produced[sorted_ids, position]
    flat_out = jnp.zeros_like(sorted_out).at[sort_order].set(sorted_out)
    share = routing_weight / lax.optimization_barrier(jnp.sum(routing_weight, -1, keepdims=True))
    combined = lax.optimization_barrier(jnp.sum(flat_out.reshape(-1, TOP, model_width).astype(jnp.float32) * share[..., None], 1))
    result = layer_norm(hidden.astype(jnp.float32) + combined, expert_norm_gain, expert_norm_bias).astype(jnp.bfloat16)
    return (result, next_state)
```

```python
import functools

import jax
import jax.numpy as jnp
from jax import lax
from jax.experimental import pallas as pl
from jax.experimental.pallas import tpu as pltpu
from jax.sharding import PartitionSpec as P

MESH = pl.DeviceIdType.MESH
F32 = jnp.float32
BF16 = jnp.bfloat16
ROWS = 4
HEAD = 64
STRIDE = 4


def dot(a, b):
    return jnp.dot(a, b, preferred_element_type=F32)


def lane_ids(shape):
    return lax.broadcasted_iota(jnp.int32, shape, len(shape) - 1)


def row_ids(shape):
    return lax.broadcasted_iota(jnp.int32, shape, len(shape) - 2)


def kernel(
    nz,
    share,
    ff,
    tok_ref,
    state_hbm,
    wr_hbm,
    wk_hbm,
    wv_hbm,
    wo_hbm,
    dl1,
    dl2,
    doff,
    cl1,
    cl2,
    coff,
    gl1,
    gl2,
    blend,
    sscale,
    hgain,
    hbias,
    mgain,
    mbias,
    egain,
    ebias,
    routes,
    rweight,
    eg_hbm,
    eu_hbm,
    ed_hbm,
    out_ref,
    next_hbm,
    st,
    wstage,
    wsend,
    wb,
    em,
    xt,
    xm,
    xh,
    ysend,
    yrecv,
    msend,
    mrecv,
    cb,
    csend,
    tok8,
    tokp,
    hidp,
    dh,
    ah,
    gh,
    ro,
    sv,
    eg,
    eu,
    ed,
    zown,
    zoth,
    zsib,
    tsum,
    r1,
    u2,
    r2,
    ld_sem,
    w_send,
    w_recv,
    q_send,
    q_recv,
    s_send,
    s_recv,
    l1_send,
    l1_recv,
    l2_send,
    l2_recv,
    a_send,
    a_recv,
    x_send,
    x_recv,
    f1_send,
    f1_recv,
    f2_send,
    f2_recv,
    bar_wait_dummy,
):
    nk = nz // STRIDE
    dim = HEAD * nz
    half = dim // 2
    nm = 4 // share
    ep = lax.axis_index("ep")
    grp = lax.axis_index("grp")
    z = ep // 2
    c = ep % 2
    gq = grp % share
    gbase = grp - gq
    res = z % STRIDE
    own_k = z // STRIDE
    sib = {"ep": z * 2 + 1 - c}

    def chip(zt):
        return {"ep": (zt % nz) * 2 + c}

    def slot_of(zt):
        return (zt % STRIDE) * nk + zt // STRIDE

    def far_first(j):
        d = nz // 2 - (j + 1) // 2
        return (z + nz + d * (1 - 2 * (j % 2))) % nz

    bar = pltpu.get_barrier_semaphore()

    @pl.loop(1, nz)
    def _(j):
        pl.semaphore_signal(bar, inc=1, device_id=chip(z + j), device_id_type=MESH)

    pl.semaphore_signal(bar, inc=1, device_id=sib, device_id_type=MESH)
    for i in range(1, share):
        pl.semaphore_signal(
            bar, inc=1, device_id={"grp": gbase + (gq + i) % share}, device_id_type=MESH
        )

    w_hbm = (wr_hbm, wk_hbm, wv_hbm, wo_hbm)
    for i in range(nm):
        for m in range(4):
            if m % nm == i:

                @pl.when(gq == m // nm)
                def _(i=i, m=m):
                    pltpu.make_async_copy(w_hbm[m], wstage.at[i], ld_sem.at[i]).start()

    st_load = pltpu.make_async_copy(state_hbm, st, ld_sem.at[4])
    eg_load = pltpu.make_async_copy(eg_hbm.at[0], eg, ld_sem.at[5])
    eu_load = pltpu.make_async_copy(eu_hbm.at[0], eu, ld_sem.at[6])
    ed_load = pltpu.make_async_copy(ed_hbm.at[0], ed, ld_sem.at[7])
    st_load.start()
    eg_load.start()
    eu_load.start()
    ed_load.start()

    lane128 = lane_ids((8, 128))
    left = lane128 < HEAD
    top = row_ids((8, 128)) < ROWS
    lane16 = lane_ids((16, 128))
    left16 = lane16 < HEAD

    tok = tok_ref[...].astype(F32)
    tok8[0:ROWS, :] = tok
    tok8[ROWS : 2 * ROWS, :] = tok
    tokp[0:ROWS, :] = tok[:, :half]
    tokp[ROWS : 2 * ROWS, :] = tok[:, half:]
    xt[res, own_k] = tokp[...].astype(BF16)

    for i in range(nm):
        pltpu.make_async_copy(w_hbm[0], wstage.at[i], ld_sem.at[i]).wait()

        @pl.loop(0, nz // 2)
        def _(t, i=i):
            at = pl.multiple_of(t * 128, 128)
            a = wstage[i, 0:16, pl.ds(at, 128)].astype(F32)
            b = wstage[i, 16:32, pl.ds(at, 128)].astype(F32)
            wsend[i, 2 * t] = jnp.where(left16, a, pltpu.roll(b, HEAD, 1)).astype(BF16)
            wsend[i, 2 * t + 1] = jnp.where(left16, pltpu.roll(a, HEAD, 1), b).astype(BF16)

        wb[gq * nm + i, c, z] = wsend[i, z]

    weight = rweight[...]
    part = weight / jnp.sum(weight, -1, keepdims=True)
    ids = routes[...]
    lanes4 = lane_ids((ROWS, 128))
    by_expert = jnp.zeros((ROWS, 128), F32)
    for k in range(ids.shape[1]):
        by_expert += jnp.where(ids[:, k : k + 1] == lanes4, part[:, k : k + 1], 0.0)
    high = by_expert.astype(BF16).astype(F32)
    low = by_expert - high
    both = jnp.where(lanes4 < HEAD, high, pltpu.roll(low, HEAD, 1))
    sv[0, 0:ROWS, :] = both
    sv[0, ROWS : 2 * ROWS, :] = both
    csend[...] = sv[0].astype(BF16)
    my_slot = slot_of(z)
    cb[c, my_slot] = csend[...]

    def gather_start(buf, n):
        for d in [nk // 2] + [x for y in range(nk // 2 - 1, 0, -1) for x in (y, nk - y)]:
            kt = (own_k + d) % nk
            pltpu.make_async_remote_copy(
                src_ref=buf.at[res, own_k],
                dst_ref=buf.at[res, own_k],
                send_sem=l1_send.at[n, d],
                recv_sem=l1_recv.at[n, nk - d],
                device_id=chip(kt * STRIDE + res),
                device_id_type=MESH,
            ).start()

    def level_two(buf, n):
        hk = nk // 2
        up, down, far = (res + 1) % STRIDE, (res + STRIDE - 1) % STRIDE, (res + 2) % STRIDE
        steps = (
            (1, buf.at[res], buf.at[down]),
            (nz - 1, buf.at[res], buf.at[up]),
            (2, buf.at[res, pl.ds(0, hk)], buf.at[far, pl.ds(0, hk)]),
            (nz - 2, buf.at[res, pl.ds(hk, hk)], buf.at[far, pl.ds(hk, hk)]),
        )
        sends, recvs = [], []
        for i, (d, src, arrives) in enumerate(steps):
            sends.append(
                pltpu.make_async_remote_copy(
                    src_ref=src,
                    dst_ref=src,
                    send_sem=l2_send.at[n, i],
                    recv_sem=l2_recv.at[n, i],
                    device_id=chip(z + d),
                    device_id_type=MESH,
                )
            )
            recvs.append(
                pltpu.make_async_remote_copy(
                    src_ref=arrives,
                    dst_ref=arrives,
                    send_sem=l2_send.at[n, i],
                    recv_sem=l2_recv.at[n, i],
                    device_id=chip(z + d),
                    device_id_type=MESH,
                )
            )
        return sends, recvs

    def gather_relay(buf, n):
        for d in range(1, nk):
            at = buf.at[res, (own_k + d) % nk]
            pltpu.make_async_remote_copy(
                src_ref=at,
                dst_ref=at,
                send_sem=l1_send.at[n, d],
                recv_sem=l1_recv.at[n, d],
                device_id=chip(z),
                device_id_type=MESH,
            ).wait_recv()
        sends, _ = level_two(buf, n)
        for s in sends:
            s.start()

    def gather_wait(buf, n):
        _, recvs = level_two(buf, n)
        for r in recvs:
            r.wait_recv()

    def gather_drain(buf, n):
        for d in range(1, nk):
            at = buf.at[res, own_k]
            pltpu.make_async_remote_copy(
                src_ref=at,
                dst_ref=at,
                send_sem=l1_send.at[n, d],
                recv_sem=l1_recv.at[n, d],
                device_id=chip(z),
                device_id_type=MESH,
            ).wait_send()
        sends, _ = level_two(buf, n)
        for s in sends:
            s.wait_send()

    def scatter(src_of, dst, send_sem, recv_sem):
        @pl.loop(0, nz - 1)
        def _(j):
            zt = far_first(j)
            pltpu.make_async_remote_copy(
                src_ref=src_of(zt),
                dst_ref=dst,
                send_sem=send_sem,
                recv_sem=recv_sem,
                device_id=chip(zt),
                device_id_type=MESH,
            ).start()

    def scatter_all(block, send_sem, recv_sem):
        return pltpu.make_async_remote_copy(
            src_ref=block.at[pl.ds(0, nz - 1)],
            dst_ref=block.at[pl.ds(0, nz - 1)],
            send_sem=send_sem,
            recv_sem=recv_sem,
            device_id=chip(z),
            device_id_type=MESH,
        )

    pl.semaphore_wait(bar, nz - 1 + 1 + share - 1)

    gather_start(xt, 0)
    for i in range(nm):
        m = gq * nm + i
        scatter(lambda zt, i=i: wsend.at[i, zt], wb.at[m, c, z], w_send.at[i], w_recv.at[i])

    tokb = tok8[...].astype(BF16)
    squash = jnp.tanh(dot(tokb, dl1[...])).astype(BF16)
    lowl = dot(tokb, cl1[...]).astype(BF16)
    opened = jax.nn.sigmoid(dot(tokb, gl1[...])).astype(BF16)

    for j in range(nz // 2):
        cols = slice(128 * j, 128 * j + 128)

        def two_heads(ref, tile, j=j):
            ref[2 * j] = tile
            ref[2 * j + 1] = pltpu.roll(tile, HEAD, 1)

        pre = doff[:, cols] + dot(squash, dl2[:, cols])
        two_heads(dh, jnp.exp(-(jnp.exp(jnp.full((8, 128), -0.5, F32)) * jax.nn.sigmoid(pre))))
        two_heads(ah, jax.nn.sigmoid(coff[:, cols] + dot(lowl, cl2[:, cols])))
        two_heads(gh, dot(opened, gl2[:, cols]))

    gather_relay(xt, 0)

    def slab(m, core, to, send_sem, recv_sem):
        return pltpu.make_async_remote_copy(
            src_ref=wb.at[m, core],
            dst_ref=wb.at[m, core],
            send_sem=send_sem,
            recv_sem=recv_sem,
            device_id=to,
            device_id_type=MESH,
        )

    for i in range(nm):
        m = gq * nm + i
        scatter_all(wb.at[m, c], w_send.at[i], w_recv.at[i]).wait_recv()
        for g in range(1, share):
            slab(
                m,
                c,
                {"grp": gbase + (gq + g) % share},
                q_send.at[g, i],
                q_recv.at[share - g, i],
            ).start()
        slab(m, c, sib, s_send.at[0, i], s_recv.at[0, i]).start()
    for g in range(1, share):
        for i in range(nm):
            m = ((gq + g) % share) * nm + i
            slab(m, c, sib, q_send.at[g, i], q_recv.at[g, i]).wait_recv()
            slab(m, c, sib, s_send.at[g, i], s_recv.at[g, i]).start()

    def widen(m, at):
        keep = left16.astype(F32).astype(BF16)
        drop = (1.0 - left16.astype(F32)).astype(BF16)
        for hk in range(2):

            @pl.loop(0, nz // 2)
            def _(zz, hk=hk):
                for core in range(2):
                    tile = wb[m, core, hk * (nz // 2) + zz]
                    base = pl.multiple_of(zz * 64 + core * 32, 32)
                    cols = slice(at + hk * 128, at + hk * 128 + 128)
                    em[pl.ds(base, 16), cols] = tile * keep
                    em[pl.ds(pl.multiple_of(base + 16, 16), 16), cols] = tile * drop

    def rows_of(value):
        return value.astype(F32).reshape(8 * nz, half).astype(BF16)

    top3 = row_ids((nz, 8, 128)) < ROWS
    left3 = lane_ids((nz, 8, 128)) < HEAD
    topw = (row_ids((8 * nz, 128)) % 8) < ROWS

    def fold(r):
        a = jnp.where(topw, r[:, 0:128], r[:, 128:256])
        a = (a + pltpu.roll(a, HEAD, 1)).reshape(nz, 8, 128)
        return a + pltpu.roll(a, ROWS, 1)

    for g in range(share):
        for i in range(nm):
            m = ((gq + g) % share) * nm + i
            slab(m, 1 - c, sib, s_send.at[g, i], s_recv.at[g, i]).wait_recv()

    for m in range(4):
        widen(m, m * 256)

    gather_wait(xt, 0)
    xv = rows_of(xt[...])
    cr = fold(dot(xv, em[:, 0:256]))
    ck = fold(dot(xv, em[:, 256:512]))
    cv = fold(dot(xv, em[:, 512:768]))
    ysend[...] = jnp.where(top3, jnp.where(left3, cr, ck), cv).astype(BF16)
    scatter(lambda zt: ysend.at[slot_of(zt)], yrecv.at[z], a_send.at[0], a_recv.at[0])
    yrecv[z] = ysend[my_slot]
    scatter(lambda zt: csend, cb.at[c, my_slot], a_send.at[2], a_recv.at[2])
    st_load.wait()
    scatter_all(yrecv, a_send.at[0], a_recv.at[0]).wait_recv()

    eye = (
        lax.broadcasted_iota(jnp.int32, (HEAD, HEAD), 0)
        == lax.broadcasted_iota(jnp.int32, (HEAD, HEAD), 1)
    ).astype(F32)

    def pick(ref, j):
        tile = jnp.broadcast_to(ref[:, 128 * j : 128 * j + 128], (8, 128))
        return tile, pltpu.roll(tile, HEAD, 1)

    blends, scales = [], []
    for j in range(nz // 2):
        blends += pick(blend, j)
        scales += pick(sscale, j)
    for h in range(nz):
        ro[h] = blends[h]
        sv[h] = scales[h]

    @pl.loop(0, nz)
    def _(h):
        y = yrecv[h].astype(F32)
        turned = pltpu.roll(y, ROWS, 0)
        rk = jnp.where(top, y, turned)
        v = jnp.where(top, turned, y)
        r = jnp.where(left, rk, 0.0)
        k = jnp.where(left, pltpu.roll(rk, HEAD, 1), 0.0)
        a = ah[h]
        unit = k * lax.rsqrt(jnp.sum(k * k, -1, keepdims=True) + 1e-06)
        written = k * (1.0 + (a - 1.0) * ro[h])
        ua = unit * a
        own = jnp.sum(r * written * sv[h], -1, keepdims=True)
        d = dh[h]
        sv[h] = own * v
        for t in range(ROWS):
            one = slice(t, t + 1)
            s = st[t, h]
            removed = jnp.sum(s * unit[one, 0:HEAD], -1, keepdims=True)
            vcol = jnp.sum(eye * v[one, 0:HEAD], -1, keepdims=True)
            n = s * d[one, 0:HEAD] - removed * ua[one, 0:HEAD] + vcol * written[one, 0:HEAD]
            st[t, h] = n
            rcol = jnp.sum(n * r[one, 0:HEAD], -1, keepdims=True)
            row = jnp.sum(eye * rcol, 0, keepdims=True)
            ro[h, t : t + 1, 0:HEAD] = row
            ro[h, ROWS + t : ROWS + t + 1, 0:HEAD] = row

    st_store = pltpu.make_async_copy(st, next_hbm, ld_sem.at[4])
    st_store.start()

    def mixer_head(h, gain, bias):
        x = jnp.where(left, ro[h], 0.0)
        mean = jnp.sum(x, -1, keepdims=True) * (1.0 / HEAD)
        dev = jnp.where(left, x - mean, 0.0)
        var = jnp.sum(dev * dev, -1, keepdims=True) * (1.0 / HEAD)
        normed = dev * lax.rsqrt(var + 0.00064) * gain + bias
        return (normed + sv[h]) * gh[h]

    def mixer_pair(j):
        g0, g1 = pick(hgain, j)
        b0, b1 = pick(hbias, j)
        one, two = mixer_head(2 * j, g0, b0), mixer_head(2 * j + 1, g1, b1)
        return jnp.where(left, one, pltpu.roll(two, HEAD, 1))

    for j in range(nz // 4):
        tile = jnp.where(top, mixer_pair(j), mixer_pair(nz // 4 + j))
        xm[res, own_k, :, 128 * j : 128 * j + 128] = tile.astype(BF16)

    gather_start(xm, 1)
    gather_relay(xm, 1)
    gather_wait(xm, 1)
    co = fold(dot(rows_of(xm[...]), em[:, 768:1024]))
    co_high = co.astype(BF16).astype(F32)
    msend[...] = jnp.where(top3, co_high, co - co_high).astype(BF16)
    scatter(lambda zt: msend.at[slot_of(zt)], mrecv.at[z], a_send.at[1], a_recv.at[1])
    mrecv[z] = msend[my_slot]

    scatter_all(cb.at[c], a_send.at[2], a_recv.at[2]).wait_recv()

    def to_sib(src, dst, n):
        return pltpu.make_async_remote_copy(
            src_ref=src,
            dst_ref=dst,
            send_sem=x_send.at[n],
            recv_sem=x_recv.at[n],
            device_id=sib,
            device_id_type=MESH,
        )

    to_sib(cb.at[c], cb.at[c], 0).start()

    scatter_all(mrecv, a_send.at[1], a_recv.at[1]).wait_recv()
    for j in range(nz // 4):

        def mixed_pair(p):
            one, two = mrecv[2 * p].astype(F32), mrecv[2 * p + 1].astype(F32)
            tile = jnp.where(left, one, two)
            return tile + pltpu.roll(tile, ROWS, 0)

        cols = slice(128 * j, 128 * j + 128)
        tokp[:, cols] += jnp.where(top, mixed_pair(j), mixed_pair(nz // 4 + j))

    topp = row_ids((8, half)) < ROWS

    def packed(ref):
        return jnp.where(topp, ref[:, 0:half], ref[:, half:dim])

    def row_total(x):
        s = jnp.broadcast_to(jnp.sum(x, -1, keepdims=True), (8, 128))
        s = s + pltpu.roll(s, ROWS, 0)
        return s[:, 0:1] * (1.0 / dim)

    def layer_norm(x, gain, bias):
        dev = x - row_total(x)
        var = row_total(dev * dev)
        return dev * lax.rsqrt(var + 1e-05) * packed(gain) + packed(bias)

    hidden = layer_norm(tokp[...], mgain, mbias).astype(BF16)
    hidp[...] = hidden.astype(F32)
    xh[c, res, own_k] = hidden
    mine = xh.at[c]
    gather_start(mine, 2)
    gather_relay(mine, 2)
    gather_wait(mine, 2)
    to_sib(xh.at[c], xh.at[c], 1).start()

    eg_load.wait()
    eu_load.wait()
    ed_load.wait()
    to_sib(cb.at[1 - c], cb.at[1 - c], 0).wait_recv()

    def wide_fold(a, b):
        width = a.shape[1]
        keep = (row_ids((8 * nz, width)) % 8) < ROWS
        x = jnp.where(keep, a, b).reshape(nz, 8, width)
        return (x + pltpu.roll(x, ROWS, 1)).reshape(8 * nz, width)

    def expert(core):
        xv = rows_of(xh[core])
        lane3 = lane_ids((nz, 8, 128))
        hit = (lane3 == ep) | (lane3 == ep + HEAD)
        coef = jnp.sum(jnp.where(hit, cb[core].astype(F32), 0.0), -1, keepdims=True)
        coef = coef.reshape(8 * nz, 1)
        gate = wide_fold(dot(xv, eg[0:half, :]), dot(xv, eg[half:dim, :]))
        up = wide_fold(dot(xv, eu[0:half, :]), dot(xv, eu[half:dim, :]))
        inner = (gate * jax.nn.sigmoid(gate) * up).astype(BF16)
        return inner, coef

    def down(inner, coef, j, width):
        a = dot(inner, ed[:, j * width : (j + 1) * width])
        b = dot(inner, ed[:, half + j * width : half + (j + 1) * width])
        keep = (row_ids((8 * nz, width)) % 8) < ROWS
        return (jnp.where(keep, a, b) * coef).reshape(STRIDE, nk, 8, width)

    width = min(256, half)
    inner, coef = expert(c)
    for j in range(half // width):
        zown[:, :, :, j * width : (j + 1) * width] = down(inner, coef, j, width).astype(BF16)
    to_sib(xh.at[1 - c], xh.at[1 - c], 1).wait_recv()
    inner, coef = expert(1 - c)
    for j in range(half // width):
        zoth[:, :, :, j * width : (j + 1) * width] = down(inner, coef, j, width).astype(BF16)
    to_sib(zoth, zsib, 2).start()
    to_sib(zoth, zsib, 2).wait_recv()
    tsum[...] = (zown[...].astype(F32) + zsib[...].astype(F32)).astype(BF16)

    hk = nk // 2
    up, down_, far = (res + 1) % STRIDE, (res + STRIDE - 1) % STRIDE, (res + 2) % STRIDE
    first = (
        (1, tsum.at[up], r1.at[0]),
        (nz - 1, tsum.at[down_], r1.at[1]),
        (2, tsum.at[far, pl.ds(0, hk)], r1.at[2, pl.ds(0, hk)]),
        (nz - 2, tsum.at[far, pl.ds(hk, hk)], r1.at[2, pl.ds(hk, hk)]),
    )
    copies = [
        pltpu.make_async_remote_copy(
            src_ref=src,
            dst_ref=dst,
            send_sem=f1_send.at[i],
            recv_sem=f1_recv.at[i],
            device_id=chip(z + d),
            device_id_type=MESH,
        )
        for i, (d, src, dst) in enumerate(first)
    ]
    for cp in copies:
        cp.start()
    for cp in copies:
        cp.wait_recv()
    u2[...] = (
        tsum[res].astype(F32)
        + r1[0].astype(F32)
        + r1[1].astype(F32)
        + r1[2].astype(F32)
    ).astype(BF16)

    def last(d):
        kt = (own_k + d) % nk
        return pltpu.make_async_remote_copy(
            src_ref=u2.at[kt],
            dst_ref=r2.at[nk - d],
            send_sem=f2_send.at[d],
            recv_sem=f2_recv.at[nk - d],
            device_id=chip(kt * STRIDE + res),
            device_id_type=MESH,
        )

    for d in [nk // 2] + [x for y in range(nk // 2 - 1, 0, -1) for x in (y, nk - y)]:
        last(d).start()
    total = hidp[...] + u2[own_k].astype(F32)
    for d in range(1, nk):
        pltpu.make_async_remote_copy(
            src_ref=r2.at[d],
            dst_ref=r2.at[d],
            send_sem=f2_send.at[d],
            recv_sem=f2_recv.at[d],
            device_id=chip(z),
            device_id_type=MESH,
        ).wait_recv()
    for d in range(1, nk):
        total = total + r2[d].astype(F32)
    y = layer_norm(total, egain, ebias)
    out_ref[:, 0:half] = y[0:ROWS, :].astype(BF16)
    out_ref[:, half:dim] = y[ROWS : 2 * ROWS, :].astype(BF16)

    gather_drain(xt, 0)
    gather_drain(xm, 1)
    gather_drain(mine, 2)
    for i in range(nm):
        scatter_all(wb.at[gq * nm + i, c], w_send.at[i], w_recv.at[i]).wait_send()
        slab(gq * nm + i, c, sib, s_send.at[0, i], s_recv.at[0, i]).wait_send()
        for g in range(1, share):
            slab(gq * nm + i, c, sib, q_send.at[g, i], q_recv.at[g, i]).wait_send()
            m = ((gq + g) % share) * nm + i
            slab(m, c, sib, s_send.at[g, i], s_recv.at[g, i]).wait_send()
    scatter_all(yrecv, a_send.at[0], a_recv.at[0]).wait_send()
    scatter_all(mrecv, a_send.at[1], a_recv.at[1]).wait_send()
    scatter_all(cb.at[c], a_send.at[2], a_recv.at[2]).wait_send()
    to_sib(cb.at[c], cb.at[c], 0).wait_send()
    to_sib(xh.at[c], xh.at[c], 1).wait_send()
    to_sib(zoth, zsib, 2).wait_send()
    for cp in copies:
        cp.wait_send()
    for d in range(1, nk):
        last(d).wait_send()
    st_store.wait()


def step(nz, share, *args):
    tokens, state = args[0], args[1]
    dim = tokens.shape[1]
    half = dim // 2
    nk = nz // STRIDE
    nm = 4 // share
    ff = args[24].shape[2]
    args = list(args)
    for i in (7, 10, 13, 14, 15, 16, 18, 19, 20, 21):
        args[i] = args[i].reshape(1, dim)
    order = [0, 1, 2, 3, 4, 17, 5, 6, 7, 8, 9, 10, 11, 12, 13, 14, 15, 16, 18, 19, 20, 21]
    order += [22, 23, 24, 25, 26]
    operands = [args[i] for i in order]
    in_hbm = {1, 2, 3, 4, 5, 24, 25, 26}
    vmem = pl.BlockSpec(memory_space=pltpu.VMEM)
    hbm = pl.BlockSpec(memory_space=pl.ANY)
    dma = pltpu.SemaphoreType.DMA
    heads = (nz, 8, 128)
    rows = (STRIDE, nk, 8, half)
    scratch = [
        pltpu.VMEM(state.shape, F32),
        pltpu.VMEM((nm, 32, dim), BF16),
        pltpu.VMEM((nm, nz, 16, 128), BF16),
        pltpu.VMEM((4, 2, nz, 16, 128), BF16),
        pltpu.VMEM((half, 1024), BF16),
        pltpu.VMEM(rows, BF16),
        pltpu.VMEM(rows, BF16),
        pltpu.VMEM((2,) + rows, BF16),
        pltpu.VMEM(heads, BF16),
        pltpu.VMEM(heads, BF16),
        pltpu.VMEM(heads, BF16),
        pltpu.VMEM(heads, BF16),
        pltpu.VMEM((2,) + heads, BF16),
        pltpu.VMEM((8, 128), BF16),
        pltpu.VMEM((8, dim), F32),
        pltpu.VMEM((8, half), F32),
        pltpu.VMEM((8, half), F32),
        pltpu.VMEM(heads, F32),
        pltpu.VMEM(heads, F32),
        pltpu.VMEM(heads, F32),
        pltpu.VMEM(heads, F32),
        pltpu.VMEM(heads, F32),
        pltpu.VMEM((dim, ff), BF16),
        pltpu.VMEM((dim, ff), BF16),
        pltpu.VMEM((ff, dim), BF16),
        pltpu.VMEM(rows, BF16),
        pltpu.VMEM(rows, BF16),
        pltpu.VMEM(rows, BF16),
        pltpu.VMEM(rows, BF16),
        pltpu.VMEM((3, nk, 8, half), BF16),
        pltpu.VMEM((nk, 8, half), BF16),
        pltpu.VMEM((nk, 8, half), BF16),
        dma((8,)),
        dma((nm,)),
        dma((nm,)),
        dma((share, nm)),
        dma((share, nm)),
        dma((share, nm)),
        dma((share, nm)),
        dma((3, nk)),
        dma((3, nk)),
        dma((3, 4)),
        dma((3, 4)),
        dma((3,)),
        dma((3,)),
        dma((3,)),
        dma((3,)),
        dma((4,)),
        dma((4,)),
        dma((nk,)),
        dma((nk,)),
        dma((1,)),
    ]
    return pl.pallas_call(
        functools.partial(kernel, nz, share, ff),
        out_shape=(
            jax.ShapeDtypeStruct(tokens.shape, BF16),
            jax.ShapeDtypeStruct(state.shape, F32),
        ),
        in_specs=[hbm if i in in_hbm else vmem for i in range(len(operands))],
        out_specs=(vmem, hbm),
        scratch_shapes=scratch,
        compiler_params=pltpu.CompilerParams(
            collective_id=0, has_side_effects=True, vmem_limit_bytes=56 * 1024 * 1024
        ),
    )(*operands)


def solution(mesh):
    nz = mesh.shape["ep"] // 2
    groups = mesh.shape["grp"]
    share = 4 if groups % 4 == 0 else 2 if groups % 2 == 0 else 1
    owned, split, copied = P(("grp", "ep"), None), P("ep", None), P()
    in_specs = (
        owned,
        P(("grp", "ep"), None, None, None),
        split,
        split,
        split,
        *([copied] * 12),
        split,
        *([copied] * 4),
        owned,
        owned,
        P("ep", None, None),
        P("ep", None, None),
        P("ep", None, None),
    )
    out_specs = (owned, P(("grp", "ep"), None, None, None))
    return jax.shard_map(
        functools.partial(step, nz, share),
        mesh=mesh,
        in_specs=in_specs,
        out_specs=out_specs,
        check_vma=False,
    )
```

```python
import functools

import jax
import jax.numpy as jnp
from jax import lax
from jax.experimental import pallas as pl
from jax.experimental.pallas import tpu as pltpu
from jax.sharding import PartitionSpec as P

MESH = pl.DeviceIdType.MESH
F32 = jnp.float32
BF16 = jnp.bfloat16
SMALL = 18
ROWS = 4
HEAD = 64
STRIDE = 4


def dot(a, b):
    return jnp.dot(a, b, preferred_element_type=F32)


def lane_ids(shape):
    return lax.broadcasted_iota(jnp.int32, shape, len(shape) - 1)


def row_ids(shape):
    return lax.broadcasted_iota(jnp.int32, shape, len(shape) - 2)


def kernel(
    nz,
    share,
    tok_hbm,
    state_hbm,
    wr_hbm,
    wk_hbm,
    wv_hbm,
    wo_hbm,
    *rest,
):
    small_hbm, rest = rest[:SMALL], rest[SMALL:]
    run(nz, share, tok_hbm, state_hbm, (wr_hbm, wk_hbm, wv_hbm, wo_hbm), small_hbm, *rest)


def run(
    nz,
    share,
    tok_hbm,
    state_hbm,
    w_hbm,
    small_hbm,
    eg_hbm,
    eu_hbm,
    ed_hbm,
    out_ref,
    next_hbm,
    tok_ref,
    *rest,
):
    small, rest = rest[:SMALL], rest[SMALL:]
    work(nz, share, tok_hbm, state_hbm, w_hbm, small_hbm, eg_hbm, eu_hbm, ed_hbm,
         out_ref, next_hbm, tok_ref, small, *rest)


def work(
    nz,
    share,
    tok_hbm,
    state_hbm,
    w_hbm,
    small_hbm,
    eg_hbm,
    eu_hbm,
    ed_hbm,
    out_ref,
    next_hbm,
    tok_ref,
    small,
    st,
    sn,
    wstage,
    wsend,
    wb,
    em,
    xt,
    xm,
    xh,
    ysend,
    yrecv,
    msend,
    mrecv,
    cb,
    csend,
    tok8,
    tokp,
    hidp,
    dh,
    ah,
    gh,
    ro,
    sv,
    bh,
    eg,
    eu,
    ed,
    zown,
    zoth,
    zsib,
    tsum,
    r1,
    u2,
    r2,
    ld_sem,
    w_send,
    w_recv,
    q_send,
    q_recv,
    s_send,
    s_recv,
    l1_send,
    l1_recv,
    l2_send,
    l2_recv,
    a_send,
    a_recv,
    x_send,
    x_recv,
    f1_send,
    f1_recv,
    f2_send,
    f2_recv,
    small_sem,
):
    (
        dl1, dl2, doff, cl1, cl2, coff, gl1, gl2, blend,
        sscale, hgain, hbias, mgain, mbias, egain, ebias, routes, rweight,
    ) = small
    nk = nz // STRIDE
    dim = HEAD * nz
    half = dim // 2
    nm = 4 // share
    ep = lax.axis_index("ep")
    grp = lax.axis_index("grp")
    z = ep // 2
    c = ep % 2
    gq = grp % share
    gbase = grp - gq
    res = z % STRIDE
    own_k = z // STRIDE
    sib = {"ep": z * 2 + 1 - c}

    def chip(zt):
        return {"ep": (zt % nz) * 2 + c}

    def slot_of(zt):
        return (zt % STRIDE) * nk + zt // STRIDE

    def far_first(j):
        d = nz // 2 - (j + 1) // 2
        return (z + nz + d * (1 - 2 * (j % 2))) % nz

    bar = pltpu.get_barrier_semaphore()

    @pl.loop(1, nz)
    def _(j):
        pl.semaphore_signal(bar, inc=1, device_id=chip(z + j), device_id_type=MESH)

    pl.semaphore_signal(bar, inc=1, device_id=sib, device_id_type=MESH)
    for i in range(1, share):
        pl.semaphore_signal(
            bar, inc=1, device_id={"grp": gbase + (gq + i) % share}, device_id_type=MESH
        )

    tok_load = pltpu.make_async_copy(tok_hbm, tok_ref, ld_sem.at[8])
    tok_load.start()
    for i in range(nm):
        for m in range(4):
            if m % nm == i:

                @pl.when(gq == m // nm)
                def _(i=i, m=m):
                    pltpu.make_async_copy(w_hbm[m], wstage.at[i], ld_sem.at[i]).start()

    st_load = pltpu.make_async_copy(state_hbm, st, ld_sem.at[4])
    eg_load = pltpu.make_async_copy(eg_hbm.at[0], eg, ld_sem.at[5])
    eu_load = pltpu.make_async_copy(eu_hbm.at[0], eu, ld_sem.at[6])
    ed_load = pltpu.make_async_copy(ed_hbm.at[0], ed, ld_sem.at[7])
    small_loads = [
        pltpu.make_async_copy(a, b, small_sem.at[i])
        for i, (a, b) in enumerate(zip(small_hbm, small))
    ]
    for cp in small_loads:
        cp.start()
    st_load.start()
    eg_load.start()
    eu_load.start()
    ed_load.start()

    lane128 = lane_ids((8, 128))
    left = lane128 < HEAD
    top = row_ids((8, 128)) < ROWS
    lane16 = lane_ids((16, 128))
    left16 = lane16 < HEAD

    tok_load.wait()
    tok = tok_ref[...].astype(F32)
    tok8[0:ROWS, :] = tok
    tok8[ROWS : 2 * ROWS, :] = tok
    tokp[0:ROWS, :] = tok[:, :half]
    tokp[ROWS : 2 * ROWS, :] = tok[:, half:]
    xt[res, own_k] = tokp[...].astype(BF16)

    for i in range(nm):
        pltpu.make_async_copy(w_hbm[0], wstage.at[i], ld_sem.at[i]).wait()

        @pl.loop(0, nz // 2)
        def _(t, i=i):
            at = pl.multiple_of(t * 128, 128)
            a = wstage[i, 0:16, pl.ds(at, 128)].astype(F32)
            b = wstage[i, 16:32, pl.ds(at, 128)].astype(F32)
            wsend[i, 2 * t] = jnp.where(left16, a, pltpu.roll(b, HEAD, 1)).astype(BF16)
            wsend[i, 2 * t + 1] = jnp.where(left16, pltpu.roll(a, HEAD, 1), b).astype(BF16)

        wb[gq * nm + i, c, z] = wsend[i, z]

    for cp in small_loads:
        cp.wait()
    weight = rweight[...]
    part = weight / jnp.sum(weight, -1, keepdims=True)
    ids = routes[...]
    lanes4 = lane_ids((ROWS, 128))
    by_expert = jnp.zeros((ROWS, 128), F32)
    for k in range(ids.shape[1]):
        by_expert += jnp.where(ids[:, k : k + 1] == lanes4, part[:, k : k + 1], 0.0)
    high = by_expert.astype(BF16).astype(F32)
    low = by_expert - high
    both = jnp.where(lanes4 < HEAD, high, pltpu.roll(low, HEAD, 1))
    sv[0, 0:ROWS, :] = both
    sv[0, ROWS : 2 * ROWS, :] = both
    csend[...] = sv[0].astype(BF16)
    my_slot = slot_of(z)
    cb[c, my_slot] = csend[...]

    side = 1 - 2 * (own_k % 2)
    hk = nk // 2

    def step_copy(buf, n, slot, sem, kt):
        at = buf.at[res, slot % nk]
        return pltpu.make_async_remote_copy(
            src_ref=at,
            dst_ref=at,
            send_sem=l1_send.at[n, sem],
            recv_sem=l1_recv.at[n, sem],
            device_id=chip((kt % nk) * STRIDE + res),
            device_id_type=MESH,
        )

    def near_copies(buf, n, slot):
        k = slot % nk
        at = buf.at[res, k]
        part = k // hk
        for i, to, sem in ((0, z + 1, 0), (1, z + nz - 1, 1), (2, z + nz + 2 - 4 * part, 2 + part)):
            pltpu.make_async_remote_copy(
                src_ref=at,
                dst_ref=at,
                send_sem=l2_send.at[n, i],
                recv_sem=l2_recv.at[n, sem],
                device_id=chip(to),
                device_id_type=MESH,
            ).start()

    direct = [(0, -1), (1, 1)] + ([(2, -2), (3, 2)] if nk > 4 else []) if nk > 2 else []
    direct += [(6, nk // 2)] if nk in (2, 4) else []
    onward = [(4, -3), (5, 3), (6, 4)] if nk == 8 else []

    def gather_start(buf, n):
        for sem, o in reversed(direct):
            step_copy(buf, n, own_k, sem, own_k + nk - o).start()
        near_copies(buf, n, own_k)

    def gather_direct(buf, n):
        for sem, o in direct:
            step_copy(buf, n, own_k + nk + o, sem, own_k).wait_recv()
            if sem == 2 and onward:
                step_copy(buf, n, own_k + nk - 2, 4, own_k + 1).start()
            if sem == 3 and onward:
                step_copy(buf, n, own_k + nk + 2, 5, own_k + nk - 1).start()
                step_copy(buf, n, own_k + nk - 2 * side, 6, own_k + nk + 2 * side).start()
            if sem < 2 or not onward:
                near_copies(buf, n, own_k + nk + o)
        if onward:
            near_copies(buf, n, own_k + nk - 2)
            near_copies(buf, n, own_k + nk + 2)

    def gather_onward(buf, n):
        for sem, o in onward:
            step_copy(buf, n, own_k + nk + o, sem, own_k).wait_recv()
            near_copies(buf, n, own_k + nk + o)

    def near_all(buf, n, i, sem, r, k0, count):
        at = buf.at[r, pl.ds(k0, count)]
        return pltpu.make_async_remote_copy(
            src_ref=at,
            dst_ref=at,
            send_sem=l2_send.at[n, i],
            recv_sem=l2_recv.at[n, sem],
            device_id=chip(z + 1),
            device_id_type=MESH,
        )

    def gather_wait(buf, n):
        near_all(buf, n, 0, 0, (res + STRIDE - 1) % STRIDE, 0, nk).wait_recv()
        near_all(buf, n, 1, 1, (res + 1) % STRIDE, 0, nk).wait_recv()
        near_all(buf, n, 2, 2, (res + 2) % STRIDE, 0, hk).wait_recv()
        near_all(buf, n, 2, 3, (res + 2) % STRIDE, hk, hk).wait_recv()

    def gather_drain(buf, n):
        for sem, _ in direct + onward:
            step_copy(buf, n, own_k, sem, own_k).wait_send()
        for i in range(3):
            near_all(buf, n, i, i, res, 0, nk).wait_send()

    def scatter(src_of, dst, send_sem, recv_sem):
        @pl.loop(0, nz - 1)
        def _(j):
            zt = far_first(j)
            pltpu.make_async_remote_copy(
                src_ref=src_of(zt),
                dst_ref=dst,
                send_sem=send_sem,
                recv_sem=recv_sem,
                device_id=chip(zt),
                device_id_type=MESH,
            ).start()

    def scatter_all(block, send_sem, recv_sem):
        return pltpu.make_async_remote_copy(
            src_ref=block.at[pl.ds(0, nz - 1)],
            dst_ref=block.at[pl.ds(0, nz - 1)],
            send_sem=send_sem,
            recv_sem=recv_sem,
            device_id=chip(z),
            device_id_type=MESH,
        )

    pl.semaphore_wait(bar, nz - 1 + 1 + share - 1)

    for i in range(nm):
        m = gq * nm + i
        scatter(lambda zt, i=i: wsend.at[i, zt], wb.at[m, c, z], w_send.at[i], w_recv.at[i])
    gather_start(xt, 0)

    tokb = tok8[...].astype(BF16)

    def dot_t(a, b):
        return lax.dot_general(a, b, (((1,), (1,)), ((), ())), preferred_element_type=F32)

    squash = jnp.tanh(dot_t(tokb, dl1[...])).astype(BF16)
    lowl = dot_t(tokb, cl1[...]).astype(BF16)
    opened = jax.nn.sigmoid(dot(tokb, gl1[...])).astype(BF16)

    for j in range(nz // 2):
        cols = slice(128 * j, 128 * j + 128)

        def two_heads(ref, tile, j=j):
            ref[2 * j] = tile
            ref[2 * j + 1] = pltpu.roll(tile, HEAD, 1)

        pre = doff[:, cols] + dot(squash, dl2[:, cols])
        two_heads(dh, jnp.exp(-(jnp.exp(jnp.full((8, 128), -0.5, F32)) * jax.nn.sigmoid(pre))))
        two_heads(ah, jax.nn.sigmoid(coff[:, cols] + dot(lowl, cl2[:, cols])))
        two_heads(gh, dot(opened, gl2[:, cols]))

    gather_direct(xt, 0)

    def slab(m, core, to, send_sem, recv_sem):
        return pltpu.make_async_remote_copy(
            src_ref=wb.at[m, core],
            dst_ref=wb.at[m, core],
            send_sem=send_sem,
            recv_sem=recv_sem,
            device_id=to,
            device_id_type=MESH,
        )

    for i in range(nm):
        m = gq * nm + i
        scatter_all(wb.at[m, c], w_send.at[i], w_recv.at[i]).wait_recv()
        for g in range(1, share):
            slab(
                m,
                c,
                {"grp": gbase + (gq + g) % share},
                q_send.at[g, i],
                q_recv.at[share - g, i],
            ).start()
        slab(m, c, sib, s_send.at[0, i], s_recv.at[0, i]).start()
    gather_onward(xt, 0)
    for g in range(1, share):
        for i in range(nm):
            m = ((gq + g) % share) * nm + i
            slab(m, c, sib, q_send.at[g, i], q_recv.at[g, i]).wait_recv()
            slab(m, c, sib, s_send.at[g, i], s_recv.at[g, i]).start()

    def widen(m, at):
        keep = left16.astype(F32).astype(BF16)
        drop = (1.0 - left16.astype(F32)).astype(BF16)
        for hk in range(2):

            @pl.loop(0, nz // 2)
            def _(zz, hk=hk):
                for core in range(2):
                    tile = wb[m, core, hk * (nz // 2) + zz]
                    base = pl.multiple_of(zz * 64 + core * 32, 32)
                    cols = slice(at + hk * 128, at + hk * 128 + 128)
                    em[pl.ds(base, 16), cols] = tile * keep
                    em[pl.ds(pl.multiple_of(base + 16, 16), 16), cols] = tile * drop

    def rows_of(value):
        return value.astype(F32).reshape(8 * nz, half).astype(BF16)

    top3 = row_ids((nz, 8, 128)) < ROWS
    left3 = lane_ids((nz, 8, 128)) < HEAD
    topw = (row_ids((8 * nz, 128)) % 8) < ROWS

    def fold(r):
        a = jnp.where(topw, r[:, 0:128], r[:, 128:256])
        a = (a + pltpu.roll(a, HEAD, 1)).reshape(nz, 8, 128)
        return a + pltpu.roll(a, ROWS, 1)

    for g in range(share):
        for i in range(nm):
            m = ((gq + g) % share) * nm + i
            slab(m, 1 - c, sib, s_send.at[g, i], s_recv.at[g, i]).wait_recv()

    for m in range(4):
        widen(m, m * 256)

    gather_wait(xt, 0)
    xv = rows_of(xt[...])
    cr = fold(dot(xv, em[:, 0:256]))
    ck = fold(dot(xv, em[:, 256:512]))
    cv = fold(dot(xv, em[:, 512:768]))
    ysend[...] = jnp.where(top3, jnp.where(left3, cr, ck), cv).astype(BF16)
    scatter(lambda zt: ysend.at[slot_of(zt)], yrecv.at[z], a_send.at[0], a_recv.at[0])
    yrecv[z] = ysend[my_slot]
    scatter(lambda zt: csend, cb.at[c, my_slot], a_send.at[2], a_recv.at[2])
    st_load.wait()
    scatter_all(yrecv, a_send.at[0], a_recv.at[0]).wait_recv()

    eye = (
        lax.broadcasted_iota(jnp.int32, (HEAD, HEAD), 0)
        == lax.broadcasted_iota(jnp.int32, (HEAD, HEAD), 1)
    ).astype(F32)

    def pick(ref, j):
        tile = jnp.broadcast_to(ref[:, 128 * j : 128 * j + 128], (8, 128))
        return tile, pltpu.roll(tile, HEAD, 1)

    blends = []
    for j in range(nz // 2):
        blends += pick(blend, j)
    for h in range(nz):
        bh[h] = blends[h]

    ones = jnp.ones((HEAD, HEAD), BF16)

    def row_sums(x):
        high = x.astype(BF16)
        low = (x - high.astype(F32)).astype(BF16)
        return dot(high, ones) + dot(low, ones)

    @pl.loop(0, nz // 2)
    def _(pair):
        for h in (2 * pair, 2 * pair + 1):
            y = yrecv[h].astype(F32)
            turned = pltpu.roll(y, ROWS, 0)
            rk = jnp.where(top, y, turned)
            v = jnp.where(top, turned, y)
            r = jnp.where(left, rk, 0.0)
            k = jnp.where(left, pltpu.roll(rk, HEAD, 1), 0.0)
            a = ah[h]
            unit = k * lax.rsqrt(jnp.sum(k * k, -1, keepdims=True) + 1e-06)
            written = k * (1.0 + (a - 1.0) * bh[h])
            ua = unit * a
            scale = sscale[pl.ds(h, 1), :]
            own = jnp.sum((r * written)[:, 0:HEAD] * scale, -1, keepdims=True)
            d = dh[h]
            sv[h] = own * v
            for t in range(ROWS):
                one = slice(t, t + 1)
                s = st[t, h]
                removed = row_sums(s * unit[one, 0:HEAD])
                vcol = dot((eye * v[one, 0:HEAD]).astype(BF16), ones)
                n = s * d[one, 0:HEAD] - removed * ua[one, 0:HEAD] + vcol * written[one, 0:HEAD]
                sn[t, h] = n
                row = jnp.sum(eye * row_sums(n * r[one, 0:HEAD]), 0, keepdims=True)
                ro[h, t : t + 1, 0:HEAD] = row
                ro[h, ROWS + t : ROWS + t + 1, 0:HEAD] = row

    st_store = pltpu.make_async_copy(sn, next_hbm, ld_sem.at[4])
    st_store.start()

    def mixer_head(h, gain, bias):
        x = jnp.where(left, ro[h], 0.0)
        mean = jnp.sum(x, -1, keepdims=True) * (1.0 / HEAD)
        dev = jnp.where(left, x - mean, 0.0)
        var = jnp.sum(dev * dev, -1, keepdims=True) * (1.0 / HEAD)
        normed = dev * lax.rsqrt(var + 0.00064) * gain + bias
        return (normed + sv[h]) * gh[h]

    def mixer_pair(j):
        g0, g1 = pick(hgain, j)
        b0, b1 = pick(hbias, j)
        one, two = mixer_head(2 * j, g0, b0), mixer_head(2 * j + 1, g1, b1)
        return jnp.where(left, one, pltpu.roll(two, HEAD, 1))

    for j in range(nz // 4):
        tile = jnp.where(top, mixer_pair(j), mixer_pair(nz // 4 + j))
        xm[res, own_k, :, 128 * j : 128 * j + 128] = tile.astype(BF16)

    gather_start(xm, 1)
    gather_direct(xm, 1)
    gather_onward(xm, 1)
    gather_wait(xm, 1)
    co = fold(dot(rows_of(xm[...]), em[:, 768:1024]))
    co_high = co.astype(BF16).astype(F32)
    msend[...] = jnp.where(top3, co_high, co - co_high).astype(BF16)
    scatter(lambda zt: msend.at[slot_of(zt)], mrecv.at[z], a_send.at[1], a_recv.at[1])
    mrecv[z] = msend[my_slot]

    scatter_all(cb.at[c], a_send.at[2], a_recv.at[2]).wait_recv()

    def to_sib(src, dst, n):
        return pltpu.make_async_remote_copy(
            src_ref=src,
            dst_ref=dst,
            send_sem=x_send.at[n],
            recv_sem=x_recv.at[n],
            device_id=sib,
            device_id_type=MESH,
        )

    to_sib(cb.at[c], cb.at[c], 0).start()

    scatter_all(mrecv, a_send.at[1], a_recv.at[1]).wait_recv()
    for j in range(nz // 4):

        def mixed_pair(p):
            one, two = mrecv[2 * p].astype(F32), mrecv[2 * p + 1].astype(F32)
            tile = jnp.where(left, one, two)
            return tile + pltpu.roll(tile, ROWS, 0)

        cols = slice(128 * j, 128 * j + 128)
        tokp[:, cols] += jnp.where(top, mixed_pair(j), mixed_pair(nz // 4 + j))

    topp = row_ids((8, half)) < ROWS

    def packed(ref):
        return jnp.where(topp, ref[:, 0:half], ref[:, half:dim])

    def row_total(x):
        s = jnp.broadcast_to(jnp.sum(x, -1, keepdims=True), (8, 128))
        s = s + pltpu.roll(s, ROWS, 0)
        return s[:, 0:1] * (1.0 / dim)

    def layer_norm(x, gain, bias):
        dev = x - row_total(x)
        var = row_total(dev * dev)
        return dev * lax.rsqrt(var + 1e-05) * packed(gain) + packed(bias)

    hidden = layer_norm(tokp[...], mgain, mbias).astype(BF16)
    hidp[...] = hidden.astype(F32)
    xh[c, res, own_k] = hidden
    mine = xh.at[c]
    gather_start(mine, 2)
    gather_direct(mine, 2)
    gather_onward(mine, 2)
    gather_wait(mine, 2)
    to_sib(xh.at[c], xh.at[c], 1).start()

    eg_load.wait()
    eu_load.wait()
    ed_load.wait()
    to_sib(cb.at[1 - c], cb.at[1 - c], 0).wait_recv()

    def wide_fold(a, b):
        width = a.shape[1]
        keep = (row_ids((8 * nz, width)) % 8) < ROWS
        x = jnp.where(keep, a, b).reshape(nz, 8, width)
        return (x + pltpu.roll(x, ROWS, 1)).reshape(8 * nz, width)

    def expert(core):
        xv = rows_of(xh[core])
        lane3 = lane_ids((nz, 8, 128))
        hit = (lane3 == ep) | (lane3 == ep + HEAD)
        coef = jnp.sum(jnp.where(hit, cb[core].astype(F32), 0.0), -1, keepdims=True)
        coef = coef.reshape(8 * nz, 1)
        gate = wide_fold(dot(xv, eg[0:half, :]), dot(xv, eg[half:dim, :]))
        up = wide_fold(dot(xv, eu[0:half, :]), dot(xv, eu[half:dim, :]))
        inner = (gate * jax.nn.sigmoid(gate) * up).astype(BF16)
        return inner, coef

    def down(inner, coef, j, width):
        a = dot(inner, ed[:, j * width : (j + 1) * width])
        b = dot(inner, ed[:, half + j * width : half + (j + 1) * width])
        keep = (row_ids((8 * nz, width)) % 8) < ROWS
        return (jnp.where(keep, a, b) * coef).reshape(STRIDE, nk, 8, width)

    width = min(256, half)
    inner, coef = expert(c)
    for j in range(half // width):
        zown[:, :, :, j * width : (j + 1) * width] = down(inner, coef, j, width).astype(BF16)
    to_sib(xh.at[1 - c], xh.at[1 - c], 1).wait_recv()
    inner, coef = expert(1 - c)
    for j in range(half // width):
        zoth[:, :, :, j * width : (j + 1) * width] = down(inner, coef, j, width).astype(BF16)
    to_sib(zoth, zsib, 2).start()
    to_sib(zoth, zsib, 2).wait_recv()
    tsum[...] = (zown[...].astype(F32) + zsib[...].astype(F32)).astype(BF16)

    def near_sum(slot):
        k = slot % nk
        part = k // hk
        up, down_, far = (res + 1) % STRIDE, (res + STRIDE - 1) % STRIDE, (res + 2) % STRIDE
        return [
            pltpu.make_async_remote_copy(
                src_ref=tsum.at[r, k],
                dst_ref=r1.at[i, k],
                send_sem=f1_send.at[i],
                recv_sem=f1_recv.at[i, k],
                device_id=chip(to),
                device_id_type=MESH,
            )
            for i, (to, r) in enumerate(
                ((z + 1, up), (z + nz - 1, down_), (z + nz + 2 - 4 * part, far))
            )
        ]

    def step_sum(kt, src, sem):
        return pltpu.make_async_remote_copy(
            src_ref=u2.at[src],
            dst_ref=r2.at[sem],
            send_sem=f2_send.at[sem],
            recv_sem=f2_recv.at[sem],
            device_id=chip((kt % nk) * STRIDE + res),
            device_id_type=MESH,
        )

    def near_total(slot):
        k = slot % nk
        for cp in near_sum(k):
            cp.wait_recv()
        return (
            tsum[res, k].astype(F32)
            + r1[0, k].astype(F32)
            + r1[1, k].astype(F32)
            + r1[2, k].astype(F32)
        )

    def arrived(sem):
        step_sum(own_k, 0, sem).wait_recv()
        return r2[sem].astype(F32)

    if nk == 8:
        order = [nk + 4, nk - 3, nk + 3, nk - 2 * side, nk + 2 * side, nk - 1, nk + 1, nk]
    else:
        order = [nk // 2] + ([1, nk - 1] if nk == 4 else []) + [nk]
    for o in order:
        for cp in near_sum(own_k + o):
            cp.start()
    if nk == 8:
        u2[0] = near_total(own_k + 4).astype(BF16)
        step_sum(own_k + nk + 2 * side * -1, 0, 0).start()
        u2[1] = near_total(own_k + nk - 3 * side).astype(BF16)
        step_sum(own_k + nk - side, 1, 1).start()
        u2[2] = near_total(own_k + nk + 3 * side).astype(BF16)
        step_sum(own_k + nk + side, 2, 2).start()
        u2[3] = near_total(own_k + nk - side).astype(BF16)
        step_sum(own_k + nk - side, 3, 3).start()
        u2[4] = near_total(own_k + nk + side).astype(BF16)
        step_sum(own_k + nk + side, 4, 4).start()
        part_b = near_total(own_k + nk + 2 * side)
        part_a = near_total(own_k + nk - 2 * side)
        u2[6] = (part_b + arrived(1)).astype(BF16)
        step_sum(own_k + nk + 2 * side, 6, 6).start()
        u2[5] = (part_a + arrived(2) + arrived(0)).astype(BF16)
        step_sum(own_k + nk - 2 * side, 5, 5).start()
        total = near_total(own_k)
        used = range(7)
    else:
        for i, o in enumerate(order[:-1]):
            u2[i] = near_total(own_k + o).astype(BF16)
            step_sum(own_k + o, i, i).start()
        total = near_total(own_k)
        used = range(len(order) - 1)
    total = total + hidp[...]
    for sem in used:
        if nk != 8 or sem >= 3:
            total = total + arrived(sem)
    y = layer_norm(total, egain, ebias)
    out_ref[:, 0:half] = y[0:ROWS, :].astype(BF16)
    out_ref[:, half:dim] = y[ROWS : 2 * ROWS, :].astype(BF16)

    gather_drain(xt, 0)
    gather_drain(xm, 1)
    gather_drain(mine, 2)
    for i in range(nm):
        scatter_all(wb.at[gq * nm + i, c], w_send.at[i], w_recv.at[i]).wait_send()
        slab(gq * nm + i, c, sib, s_send.at[0, i], s_recv.at[0, i]).wait_send()
        for g in range(1, share):
            slab(gq * nm + i, c, sib, q_send.at[g, i], q_recv.at[g, i]).wait_send()
            m = ((gq + g) % share) * nm + i
            slab(m, c, sib, s_send.at[g, i], s_recv.at[g, i]).wait_send()
    scatter_all(yrecv, a_send.at[0], a_recv.at[0]).wait_send()
    scatter_all(mrecv, a_send.at[1], a_recv.at[1]).wait_send()
    scatter_all(cb.at[c], a_send.at[2], a_recv.at[2]).wait_send()
    to_sib(cb.at[c], cb.at[c], 0).wait_send()
    to_sib(xh.at[c], xh.at[c], 1).wait_send()
    to_sib(zoth, zsib, 2).wait_send()
    for i in range(3):
        pltpu.make_async_remote_copy(
            src_ref=tsum.at[res],
            dst_ref=r1.at[i],
            send_sem=f1_send.at[i],
            recv_sem=f1_recv.at[i, 0],
            device_id=chip(z + 1),
            device_id_type=MESH,
        ).wait_send()
    for sem in used:
        step_sum(own_k, sem, sem).wait_send()
    st_store.wait()


def step(nz, share, *args):
    tokens, state = args[0], args[1]
    dim = tokens.shape[1]
    half = dim // 2
    nk = nz // STRIDE
    nm = 4 // share
    ff = args[24].shape[2]
    args = list(args)
    args[5], args[8] = args[5].T, args[8].T
    for i in (7, 10, 13, 15, 16, 18, 19, 20, 21):
        args[i] = args[i].reshape(1, dim)
    small = [5, 6, 7, 8, 9, 10, 11, 12, 13, 14, 15, 16, 18, 19, 20, 21, 22, 23]
    operands = [args[i] for i in [0, 1, 2, 3, 4, 17] + small + [24, 25, 26]]
    vmem = pl.BlockSpec(memory_space=pltpu.VMEM)
    hbm = pl.BlockSpec(memory_space=pl.ANY)
    dma = pltpu.SemaphoreType.DMA
    heads = (nz, 8, 128)
    rows = (STRIDE, nk, 8, half)
    scratch = [
        pltpu.VMEM(tokens.shape, BF16),
        *[pltpu.VMEM(args[i].shape, args[i].dtype) for i in small],
        pltpu.VMEM(state.shape, F32),
        pltpu.VMEM(state.shape, F32),
        pltpu.VMEM((nm, 32, dim), BF16),
        pltpu.VMEM((nm, nz, 16, 128), BF16),
        pltpu.VMEM((4, 2, nz, 16, 128), BF16),
        pltpu.VMEM((half, 1024), BF16),
        pltpu.VMEM(rows, BF16),
        pltpu.VMEM(rows, BF16),
        pltpu.VMEM((2,) + rows, BF16),
        pltpu.VMEM(heads, BF16),
        pltpu.VMEM(heads, BF16),
        pltpu.VMEM(heads, BF16),
        pltpu.VMEM(heads, BF16),
        pltpu.VMEM((2,) + heads, BF16),
        pltpu.VMEM((8, 128), BF16),
        pltpu.VMEM((8, dim), F32),
        pltpu.VMEM((8, half), F32),
        pltpu.VMEM((8, half), F32),
        pltpu.VMEM(heads, F32),
        pltpu.VMEM(heads, F32),
        pltpu.VMEM(heads, F32),
        pltpu.VMEM(heads, F32),
        pltpu.VMEM(heads, F32),
        pltpu.VMEM(heads, F32),
        pltpu.VMEM((dim, ff), BF16),
        pltpu.VMEM((dim, ff), BF16),
        pltpu.VMEM((ff, dim), BF16),
        pltpu.VMEM(rows, BF16),
        pltpu.VMEM(rows, BF16),
        pltpu.VMEM(rows, BF16),
        pltpu.VMEM(rows, BF16),
        pltpu.VMEM((3, nk, 8, half), BF16),
        pltpu.VMEM((nk, 8, half), BF16),
        pltpu.VMEM((nk, 8, half), BF16),
        dma((9,)),
        dma((nm,)),
        dma((nm,)),
        dma((share, nm)),
        dma((share, nm)),
        dma((share, nm)),
        dma((share, nm)),
        dma((3, 7)),
        dma((3, 7)),
        dma((3, 3)),
        dma((3, 4)),
        dma((3,)),
        dma((3,)),
        dma((3,)),
        dma((3,)),
        dma((3,)),
        dma((3, nk)),
        dma((7,)),
        dma((7,)),
        dma((SMALL,)),
    ]
    return pl.pallas_call(
        functools.partial(kernel, nz, share),
        out_shape=(
            jax.ShapeDtypeStruct(tokens.shape, BF16),
            jax.ShapeDtypeStruct(state.shape, F32),
        ),
        in_specs=[hbm] * len(operands),
        out_specs=(vmem, hbm),
        scratch_shapes=scratch,
        compiler_params=pltpu.CompilerParams(
            collective_id=0, has_side_effects=True, vmem_limit_bytes=56 * 1024 * 1024
        ),
    )(*operands)


def solution(mesh):
    nz = mesh.shape["ep"] // 2
    groups = mesh.shape["grp"]
    share = 4 if groups % 4 == 0 else 2 if groups % 2 == 0 else 1
    owned, split, copied = P(("grp", "ep"), None), P("ep", None), P()
    in_specs = (
        owned,
        P(("grp", "ep"), None, None, None),
        split,
        split,
        split,
        *([copied] * 12),
        split,
        *([copied] * 4),
        owned,
        owned,
        P("ep", None, None),
        P("ep", None, None),
        P("ep", None, None),
    )
    out_specs = (owned, P(("grp", "ep"), None, None, None))
    return jax.shard_map(
        functools.partial(step, nz, share),
        mesh=mesh,
        in_specs=in_specs,
        out_specs=out_specs,
        check_vma=False,
    )
```

```python
import functools

import jax
import jax.numpy as jnp
from jax import lax
from jax.experimental import pallas as pl
from jax.experimental.pallas import tpu as pltpu
from jax.sharding import PartitionSpec as P

MESH = pl.DeviceIdType.MESH
F32 = jnp.float32
BF16 = jnp.bfloat16
SMALL = 18
ROWS = 4
HEAD = 64
STRIDE = 4


def dot(a, b):
    return jnp.dot(a, b, preferred_element_type=F32)


def lane_ids(shape):
    return lax.broadcasted_iota(jnp.int32, shape, len(shape) - 1)


def row_ids(shape):
    return lax.broadcasted_iota(jnp.int32, shape, len(shape) - 2)


def kernel(
    nz,
    share,
    tok_hbm,
    state_hbm,
    wr_hbm,
    wk_hbm,
    wv_hbm,
    wo_hbm,
    *rest,
):
    small_hbm, rest = rest[:SMALL], rest[SMALL:]
    run(nz, share, tok_hbm, state_hbm, (wr_hbm, wk_hbm, wv_hbm, wo_hbm), small_hbm, *rest)


def run(
    nz,
    share,
    tok_hbm,
    state_hbm,
    w_hbm,
    small_hbm,
    eg_hbm,
    eu_hbm,
    ed_hbm,
    out_ref,
    next_hbm,
    tok_ref,
    *rest,
):
    small, rest = rest[:SMALL], rest[SMALL:]
    work(nz, share, tok_hbm, state_hbm, w_hbm, small_hbm, eg_hbm, eu_hbm, ed_hbm,
         out_ref, next_hbm, tok_ref, small, *rest)


def work(
    nz,
    share,
    tok_hbm,
    state_hbm,
    w_hbm,
    small_hbm,
    eg_hbm,
    eu_hbm,
    ed_hbm,
    out_ref,
    next_hbm,
    tok_ref,
    small,
    st,
    sn,
    wstage,
    wsend,
    wb,
    em,
    xt,
    xm,
    xh,
    ysend,
    yrecv,
    msend,
    mrecv,
    cb,
    csend,
    tok8,
    tokp,
    hidp,
    dh,
    ah,
    gh,
    ro,
    sv,
    bh,
    eg,
    eu,
    ed,
    zown,
    zoth,
    zsib,
    tsum,
    r1,
    u2,
    r2,
    ld_sem,
    w_send,
    w_recv,
    q_send,
    q_recv,
    s_send,
    s_recv,
    l1_send,
    l1_recv,
    l2_send,
    l2_recv,
    a_send,
    a_recv,
    x_send,
    x_recv,
    f1_send,
    f1_recv,
    f2_send,
    f2_recv,
    small_sem,
):
    (
        dl1, dl2, doff, cl1, cl2, coff, gl1, gl2, blend,
        sscale, hgain, hbias, mgain, mbias, egain, ebias, routes, rweight,
    ) = small
    nk = nz // STRIDE
    dim = HEAD * nz
    half = dim // 2
    nm = 4 // share
    ep = lax.axis_index("ep")
    grp = lax.axis_index("grp")
    z = ep // 2
    c = ep % 2
    gq = grp % share
    gbase = grp - gq
    res = z % STRIDE
    own_k = z // STRIDE
    sib = {"ep": z * 2 + 1 - c}

    def chip(zt):
        return {"ep": (zt % nz) * 2 + c}

    def slot_of(zt):
        return (zt % STRIDE) * nk + zt // STRIDE

    def far_first(j):
        d = nz // 2 - (j + 1) // 2
        return (z + nz + d * (1 - 2 * (j % 2))) % nz

    bar = pltpu.get_barrier_semaphore()

    @pl.loop(1, nz)
    def _(j):
        pl.semaphore_signal(bar, inc=1, device_id=chip(z + j), device_id_type=MESH)

    pl.semaphore_signal(bar, inc=1, device_id=sib, device_id_type=MESH)
    for i in range(1, share):
        pl.semaphore_signal(
            bar, inc=1, device_id={"grp": gbase + (gq + i) % share}, device_id_type=MESH
        )

    tok_load = pltpu.make_async_copy(tok_hbm, tok_ref, ld_sem.at[8])
    tok_load.start()
    for i in range(nm):
        for m in range(4):
            if m % nm == i:

                @pl.when(gq == m // nm)
                def _(i=i, m=m):
                    pltpu.make_async_copy(w_hbm[m], wstage.at[i], ld_sem.at[i]).start()

    st_load = pltpu.make_async_copy(state_hbm, st, ld_sem.at[4])
    eg_load = pltpu.make_async_copy(eg_hbm.at[0], eg, ld_sem.at[5])
    eu_load = pltpu.make_async_copy(eu_hbm.at[0], eu, ld_sem.at[6])
    ed_load = pltpu.make_async_copy(ed_hbm.at[0], ed, ld_sem.at[7])
    small_loads = [
        pltpu.make_async_copy(a, b, small_sem.at[i])
        for i, (a, b) in enumerate(zip(small_hbm, small))
    ]
    for cp in small_loads:
        cp.start()
    st_load.start()
    eg_load.start()
    eu_load.start()
    ed_load.start()

    lane128 = lane_ids((8, 128))
    left = lane128 < HEAD
    top = row_ids((8, 128)) < ROWS
    lane16 = lane_ids((16, 128))
    left16 = lane16 < HEAD

    tok_load.wait()
    tok = tok_ref[...].astype(F32)
    tok8[0:ROWS, :] = tok
    tok8[ROWS : 2 * ROWS, :] = tok
    tokp[0:ROWS, :] = tok[:, :half]
    tokp[ROWS : 2 * ROWS, :] = tok[:, half:]
    xt[res, own_k] = tokp[...].astype(BF16)

    for i in range(nm):
        pltpu.make_async_copy(w_hbm[0], wstage.at[i], ld_sem.at[i]).wait()

        @pl.loop(0, nz // 2)
        def _(t, i=i):
            at = pl.multiple_of(t * 128, 128)
            a = wstage[i, 0:16, pl.ds(at, 128)].astype(F32)
            b = wstage[i, 16:32, pl.ds(at, 128)].astype(F32)
            wsend[i, 2 * t] = jnp.where(left16, a, pltpu.roll(b, HEAD, 1)).astype(BF16)
            wsend[i, 2 * t + 1] = jnp.where(left16, pltpu.roll(a, HEAD, 1), b).astype(BF16)

        wb[gq * nm + i, c, z] = wsend[i, z]

    for cp in small_loads:
        cp.wait()
    weight = rweight[...]
    part = weight / jnp.sum(weight, -1, keepdims=True)
    ids = routes[...]
    lanes4 = lane_ids((ROWS, 128))
    by_expert = jnp.zeros((ROWS, 128), F32)
    for k in range(ids.shape[1]):
        by_expert += jnp.where(ids[:, k : k + 1] == lanes4, part[:, k : k + 1], 0.0)
    high = by_expert.astype(BF16).astype(F32)
    low = by_expert - high
    both = jnp.where(lanes4 < HEAD, high, pltpu.roll(low, HEAD, 1))
    sv[0, 0:ROWS, :] = both
    sv[0, ROWS : 2 * ROWS, :] = both
    csend[...] = sv[0].astype(BF16)
    my_slot = slot_of(z)
    cb[c, my_slot] = csend[...]

    side = 1 - 2 * (own_k % 2)
    hk = nk // 2

    def step_copy(buf, n, slot, sem, kt):
        at = buf.at[res, slot % nk]
        return pltpu.make_async_remote_copy(
            src_ref=at,
            dst_ref=at,
            send_sem=l1_send.at[n, sem],
            recv_sem=l1_recv.at[n, sem],
            device_id=chip((kt % nk) * STRIDE + res),
            device_id_type=MESH,
        )

    def near_copies(buf, n, slot):
        k = slot % nk
        at = buf.at[res, k]
        part = k // hk
        for i, to, sem in ((0, z + 1, 0), (1, z + nz - 1, 1), (2, z + nz + 2 - 4 * part, 2 + part)):
            pltpu.make_async_remote_copy(
                src_ref=at,
                dst_ref=at,
                send_sem=l2_send.at[n, i],
                recv_sem=l2_recv.at[n, sem],
                device_id=chip(to),
                device_id_type=MESH,
            ).start()

    direct = [(0, -1), (1, 1)] + ([(2, -2), (3, 2)] if nk > 4 else []) if nk > 2 else []
    direct += [(6, nk // 2)] if nk in (2, 4) else []
    onward = [(4, -3), (5, 3), (6, 4)] if nk == 8 else []

    def gather_start(buf, n):
        for sem, o in reversed(direct):
            step_copy(buf, n, own_k, sem, own_k + nk - o).start()
        near_copies(buf, n, own_k)

    def gather_direct(buf, n):
        for sem, o in direct:
            step_copy(buf, n, own_k + nk + o, sem, own_k).wait_recv()
            if sem == 2 and onward:
                step_copy(buf, n, own_k + nk - 2, 4, own_k + 1).start()
            if sem == 3 and onward:
                step_copy(buf, n, own_k + nk + 2, 5, own_k + nk - 1).start()
                step_copy(buf, n, own_k + nk - 2 * side, 6, own_k + nk + 2 * side).start()
            if sem < 2 or not onward:
                near_copies(buf, n, own_k + nk + o)
        if onward:
            near_copies(buf, n, own_k + nk - 2)
            near_copies(buf, n, own_k + nk + 2)

    def gather_onward(buf, n):
        for sem, o in onward:
            step_copy(buf, n, own_k + nk + o, sem, own_k).wait_recv()
            near_copies(buf, n, own_k + nk + o)

    def near_all(buf, n, i, sem, r, k0, count):
        at = buf.at[r, pl.ds(k0, count)]
        return pltpu.make_async_remote_copy(
            src_ref=at,
            dst_ref=at,
            send_sem=l2_send.at[n, i],
            recv_sem=l2_recv.at[n, sem],
            device_id=chip(z + 1),
            device_id_type=MESH,
        )

    def gather_wait(buf, n):
        near_all(buf, n, 0, 0, (res + STRIDE - 1) % STRIDE, 0, nk).wait_recv()
        near_all(buf, n, 1, 1, (res + 1) % STRIDE, 0, nk).wait_recv()
        near_all(buf, n, 2, 2, (res + 2) % STRIDE, 0, hk).wait_recv()
        near_all(buf, n, 2, 3, (res + 2) % STRIDE, hk, hk).wait_recv()

    def gather_drain(buf, n):
        for sem, _ in direct + onward:
            step_copy(buf, n, own_k, sem, own_k).wait_send()
        for i in range(3):
            near_all(buf, n, i, i, res, 0, nk).wait_send()

    def scatter(src_of, dst, send_sem, recv_sem):
        @pl.loop(0, nz - 1)
        def _(j):
            zt = far_first(j)
            pltpu.make_async_remote_copy(
                src_ref=src_of(zt),
                dst_ref=dst,
                send_sem=send_sem,
                recv_sem=recv_sem,
                device_id=chip(zt),
                device_id_type=MESH,
            ).start()

    def scatter_all(block, send_sem, recv_sem):
        return pltpu.make_async_remote_copy(
            src_ref=block.at[pl.ds(0, nz - 1)],
            dst_ref=block.at[pl.ds(0, nz - 1)],
            send_sem=send_sem,
            recv_sem=recv_sem,
            device_id=chip(z),
            device_id_type=MESH,
        )

    tokb = tok8[...].astype(BF16)

    def dot_t(a, b):
        return lax.dot_general(a, b, (((1,), (1,)), ((), ())), preferred_element_type=F32)

    squash = jnp.tanh(dot_t(tokb, dl1[...])).astype(BF16)
    lowl = dot_t(tokb, cl1[...]).astype(BF16)
    opened = jax.nn.sigmoid(dot(tokb, gl1[...])).astype(BF16)

    for j in range(nz // 2):
        cols = slice(128 * j, 128 * j + 128)

        def two_heads(ref, tile, j=j):
            ref[2 * j] = tile
            ref[2 * j + 1] = pltpu.roll(tile, HEAD, 1)

        pre = doff[:, cols] + dot(squash, dl2[:, cols])
        two_heads(dh, jnp.exp(-(jnp.exp(jnp.full((8, 128), -0.5, F32)) * jax.nn.sigmoid(pre))))
        two_heads(ah, jax.nn.sigmoid(coff[:, cols] + dot(lowl, cl2[:, cols])))
        two_heads(gh, dot(opened, gl2[:, cols]))

    pl.semaphore_wait(bar, nz - 1 + 1 + share - 1)

    for i in range(nm):
        m = gq * nm + i
        scatter(lambda zt, i=i: wsend.at[i, zt], wb.at[m, c, z], w_send.at[i], w_recv.at[i])
    gather_start(xt, 0)

    gather_direct(xt, 0)

    def slab(m, core, to, send_sem, recv_sem):
        return pltpu.make_async_remote_copy(
            src_ref=wb.at[m, core],
            dst_ref=wb.at[m, core],
            send_sem=send_sem,
            recv_sem=recv_sem,
            device_id=to,
            device_id_type=MESH,
        )

    for i in range(nm):
        m = gq * nm + i
        scatter_all(wb.at[m, c], w_send.at[i], w_recv.at[i]).wait_recv()
        for g in range(1, share):
            slab(
                m,
                c,
                {"grp": gbase + (gq + g) % share},
                q_send.at[g, i],
                q_recv.at[share - g, i],
            ).start()
        slab(m, c, sib, s_send.at[0, i], s_recv.at[0, i]).start()
    gather_onward(xt, 0)
    for g in range(1, share):
        for i in range(nm):
            m = ((gq + g) % share) * nm + i
            slab(m, c, sib, q_send.at[g, i], q_recv.at[g, i]).wait_recv()
            slab(m, c, sib, s_send.at[g, i], s_recv.at[g, i]).start()

    def widen(m, at):
        keep = left16.astype(F32).astype(BF16)
        drop = (1.0 - left16.astype(F32)).astype(BF16)
        for hk in range(2):

            @pl.loop(0, nz // 2)
            def _(zz, hk=hk):
                for core in range(2):
                    tile = wb[m, core, hk * (nz // 2) + zz]
                    base = pl.multiple_of(zz * 64 + core * 32, 32)
                    cols = slice(at + hk * 128, at + hk * 128 + 128)
                    em[pl.ds(base, 16), cols] = tile * keep
                    em[pl.ds(pl.multiple_of(base + 16, 16), 16), cols] = tile * drop

    def rows_of(value):
        return value.astype(F32).reshape(8 * nz, half).astype(BF16)

    top3 = row_ids((nz, 8, 128)) < ROWS
    left3 = lane_ids((nz, 8, 128)) < HEAD
    topw = (row_ids((8 * nz, 128)) % 8) < ROWS

    def fold(r):
        a = jnp.where(topw, r[:, 0:128], r[:, 128:256])
        a = (a + pltpu.roll(a, HEAD, 1)).reshape(nz, 8, 128)
        return a + pltpu.roll(a, ROWS, 1)

    for g in range(share):
        for i in range(nm):
            m = ((gq + g) % share) * nm + i
            slab(m, 1 - c, sib, s_send.at[g, i], s_recv.at[g, i]).wait_recv()

    for m in range(4):
        widen(m, m * 256)

    gather_wait(xt, 0)
    xv = rows_of(xt[...])
    cr = fold(dot(xv, em[:, 0:256]))
    ck = fold(dot(xv, em[:, 256:512]))
    cv = fold(dot(xv, em[:, 512:768]))
    ysend[...] = jnp.where(top3, jnp.where(left3, cr, ck), cv).astype(BF16)
    scatter(lambda zt: ysend.at[slot_of(zt)], yrecv.at[z], a_send.at[0], a_recv.at[0])
    yrecv[z] = ysend[my_slot]
    scatter(lambda zt: csend, cb.at[c, my_slot], a_send.at[2], a_recv.at[2])
    st_load.wait()
    scatter_all(yrecv, a_send.at[0], a_recv.at[0]).wait_recv()

    eye = (
        lax.broadcasted_iota(jnp.int32, (HEAD, HEAD), 0)
        == lax.broadcasted_iota(jnp.int32, (HEAD, HEAD), 1)
    ).astype(F32)

    def pick(ref, j):
        tile = jnp.broadcast_to(ref[:, 128 * j : 128 * j + 128], (8, 128))
        return tile, pltpu.roll(tile, HEAD, 1)

    blends = []
    for j in range(nz // 2):
        blends += pick(blend, j)
    for h in range(nz):
        bh[h] = blends[h]

    @pl.loop(0, nz // 2)
    def _(pair):
        for h in (2 * pair, 2 * pair + 1):
            y = yrecv[h].astype(F32)
            turned = pltpu.roll(y, ROWS, 0)
            rk = jnp.where(top, y, turned)
            v = jnp.where(top, turned, y)
            r = jnp.where(left, rk, 0.0)
            k = jnp.where(left, pltpu.roll(rk, HEAD, 1), 0.0)
            a = ah[h]
            unit = k * lax.rsqrt(jnp.sum(k * k, -1, keepdims=True) + 1e-06)
            written = k * (1.0 + (a - 1.0) * bh[h])
            ua = unit * a
            scale = sscale[pl.ds(h, 1), :]
            own = jnp.sum((r * written)[:, 0:HEAD] * scale, -1, keepdims=True)
            d = dh[h]
            sv[h] = own * v
            for t in range(ROWS):
                one = slice(t, t + 1)
                s = st[t, h]
                removed = jnp.sum(s * unit[one, 0:HEAD], -1, keepdims=True)
                vcol = jnp.sum(eye * v[one, 0:HEAD], -1, keepdims=True)
                n = s * d[one, 0:HEAD] - removed * ua[one, 0:HEAD] + vcol * written[one, 0:HEAD]
                sn[t, h] = n
                read = jnp.sum(n * r[one, 0:HEAD], -1, keepdims=True)
                row = jnp.sum(eye * read, 0, keepdims=True)
                ro[h, t : t + 1, 0:HEAD] = row
                ro[h, ROWS + t : ROWS + t + 1, 0:HEAD] = row

    st_store = pltpu.make_async_copy(sn, next_hbm, ld_sem.at[4])
    st_store.start()

    def mixer_head(h, gain, bias):
        x = jnp.where(left, ro[h], 0.0)
        mean = jnp.sum(x, -1, keepdims=True) * (1.0 / HEAD)
        dev = jnp.where(left, x - mean, 0.0)
        var = jnp.sum(dev * dev, -1, keepdims=True) * (1.0 / HEAD)
        normed = dev * lax.rsqrt(var + 0.00064) * gain + bias
        return (normed + sv[h]) * gh[h]

    def mixer_pair(j):
        g0, g1 = pick(hgain, j)
        b0, b1 = pick(hbias, j)
        one, two = mixer_head(2 * j, g0, b0), mixer_head(2 * j + 1, g1, b1)
        return jnp.where(left, one, pltpu.roll(two, HEAD, 1))

    for j in range(nz // 4):
        tile = jnp.where(top, mixer_pair(j), mixer_pair(nz // 4 + j))
        xm[res, own_k, :, 128 * j : 128 * j + 128] = tile.astype(BF16)

    gather_start(xm, 1)
    gather_direct(xm, 1)
    gather_onward(xm, 1)
    gather_wait(xm, 1)
    co = fold(dot(rows_of(xm[...]), em[:, 768:1024]))
    co_high = co.astype(BF16).astype(F32)
    msend[...] = jnp.where(top3, co_high, co - co_high).astype(BF16)
    scatter(lambda zt: msend.at[slot_of(zt)], mrecv.at[z], a_send.at[1], a_recv.at[1])
    mrecv[z] = msend[my_slot]

    scatter_all(cb.at[c], a_send.at[2], a_recv.at[2]).wait_recv()

    def to_sib(src, dst, n):
        return pltpu.make_async_remote_copy(
            src_ref=src,
            dst_ref=dst,
            send_sem=x_send.at[n],
            recv_sem=x_recv.at[n],
            device_id=sib,
            device_id_type=MESH,
        )

    to_sib(cb.at[c], cb.at[c], 0).start()

    scatter_all(mrecv, a_send.at[1], a_recv.at[1]).wait_recv()
    for j in range(nz // 4):

        def mixed_pair(p):
            one, two = mrecv[2 * p].astype(F32), mrecv[2 * p + 1].astype(F32)
            tile = jnp.where(left, one, two)
            return tile + pltpu.roll(tile, ROWS, 0)

        cols = slice(128 * j, 128 * j + 128)
        tokp[:, cols] += jnp.where(top, mixed_pair(j), mixed_pair(nz // 4 + j))

    topp = row_ids((8, half)) < ROWS

    def packed(ref):
        return jnp.where(topp, ref[:, 0:half], ref[:, half:dim])

    def row_total(x):
        s = jnp.broadcast_to(jnp.sum(x, -1, keepdims=True), (8, 128))
        s = s + pltpu.roll(s, ROWS, 0)
        return s[:, 0:1] * (1.0 / dim)

    def layer_norm(x, gain, bias):
        dev = x - row_total(x)
        var = row_total(dev * dev)
        return dev * lax.rsqrt(var + 1e-05) * packed(gain) + packed(bias)

    hidden = layer_norm(tokp[...], mgain, mbias).astype(BF16)
    hidp[...] = hidden.astype(F32)
    xh[c, res, own_k] = hidden
    mine = xh.at[c]
    gather_start(mine, 2)
    gather_direct(mine, 2)
    gather_onward(mine, 2)
    gather_wait(mine, 2)
    to_sib(xh.at[c], xh.at[c], 1).start()

    eg_load.wait()
    eu_load.wait()
    ed_load.wait()
    to_sib(cb.at[1 - c], cb.at[1 - c], 0).wait_recv()

    def wide_fold(a, b):
        width = a.shape[1]
        keep = (row_ids((8 * nz, width)) % 8) < ROWS
        x = jnp.where(keep, a, b).reshape(nz, 8, width)
        return (x + pltpu.roll(x, ROWS, 1)).reshape(8 * nz, width)

    def expert(core):
        xv = rows_of(xh[core])
        lane3 = lane_ids((nz, 8, 128))
        hit = (lane3 == ep) | (lane3 == ep + HEAD)
        coef = jnp.sum(jnp.where(hit, cb[core].astype(F32), 0.0), -1, keepdims=True)
        coef = coef.reshape(8 * nz, 1)
        gate = wide_fold(dot(xv, eg[0:half, :]), dot(xv, eg[half:dim, :]))
        up = wide_fold(dot(xv, eu[0:half, :]), dot(xv, eu[half:dim, :]))
        inner = (gate * jax.nn.sigmoid(gate) * up).astype(BF16)
        return inner, coef

    def down(inner, coef, j, width):
        a = dot(inner, ed[:, j * width : (j + 1) * width])
        b = dot(inner, ed[:, half + j * width : half + (j + 1) * width])
        keep = (row_ids((8 * nz, width)) % 8) < ROWS
        return (jnp.where(keep, a, b) * coef).reshape(STRIDE, nk, 8, width)

    width = min(256, half)
    inner, coef = expert(c)
    for j in range(half // width):
        zown[:, :, :, j * width : (j + 1) * width] = down(inner, coef, j, width).astype(BF16)
    to_sib(xh.at[1 - c], xh.at[1 - c], 1).wait_recv()
    inner, coef = expert(1 - c)
    for j in range(half // width):
        zoth[:, :, :, j * width : (j + 1) * width] = down(inner, coef, j, width).astype(BF16)
    to_sib(zoth, zsib, 2).start()
    to_sib(zoth, zsib, 2).wait_recv()
    tsum[...] = (zown[...].astype(F32) + zsib[...].astype(F32)).astype(BF16)

    def near_sum(slot):
        k = slot % nk
        part = k // hk
        up, down_, far = (res + 1) % STRIDE, (res + STRIDE - 1) % STRIDE, (res + 2) % STRIDE
        return [
            pltpu.make_async_remote_copy(
                src_ref=tsum.at[r, k],
                dst_ref=r1.at[i, k],
                send_sem=f1_send.at[i],
                recv_sem=f1_recv.at[i, k],
                device_id=chip(to),
                device_id_type=MESH,
            )
            for i, (to, r) in enumerate(
                ((z + 1, up), (z + nz - 1, down_), (z + nz + 2 - 4 * part, far))
            )
        ]

    def step_sum(kt, src, sem):
        return pltpu.make_async_remote_copy(
            src_ref=u2.at[src],
            dst_ref=r2.at[sem],
            send_sem=f2_send.at[sem],
            recv_sem=f2_recv.at[sem],
            device_id=chip((kt % nk) * STRIDE + res),
            device_id_type=MESH,
        )

    def near_total(slot):
        k = slot % nk
        for cp in near_sum(k):
            cp.wait_recv()
        return (
            tsum[res, k].astype(F32)
            + r1[0, k].astype(F32)
            + r1[1, k].astype(F32)
            + r1[2, k].astype(F32)
        )

    def arrived(sem):
        step_sum(own_k, 0, sem).wait_recv()
        return r2[sem].astype(F32)

    if nk == 8:
        order = [nk + 4, nk - 3, nk + 3, nk - 2 * side, nk + 2 * side, nk - 1, nk + 1, nk]
    else:
        order = [nk // 2] + ([1, nk - 1] if nk == 4 else []) + [nk]
    for o in order:
        for cp in near_sum(own_k + o):
            cp.start()
    if nk == 8:
        u2[0] = near_total(own_k + 4).astype(BF16)
        step_sum(own_k + nk + 2 * side * -1, 0, 0).start()
        u2[1] = near_total(own_k + nk - 3 * side).astype(BF16)
        step_sum(own_k + nk - side, 1, 1).start()
        u2[2] = near_total(own_k + nk + 3 * side).astype(BF16)
        step_sum(own_k + nk + side, 2, 2).start()
        u2[3] = near_total(own_k + nk - side).astype(BF16)
        step_sum(own_k + nk - side, 3, 3).start()
        u2[4] = near_total(own_k + nk + side).astype(BF16)
        step_sum(own_k + nk + side, 4, 4).start()
        part_b = near_total(own_k + nk + 2 * side)
        part_a = near_total(own_k + nk - 2 * side)
        u2[6] = (part_b + arrived(1)).astype(BF16)
        step_sum(own_k + nk + 2 * side, 6, 6).start()
        u2[5] = (part_a + arrived(2) + arrived(0)).astype(BF16)
        step_sum(own_k + nk - 2 * side, 5, 5).start()
        total = near_total(own_k)
        used = range(7)
    else:
        for i, o in enumerate(order[:-1]):
            u2[i] = near_total(own_k + o).astype(BF16)
            step_sum(own_k + o, i, i).start()
        total = near_total(own_k)
        used = range(len(order) - 1)
    total = total + hidp[...]
    for sem in used:
        if nk != 8 or sem >= 3:
            total = total + arrived(sem)
    y = layer_norm(total, egain, ebias)
    out_ref[:, 0:half] = y[0:ROWS, :].astype(BF16)
    out_ref[:, half:dim] = y[ROWS : 2 * ROWS, :].astype(BF16)

    gather_drain(xt, 0)
    gather_drain(xm, 1)
    gather_drain(mine, 2)
    for i in range(nm):
        scatter_all(wb.at[gq * nm + i, c], w_send.at[i], w_recv.at[i]).wait_send()
        slab(gq * nm + i, c, sib, s_send.at[0, i], s_recv.at[0, i]).wait_send()
        for g in range(1, share):
            slab(gq * nm + i, c, sib, q_send.at[g, i], q_recv.at[g, i]).wait_send()
            m = ((gq + g) % share) * nm + i
            slab(m, c, sib, s_send.at[g, i], s_recv.at[g, i]).wait_send()
    scatter_all(yrecv, a_send.at[0], a_recv.at[0]).wait_send()
    scatter_all(mrecv, a_send.at[1], a_recv.at[1]).wait_send()
    scatter_all(cb.at[c], a_send.at[2], a_recv.at[2]).wait_send()
    to_sib(cb.at[c], cb.at[c], 0).wait_send()
    to_sib(xh.at[c], xh.at[c], 1).wait_send()
    to_sib(zoth, zsib, 2).wait_send()
    for i in range(3):
        pltpu.make_async_remote_copy(
            src_ref=tsum.at[res],
            dst_ref=r1.at[i],
            send_sem=f1_send.at[i],
            recv_sem=f1_recv.at[i, 0],
            device_id=chip(z + 1),
            device_id_type=MESH,
        ).wait_send()
    for sem in used:
        step_sum(own_k, sem, sem).wait_send()
    st_store.wait()


def step(nz, share, *args):
    tokens, state = args[0], args[1]
    dim = tokens.shape[1]
    half = dim // 2
    nk = nz // STRIDE
    nm = 4 // share
    ff = args[24].shape[2]
    args = list(args)
    args[5], args[8] = args[5].T, args[8].T
    for i in (7, 10, 13, 15, 16, 18, 19, 20, 21):
        args[i] = args[i].reshape(1, dim)
    small = [5, 6, 7, 8, 9, 10, 11, 12, 13, 14, 15, 16, 18, 19, 20, 21, 22, 23]
    operands = [args[i] for i in [0, 1, 2, 3, 4, 17] + small + [24, 25, 26]]
    vmem = pl.BlockSpec(memory_space=pltpu.VMEM)
    hbm = pl.BlockSpec(memory_space=pl.ANY)
    dma = pltpu.SemaphoreType.DMA
    heads = (nz, 8, 128)
    rows = (STRIDE, nk, 8, half)
    scratch = [
        pltpu.VMEM(tokens.shape, BF16),
        *[pltpu.VMEM(args[i].shape, args[i].dtype) for i in small],
        pltpu.VMEM(state.shape, F32),
        pltpu.VMEM(state.shape, F32),
        pltpu.VMEM((nm, 32, dim), BF16),
        pltpu.VMEM((nm, nz, 16, 128), BF16),
        pltpu.VMEM((4, 2, nz, 16, 128), BF16),
        pltpu.VMEM((half, 1024), BF16),
        pltpu.VMEM(rows, BF16),
        pltpu.VMEM(rows, BF16),
        pltpu.VMEM((2,) + rows, BF16),
        pltpu.VMEM(heads, BF16),
        pltpu.VMEM(heads, BF16),
        pltpu.VMEM(heads, BF16),
        pltpu.VMEM(heads, BF16),
        pltpu.VMEM((2,) + heads, BF16),
        pltpu.VMEM((8, 128), BF16),
        pltpu.VMEM((8, dim), F32),
        pltpu.VMEM((8, half), F32),
        pltpu.VMEM((8, half), F32),
        pltpu.VMEM(heads, F32),
        pltpu.VMEM(heads, F32),
        pltpu.VMEM(heads, F32),
        pltpu.VMEM(heads, F32),
        pltpu.VMEM(heads, F32),
        pltpu.VMEM(heads, F32),
        pltpu.VMEM((dim, ff), BF16),
        pltpu.VMEM((dim, ff), BF16),
        pltpu.VMEM((ff, dim), BF16),
        pltpu.VMEM(rows, BF16),
        pltpu.VMEM(rows, BF16),
        pltpu.VMEM(rows, BF16),
        pltpu.VMEM(rows, BF16),
        pltpu.VMEM((3, nk, 8, half), BF16),
        pltpu.VMEM((nk, 8, half), BF16),
        pltpu.VMEM((nk, 8, half), BF16),
        dma((9,)),
        dma((nm,)),
        dma((nm,)),
        dma((share, nm)),
        dma((share, nm)),
        dma((share, nm)),
        dma((share, nm)),
        dma((3, 7)),
        dma((3, 7)),
        dma((3, 3)),
        dma((3, 4)),
        dma((3,)),
        dma((3,)),
        dma((3,)),
        dma((3,)),
        dma((3,)),
        dma((3, nk)),
        dma((7,)),
        dma((7,)),
        dma((SMALL,)),
    ]
    return pl.pallas_call(
        functools.partial(kernel, nz, share),
        out_shape=(
            jax.ShapeDtypeStruct(tokens.shape, BF16),
            jax.ShapeDtypeStruct(state.shape, F32),
        ),
        in_specs=[hbm] * len(operands),
        out_specs=(vmem, hbm),
        scratch_shapes=scratch,
        compiler_params=pltpu.CompilerParams(
            collective_id=0, has_side_effects=True, vmem_limit_bytes=56 * 1024 * 1024
        ),
    )(*operands)


def solution(mesh):
    nz = mesh.shape["ep"] // 2
    groups = mesh.shape["grp"]
    share = 4 if groups % 4 == 0 else 2 if groups % 2 == 0 else 1
    owned, split, copied = P(("grp", "ep"), None), P("ep", None), P()
    in_specs = (
        owned,
        P(("grp", "ep"), None, None, None),
        split,
        split,
        split,
        *([copied] * 12),
        split,
        *([copied] * 4),
        owned,
        owned,
        P("ep", None, None),
        P("ep", None, None),
        P("ep", None, None),
    )
    out_specs = (owned, P(("grp", "ep"), None, None, None))
    return jax.shard_map(
        functools.partial(step, nz, share),
        mesh=mesh,
        in_specs=in_specs,
        out_specs=out_specs,
        check_vma=False,
    )
```

```python
import functools

import jax
import jax.numpy as jnp
from jax import lax
from jax.experimental import pallas as pl
from jax.experimental.pallas import tpu as pltpu
from jax.sharding import PartitionSpec as P

MESH = pl.DeviceIdType.MESH
F32 = jnp.float32
BF16 = jnp.bfloat16
SMALL = 18
ROWS = 4
HEAD = 64
STRIDE = 4


def dot(a, b):
    return jnp.dot(a, b, preferred_element_type=F32)


def lane_ids(shape):
    return lax.broadcasted_iota(jnp.int32, shape, len(shape) - 1)


def row_ids(shape):
    return lax.broadcasted_iota(jnp.int32, shape, len(shape) - 2)


def kernel(
    nz,
    share,
    tok_hbm,
    state_hbm,
    wr_hbm,
    wk_hbm,
    wv_hbm,
    wo_hbm,
    *rest,
):
    small_hbm, rest = rest[:SMALL], rest[SMALL:]
    run(nz, share, tok_hbm, state_hbm, (wr_hbm, wk_hbm, wv_hbm, wo_hbm), small_hbm, *rest)


def run(
    nz,
    share,
    tok_hbm,
    state_hbm,
    w_hbm,
    small_hbm,
    eg_hbm,
    eu_hbm,
    ed_hbm,
    out_ref,
    next_hbm,
    tok_ref,
    *rest,
):
    small, rest = rest[:SMALL], rest[SMALL:]
    work(nz, share, tok_hbm, state_hbm, w_hbm, small_hbm, eg_hbm, eu_hbm, ed_hbm,
         out_ref, next_hbm, tok_ref, small, *rest)


def work(
    nz,
    share,
    tok_hbm,
    state_hbm,
    w_hbm,
    small_hbm,
    eg_hbm,
    eu_hbm,
    ed_hbm,
    out_ref,
    next_hbm,
    tok_ref,
    small,
    st,
    sn,
    wstage,
    wsend,
    wb,
    em,
    xt,
    xm,
    xg,
    x2,
    hid,
    ysend,
    yrecv,
    cb,
    csend,
    tok8,
    tokp,
    hidp,
    dh,
    ah,
    gh,
    ro,
    sv,
    bh,
    eg,
    eu,
    ed,
    zown,
    zoth,
    zsib,
    tsum,
    r1,
    u2,
    r2,
    ld_sem,
    w_send,
    w_recv,
    q_send,
    q_recv,
    s_send,
    s_recv,
    l1_send,
    l1_recv,
    l2_send,
    l2_recv,
    a_send,
    a_recv,
    x_send,
    x_recv,
    f1_send,
    f1_recv,
    f2_send,
    f2_recv,
    small_sem,
):
    (
        dl1, dl2, doff, cl1, cl2, coff, gl1, gl2, blend,
        sscale, hgain, hbias, mgain, mbias, egain, ebias, routes, rweight,
    ) = small
    nk = nz // STRIDE
    dim = HEAD * nz
    half = dim // 2
    nm = 4 // share
    ep = lax.axis_index("ep")
    grp = lax.axis_index("grp")
    z = ep // 2
    c = ep % 2
    gq = grp % share
    gbase = grp - gq
    res = z % STRIDE
    own_k = z // STRIDE
    sib = {"ep": z * 2 + 1 - c}

    def chip(zt):
        return {"ep": (zt % nz) * 2 + c}

    def slot_of(zt):
        return (zt % STRIDE) * nk + zt // STRIDE

    def far_first(j):
        d = nz // 2 - (j + 1) // 2
        return (z + nz + d * (1 - 2 * (j % 2))) % nz

    bar = pltpu.get_barrier_semaphore()

    @pl.loop(1, nz)
    def _(j):
        pl.semaphore_signal(bar, inc=1, device_id=chip(z + j), device_id_type=MESH)

    pl.semaphore_signal(bar, inc=1, device_id=sib, device_id_type=MESH)
    for i in range(1, share):
        pl.semaphore_signal(
            bar, inc=1, device_id={"grp": gbase + (gq + i) % share}, device_id_type=MESH
        )

    tok_load = pltpu.make_async_copy(tok_hbm, tok_ref, ld_sem.at[8])
    tok_load.start()
    for i in range(nm):
        for m in range(4):
            if m % nm == i:

                @pl.when(gq == m // nm)
                def _(i=i, m=m):
                    pltpu.make_async_copy(w_hbm[m], wstage.at[i], ld_sem.at[i]).start()

    st_load = pltpu.make_async_copy(state_hbm, st, ld_sem.at[4])
    eg_load = pltpu.make_async_copy(eg_hbm.at[0], eg, ld_sem.at[5])
    eu_load = pltpu.make_async_copy(eu_hbm.at[0], eu, ld_sem.at[6])
    ed_load = pltpu.make_async_copy(ed_hbm.at[0], ed, ld_sem.at[7])
    small_loads = [
        pltpu.make_async_copy(a, b, small_sem.at[i])
        for i, (a, b) in enumerate(zip(small_hbm, small))
    ]
    for cp in small_loads:
        cp.start()
    st_load.start()
    eg_load.start()
    eu_load.start()
    ed_load.start()

    lane128 = lane_ids((8, 128))
    left = lane128 < HEAD
    top = row_ids((8, 128)) < ROWS
    lane16 = lane_ids((16, 128))
    left16 = lane16 < HEAD

    tok_load.wait()
    tok = tok_ref[...].astype(F32)
    tok8[0:ROWS, :] = tok
    tok8[ROWS : 2 * ROWS, :] = tok
    tokp[0:ROWS, :] = tok[:, :half]
    tokp[ROWS : 2 * ROWS, :] = tok[:, half:]
    xt[res, own_k] = tokp[...].astype(BF16)

    for i in range(nm):
        pltpu.make_async_copy(w_hbm[0], wstage.at[i], ld_sem.at[i]).wait()

        @pl.loop(0, nz // 2)
        def _(t, i=i):
            at = pl.multiple_of(t * 128, 128)
            a = wstage[i, 0:16, pl.ds(at, 128)].astype(F32)
            b = wstage[i, 16:32, pl.ds(at, 128)].astype(F32)
            wsend[i, 2 * t] = jnp.where(left16, a, pltpu.roll(b, HEAD, 1)).astype(BF16)
            wsend[i, 2 * t + 1] = jnp.where(left16, pltpu.roll(a, HEAD, 1), b).astype(BF16)

        wb[gq * nm + i, c, z] = wsend[i, z]

    for cp in small_loads:
        cp.wait()
    weight = rweight[...]
    part = weight / jnp.sum(weight, -1, keepdims=True)
    ids = routes[...]
    lanes4 = lane_ids((ROWS, 128))
    by_expert = jnp.zeros((ROWS, 128), F32)
    for k in range(ids.shape[1]):
        by_expert += jnp.where(ids[:, k : k + 1] == lanes4, part[:, k : k + 1], 0.0)
    high = by_expert.astype(BF16).astype(F32)
    low = by_expert - high
    both = jnp.where(lanes4 < HEAD, high, pltpu.roll(low, HEAD, 1))
    sv[0, 0:ROWS, :] = both
    sv[0, ROWS : 2 * ROWS, :] = both
    csend[...] = sv[0].astype(BF16)
    my_slot = slot_of(z)
    cb[c, my_slot] = csend[...]

    side = 1 - 2 * (own_k % 2)
    hk = nk // 2

    def step_copy(buf, n, slot, sem, kt):
        at = buf.at[res, slot % nk]
        return pltpu.make_async_remote_copy(
            src_ref=at,
            dst_ref=at,
            send_sem=l1_send.at[n, sem],
            recv_sem=l1_recv.at[n, sem],
            device_id=chip((kt % nk) * STRIDE + res),
            device_id_type=MESH,
        )

    def near_copies(buf, n, slot):
        k = slot % nk
        at = buf.at[res, k]
        part = k // hk
        for i, to, sem in ((0, z + 1, 0), (1, z + nz - 1, 1), (2, z + nz + 2 - 4 * part, 2 + part)):
            pltpu.make_async_remote_copy(
                src_ref=at,
                dst_ref=at,
                send_sem=l2_send.at[n, i],
                recv_sem=l2_recv.at[n, sem],
                device_id=chip(to),
                device_id_type=MESH,
            ).start()

    direct = [(0, -1), (1, 1)] + ([(2, -2), (3, 2)] if nk > 4 else []) if nk > 2 else []
    direct += [(6, nk // 2)] if nk in (2, 4) else []
    onward = [(4, -3), (5, 3), (6, 4)] if nk == 8 else []

    def gather_start(buf, n):
        for sem, o in reversed(direct):
            step_copy(buf, n, own_k, sem, own_k + nk - o).start()
        near_copies(buf, n, own_k)

    def gather_direct(buf, n):
        for sem, o in direct:
            step_copy(buf, n, own_k + nk + o, sem, own_k).wait_recv()
            if sem == 2 and onward:
                step_copy(buf, n, own_k + nk - 2, 4, own_k + 1).start()
            if sem == 3 and onward:
                step_copy(buf, n, own_k + nk + 2, 5, own_k + nk - 1).start()
                step_copy(buf, n, own_k + nk - 2 * side, 6, own_k + nk + 2 * side).start()
            if sem < 2 or not onward:
                near_copies(buf, n, own_k + nk + o)
        if onward:
            near_copies(buf, n, own_k + nk - 2)
            near_copies(buf, n, own_k + nk + 2)

    def gather_onward(buf, n):
        for sem, o in onward:
            step_copy(buf, n, own_k + nk + o, sem, own_k).wait_recv()
            near_copies(buf, n, own_k + nk + o)

    def near_all(buf, n, i, sem, r, k0, count):
        at = buf.at[r, pl.ds(k0, count)]
        return pltpu.make_async_remote_copy(
            src_ref=at,
            dst_ref=at,
            send_sem=l2_send.at[n, i],
            recv_sem=l2_recv.at[n, sem],
            device_id=chip(z + 1),
            device_id_type=MESH,
        )

    def gather_wait(buf, n):
        near_all(buf, n, 0, 0, (res + STRIDE - 1) % STRIDE, 0, nk).wait_recv()
        near_all(buf, n, 1, 1, (res + 1) % STRIDE, 0, nk).wait_recv()
        near_all(buf, n, 2, 2, (res + 2) % STRIDE, 0, hk).wait_recv()
        near_all(buf, n, 2, 3, (res + 2) % STRIDE, hk, hk).wait_recv()

    def gather_drain(buf, n):
        for sem, _ in direct + onward:
            step_copy(buf, n, own_k, sem, own_k).wait_send()
        for i in range(3):
            near_all(buf, n, i, i, res, 0, nk).wait_send()

    def scatter(src_of, dst, send_sem, recv_sem):
        @pl.loop(0, nz - 1)
        def _(j):
            zt = far_first(j)
            pltpu.make_async_remote_copy(
                src_ref=src_of(zt),
                dst_ref=dst,
                send_sem=send_sem,
                recv_sem=recv_sem,
                device_id=chip(zt),
                device_id_type=MESH,
            ).start()

    def scatter_all(block, send_sem, recv_sem):
        return pltpu.make_async_remote_copy(
            src_ref=block.at[pl.ds(0, nz - 1)],
            dst_ref=block.at[pl.ds(0, nz - 1)],
            send_sem=send_sem,
            recv_sem=recv_sem,
            device_id=chip(z),
            device_id_type=MESH,
        )

    tokb = tok8[...].astype(BF16)

    def dot_t(a, b):
        return lax.dot_general(a, b, (((1,), (1,)), ((), ())), preferred_element_type=F32)

    squash = jnp.tanh(dot_t(tokb, dl1[...])).astype(BF16)
    lowl = dot_t(tokb, cl1[...]).astype(BF16)
    opened = jax.nn.sigmoid(dot(tokb, gl1[...])).astype(BF16)

    for j in range(nz // 2):
        cols = slice(128 * j, 128 * j + 128)

        def two_heads(ref, tile, j=j):
            ref[2 * j] = tile
            ref[2 * j + 1] = pltpu.roll(tile, HEAD, 1)

        pre = doff[:, cols] + dot(squash, dl2[:, cols])
        two_heads(dh, jnp.exp(-(jnp.exp(jnp.full((8, 128), -0.5, F32)) * jax.nn.sigmoid(pre))))
        two_heads(ah, jax.nn.sigmoid(coff[:, cols] + dot(lowl, cl2[:, cols])))
        two_heads(gh, dot(opened, gl2[:, cols]))

    pl.semaphore_wait(bar, nz - 1 + 1 + share - 1)

    for i in range(nm):
        m = gq * nm + i
        scatter(lambda zt, i=i: wsend.at[i, zt], wb.at[m, c, z], w_send.at[i], w_recv.at[i])
    gather_start(xt, 0)

    gather_direct(xt, 0)

    def slab(m, core, to, send_sem, recv_sem):
        return pltpu.make_async_remote_copy(
            src_ref=wb.at[m, core],
            dst_ref=wb.at[m, core],
            send_sem=send_sem,
            recv_sem=recv_sem,
            device_id=to,
            device_id_type=MESH,
        )

    for i in range(nm):
        m = gq * nm + i
        scatter_all(wb.at[m, c], w_send.at[i], w_recv.at[i]).wait_recv()
        for g in range(1, share):
            slab(
                m,
                c,
                {"grp": gbase + (gq + g) % share},
                q_send.at[g, i],
                q_recv.at[share - g, i],
            ).start()
        slab(m, c, sib, s_send.at[0, i], s_recv.at[0, i]).start()
    gather_onward(xt, 0)
    for g in range(1, share):
        for i in range(nm):
            m = ((gq + g) % share) * nm + i
            slab(m, c, sib, q_send.at[g, i], q_recv.at[g, i]).wait_recv()
            slab(m, c, sib, s_send.at[g, i], s_recv.at[g, i]).start()

    def widen(m, at):
        keep = left16.astype(F32).astype(BF16)
        drop = (1.0 - left16.astype(F32)).astype(BF16)
        for hk in range(2):

            @pl.loop(0, nz // 2)
            def _(zz, hk=hk):
                for core in range(2):
                    tile = wb[m, core, hk * (nz // 2) + zz]
                    base = pl.multiple_of(zz * 64 + core * 32, 32)
                    cols = slice(at + hk * 128, at + hk * 128 + 128)
                    em[pl.ds(base, 16), cols] = tile * keep
                    em[pl.ds(pl.multiple_of(base + 16, 16), 16), cols] = tile * drop

    def rows_of(value):
        return value.astype(F32).reshape(8 * nz, half).astype(BF16)

    top3 = row_ids((nz, 8, 128)) < ROWS
    left3 = lane_ids((nz, 8, 128)) < HEAD
    topw = (row_ids((8 * nz, 128)) % 8) < ROWS

    def fold(r):
        a = jnp.where(topw, r[:, 0:128], r[:, 128:256])
        a = (a + pltpu.roll(a, HEAD, 1)).reshape(nz, 8, 128)
        return a + pltpu.roll(a, ROWS, 1)

    for g in range(share):
        for i in range(nm):
            m = ((gq + g) % share) * nm + i
            slab(m, 1 - c, sib, s_send.at[g, i], s_recv.at[g, i]).wait_recv()

    for m in range(4):
        widen(m, m * 256)

    gather_wait(xt, 0)
    xv = rows_of(xt[...])
    cr = fold(dot(xv, em[:, 0:256]))
    ck = fold(dot(xv, em[:, 256:512]))
    cv = fold(dot(xv, em[:, 512:768]))
    ysend[...] = jnp.where(top3, jnp.where(left3, cr, ck), cv).astype(BF16)
    scatter(lambda zt: ysend.at[slot_of(zt)], yrecv.at[z], a_send.at[0], a_recv.at[0])
    yrecv[z] = ysend[my_slot]
    scatter(lambda zt: csend, cb.at[c, my_slot], a_send.at[2], a_recv.at[2])
    topk = row_ids((nk, 8, 128)) < ROWS
    leftk = lane_ids((nk, 8, 128)) < HEAD
    for s in range(2):
        for m in range(half // 128):
            one = xt[2 * s, :, :, 128 * m : 128 * m + 128].astype(F32)
            two = xt[2 * s + 1, :, :, 128 * m : 128 * m + 128].astype(F32)
            x2[s, :, :, 128 * m : 128 * m + 128] = jnp.where(topk, one, pltpu.roll(two, ROWS, 1))
            x2[s, :, :, half + 128 * m : half + 128 * m + 128] = jnp.where(
                topk, pltpu.roll(one, ROWS, 1), two
            )
    st_load.wait()
    scatter_all(yrecv, a_send.at[0], a_recv.at[0]).wait_recv()

    eye = (
        lax.broadcasted_iota(jnp.int32, (HEAD, HEAD), 0)
        == lax.broadcasted_iota(jnp.int32, (HEAD, HEAD), 1)
    ).astype(F32)

    def pick(ref, j):
        tile = jnp.broadcast_to(ref[:, 128 * j : 128 * j + 128], (8, 128))
        return tile, pltpu.roll(tile, HEAD, 1)

    blends = []
    for j in range(nz // 2):
        blends += pick(blend, j)
    for h in range(nz):
        bh[h] = blends[h]

    @pl.loop(0, nz // 2)
    def _(pair):
        for h in (2 * pair, 2 * pair + 1):
            y = yrecv[h].astype(F32)
            turned = pltpu.roll(y, ROWS, 0)
            rk = jnp.where(top, y, turned)
            v = jnp.where(top, turned, y)
            r = jnp.where(left, rk, 0.0)
            k = jnp.where(left, pltpu.roll(rk, HEAD, 1), 0.0)
            a = ah[h]
            unit = k * lax.rsqrt(jnp.sum(k * k, -1, keepdims=True) + 1e-06)
            written = k * (1.0 + (a - 1.0) * bh[h])
            ua = unit * a
            scale = sscale[pl.ds(h, 1), :]
            own = jnp.sum((r * written)[:, 0:HEAD] * scale, -1, keepdims=True)
            d = dh[h]
            sv[h] = own * v
            for t in range(ROWS):
                one = slice(t, t + 1)
                s = st[t, h]
                removed = jnp.sum(s * unit[one, 0:HEAD], -1, keepdims=True)
                vcol = jnp.sum(eye * v[one, 0:HEAD], -1, keepdims=True)
                n = s * d[one, 0:HEAD] - removed * ua[one, 0:HEAD] + vcol * written[one, 0:HEAD]
                sn[t, h] = n
                read = jnp.sum(n * r[one, 0:HEAD], -1, keepdims=True)
                row = jnp.sum(eye * read, 0, keepdims=True)
                ro[h, t : t + 1, 0:HEAD] = row
                ro[h, ROWS + t : ROWS + t + 1, 0:HEAD] = row

    st_store = pltpu.make_async_copy(sn, next_hbm, ld_sem.at[4])
    st_store.start()

    def mixer_head(h, gain, bias):
        x = jnp.where(left, ro[h], 0.0)
        mean = jnp.sum(x, -1, keepdims=True) * (1.0 / HEAD)
        dev = jnp.where(left, x - mean, 0.0)
        var = jnp.sum(dev * dev, -1, keepdims=True) * (1.0 / HEAD)
        normed = dev * lax.rsqrt(var + 0.00064) * gain + bias
        return (normed + sv[h]) * gh[h]

    def mixer_pair(j):
        g0, g1 = pick(hgain, j)
        b0, b1 = pick(hbias, j)
        one, two = mixer_head(2 * j, g0, b0), mixer_head(2 * j + 1, g1, b1)
        return jnp.where(left, one, pltpu.roll(two, HEAD, 1))

    for j in range(nz // 4):
        tile = jnp.where(top, mixer_pair(j), mixer_pair(nz // 4 + j))
        xm[res, own_k, :, 128 * j : 128 * j + 128] = tile.astype(BF16)

    gather_start(xm, 1)
    gather_direct(xm, 1)
    gather_onward(xm, 1)
    gather_wait(xm, 1)
    co = fold(dot(rows_of(xm[...]), em[:, 768:1024]))
    xg[res, own_k] = jnp.where(
        leftk,
        jnp.where(topk, co[0:nk], co[nk : 2 * nk]),
        jnp.where(topk, co[2 * nk : 3 * nk], co[3 * nk :]),
    ).astype(BF16)
    gather_start(xg, 2)

    scatter_all(cb.at[c], a_send.at[2], a_recv.at[2]).wait_recv()

    def to_sib(src, dst, n):
        return pltpu.make_async_remote_copy(
            src_ref=src,
            dst_ref=dst,
            send_sem=x_send.at[n],
            recv_sem=x_recv.at[n],
            device_id=sib,
            device_id_type=MESH,
        )

    to_sib(cb.at[c], cb.at[c], 0).start()

    gather_direct(xg, 2)
    gather_onward(xg, 2)
    gather_wait(xg, 2)
    for j in range(nz // 2):
        cols = slice(128 * j, 128 * j + 128)
        one = xg[2 * j % STRIDE, 2 * j // STRIDE].astype(F32)
        two = xg[(2 * j + 1) % STRIDE, (2 * j + 1) // STRIDE].astype(F32)
        x2[0, :, :, cols] += jnp.where(leftk, one, pltpu.roll(two, HEAD, 2))
        x2[1, :, :, cols] += jnp.where(leftk, pltpu.roll(one, HEAD, 2), two)

    some = max(1, nk // 2)
    for s in range(2):
        for k in range(0, nk, some):
            x = x2[s, k : k + some]
            dev = x - jnp.mean(x, -1, keepdims=True)
            var = jnp.mean(dev * dev, -1, keepdims=True)
            y = dev * lax.rsqrt(var + 1e-05) * mgain[...] + mbias[...]
            x2[s, k : k + some] = y
            base = 8 * (s * nk + k)
            hid[c, base : base + 8 * some, :] = y.reshape(8 * some, dim).astype(BF16)

    to_sib(hid.at[c], hid.at[c], 1).start()

    topp = row_ids((8, half)) < ROWS

    def packed(ref):
        return jnp.where(topp, ref[:, 0:half], ref[:, half:dim])

    def row_total(x):
        s = jnp.broadcast_to(jnp.sum(x, -1, keepdims=True), (8, 128))
        s = s + pltpu.roll(s, ROWS, 0)
        return s[:, 0:1] * (1.0 / dim)

    def layer_norm(x, gain, bias):
        dev = x - row_total(x)
        var = row_total(dev * dev)
        return dev * lax.rsqrt(var + 1e-05) * packed(gain) + packed(bias)

    two_rows = x2[res // 2, own_k].astype(BF16).astype(F32)
    mine = row_ids((8, dim)) // ROWS == res % 2
    doubled = jnp.where(mine, two_rows, pltpu.roll(two_rows, ROWS, 0))
    hidp[...] = jnp.where(topp, doubled[:, 0:half], doubled[:, half:dim])

    eg_load.wait()
    eu_load.wait()
    ed_load.wait()
    to_sib(cb.at[1 - c], cb.at[1 - c], 0).wait_recv()

    def expert(core):
        xv = hid[core]
        lane3 = lane_ids((nz, 8, 128))
        hit = (lane3 == ep) | (lane3 == ep + HEAD)
        coef = jnp.sum(jnp.where(hit, cb[core].astype(F32), 0.0), -1, keepdims=True)
        top1 = row_ids((nk, 8, 1)) < ROWS
        coef = jnp.concatenate(
            [
                jnp.where(top1, coef[0:nk], coef[nk : 2 * nk]),
                jnp.where(top1, coef[2 * nk : 3 * nk], coef[3 * nk :]),
            ],
            0,
        ).reshape(ROWS * nz, 1)
        gate = dot(xv, eg[...])
        up = dot(xv, eu[...])
        inner = (gate * jax.nn.sigmoid(gate) * up).astype(BF16)
        return inner, coef

    def down(inner, coef, z, j, width):
        cols = slice(j * width, (j + 1) * width)
        low = dot(inner, ed[:, cols]) * coef
        high = dot(inner, ed[:, half + j * width : half + (j + 1) * width]) * coef
        low, high = low.reshape(2, nk, 8, width), high.reshape(2, nk, 8, width)
        keep = row_ids((nk, 8, width)) < ROWS
        for s in range(2):
            one = jnp.where(keep, low[s], pltpu.roll(high[s], ROWS, 1))
            two = jnp.where(keep, pltpu.roll(low[s], ROWS, 1), high[s])
            z[2 * s, :, :, cols] = one.astype(BF16)
            z[2 * s + 1, :, :, cols] = two.astype(BF16)

    width = min(256, half)
    inner, coef = expert(c)
    for j in range(half // width):
        down(inner, coef, zown, j, width)
    to_sib(hid.at[1 - c], hid.at[1 - c], 1).wait_recv()
    inner, coef = expert(1 - c)
    for j in range(half // width):
        down(inner, coef, zoth, j, width)
    to_sib(zoth, zsib, 2).start()
    to_sib(zoth, zsib, 2).wait_recv()
    tsum[...] = (zown[...].astype(F32) + zsib[...].astype(F32)).astype(BF16)

    def near_sum(slot):
        k = slot % nk
        part = k // hk
        up, down_, far = (res + 1) % STRIDE, (res + STRIDE - 1) % STRIDE, (res + 2) % STRIDE
        return [
            pltpu.make_async_remote_copy(
                src_ref=tsum.at[r, k],
                dst_ref=r1.at[i, k],
                send_sem=f1_send.at[i],
                recv_sem=f1_recv.at[i, k],
                device_id=chip(to),
                device_id_type=MESH,
            )
            for i, (to, r) in enumerate(
                ((z + 1, up), (z + nz - 1, down_), (z + nz + 2 - 4 * part, far))
            )
        ]

    def step_sum(kt, src, sem):
        return pltpu.make_async_remote_copy(
            src_ref=u2.at[src],
            dst_ref=r2.at[sem],
            send_sem=f2_send.at[sem],
            recv_sem=f2_recv.at[sem],
            device_id=chip((kt % nk) * STRIDE + res),
            device_id_type=MESH,
        )

    def near_total(slot):
        k = slot % nk
        for cp in near_sum(k):
            cp.wait_recv()
        return (
            tsum[res, k].astype(F32)
            + r1[0, k].astype(F32)
            + r1[1, k].astype(F32)
            + r1[2, k].astype(F32)
        )

    def arrived(sem):
        step_sum(own_k, 0, sem).wait_recv()
        return r2[sem].astype(F32)

    if nk == 8:
        order = [nk + 4, nk - 3, nk + 3, nk - 2 * side, nk + 2 * side, nk - 1, nk + 1, nk]
    else:
        order = [nk // 2] + ([1, nk - 1] if nk == 4 else []) + [nk]
    for o in order:
        for cp in near_sum(own_k + o):
            cp.start()
    if nk == 8:
        u2[0] = near_total(own_k + 4).astype(BF16)
        step_sum(own_k + nk + 2 * side * -1, 0, 0).start()
        u2[1] = near_total(own_k + nk - 3 * side).astype(BF16)
        step_sum(own_k + nk - side, 1, 1).start()
        u2[2] = near_total(own_k + nk + 3 * side).astype(BF16)
        step_sum(own_k + nk + side, 2, 2).start()
        u2[3] = near_total(own_k + nk - side).astype(BF16)
        step_sum(own_k + nk - side, 3, 3).start()
        u2[4] = near_total(own_k + nk + side).astype(BF16)
        step_sum(own_k + nk + side, 4, 4).start()
        part_b = near_total(own_k + nk + 2 * side)
        part_a = near_total(own_k + nk - 2 * side)
        u2[6] = (part_b + arrived(1)).astype(BF16)
        step_sum(own_k + nk + 2 * side, 6, 6).start()
        u2[5] = (part_a + arrived(2) + arrived(0)).astype(BF16)
        step_sum(own_k + nk - 2 * side, 5, 5).start()
        total = near_total(own_k)
        used = range(7)
    else:
        for i, o in enumerate(order[:-1]):
            u2[i] = near_total(own_k + o).astype(BF16)
            step_sum(own_k + o, i, i).start()
        total = near_total(own_k)
        used = range(len(order) - 1)
    total = total + hidp[...]
    for sem in used:
        if nk != 8 or sem >= 3:
            total = total + arrived(sem)
    y = layer_norm(total, egain, ebias)
    out_ref[:, 0:half] = y[0:ROWS, :].astype(BF16)
    out_ref[:, half:dim] = y[ROWS : 2 * ROWS, :].astype(BF16)

    gather_drain(xt, 0)
    gather_drain(xm, 1)
    gather_drain(xg, 2)
    for i in range(nm):
        scatter_all(wb.at[gq * nm + i, c], w_send.at[i], w_recv.at[i]).wait_send()
        slab(gq * nm + i, c, sib, s_send.at[0, i], s_recv.at[0, i]).wait_send()
        for g in range(1, share):
            slab(gq * nm + i, c, sib, q_send.at[g, i], q_recv.at[g, i]).wait_send()
            m = ((gq + g) % share) * nm + i
            slab(m, c, sib, s_send.at[g, i], s_recv.at[g, i]).wait_send()
    scatter_all(yrecv, a_send.at[0], a_recv.at[0]).wait_send()
    scatter_all(cb.at[c], a_send.at[2], a_recv.at[2]).wait_send()
    to_sib(cb.at[c], cb.at[c], 0).wait_send()
    to_sib(hid.at[c], hid.at[c], 1).wait_send()
    to_sib(zoth, zsib, 2).wait_send()
    for i in range(3):
        pltpu.make_async_remote_copy(
            src_ref=tsum.at[res],
            dst_ref=r1.at[i],
            send_sem=f1_send.at[i],
            recv_sem=f1_recv.at[i, 0],
            device_id=chip(z + 1),
            device_id_type=MESH,
        ).wait_send()
    for sem in used:
        step_sum(own_k, sem, sem).wait_send()
    st_store.wait()


def step(nz, share, *args):
    tokens, state = args[0], args[1]
    dim = tokens.shape[1]
    half = dim // 2
    nk = nz // STRIDE
    nm = 4 // share
    ff = args[24].shape[2]
    args = list(args)
    args[5], args[8] = args[5].T, args[8].T
    for i in (7, 10, 13, 15, 16, 18, 19, 20, 21):
        args[i] = args[i].reshape(1, dim)
    small = [5, 6, 7, 8, 9, 10, 11, 12, 13, 14, 15, 16, 18, 19, 20, 21, 22, 23]
    operands = [args[i] for i in [0, 1, 2, 3, 4, 17] + small + [24, 25, 26]]
    vmem = pl.BlockSpec(memory_space=pltpu.VMEM)
    hbm = pl.BlockSpec(memory_space=pl.ANY)
    dma = pltpu.SemaphoreType.DMA
    heads = (nz, 8, 128)
    rows = (STRIDE, nk, 8, half)
    scratch = [
        pltpu.VMEM(tokens.shape, BF16),
        *[pltpu.VMEM(args[i].shape, args[i].dtype) for i in small],
        pltpu.VMEM(state.shape, F32),
        pltpu.VMEM(state.shape, F32),
        pltpu.VMEM((nm, 32, dim), BF16),
        pltpu.VMEM((nm, nz, 16, 128), BF16),
        pltpu.VMEM((4, 2, nz, 16, 128), BF16),
        pltpu.VMEM((half, 1024), BF16),
        pltpu.VMEM(rows, BF16),
        pltpu.VMEM(rows, BF16),
        pltpu.VMEM((STRIDE, nk, nk, 8, 128), BF16),
        pltpu.VMEM((2, nk, 8, dim), F32),
        pltpu.VMEM((2, ROWS * nz, dim), BF16),
        pltpu.VMEM(heads, BF16),
        pltpu.VMEM(heads, BF16),
        pltpu.VMEM((2,) + heads, BF16),
        pltpu.VMEM((8, 128), BF16),
        pltpu.VMEM((8, dim), F32),
        pltpu.VMEM((8, half), F32),
        pltpu.VMEM((8, half), F32),
        pltpu.VMEM(heads, F32),
        pltpu.VMEM(heads, F32),
        pltpu.VMEM(heads, F32),
        pltpu.VMEM(heads, F32),
        pltpu.VMEM(heads, F32),
        pltpu.VMEM(heads, F32),
        pltpu.VMEM((dim, ff), BF16),
        pltpu.VMEM((dim, ff), BF16),
        pltpu.VMEM((ff, dim), BF16),
        pltpu.VMEM(rows, BF16),
        pltpu.VMEM(rows, BF16),
        pltpu.VMEM(rows, BF16),
        pltpu.VMEM(rows, BF16),
        pltpu.VMEM((3, nk, 8, half), BF16),
        pltpu.VMEM((nk, 8, half), BF16),
        pltpu.VMEM((nk, 8, half), BF16),
        dma((9,)),
        dma((nm,)),
        dma((nm,)),
        dma((share, nm)),
        dma((share, nm)),
        dma((share, nm)),
        dma((share, nm)),
        dma((3, 7)),
        dma((3, 7)),
        dma((3, 3)),
        dma((3, 4)),
        dma((3,)),
        dma((3,)),
        dma((3,)),
        dma((3,)),
        dma((3,)),
        dma((3, nk)),
        dma((7,)),
        dma((7,)),
        dma((SMALL,)),
    ]
    return pl.pallas_call(
        functools.partial(kernel, nz, share),
        out_shape=(
            jax.ShapeDtypeStruct(tokens.shape, BF16),
            jax.ShapeDtypeStruct(state.shape, F32),
        ),
        in_specs=[hbm] * len(operands),
        out_specs=(vmem, hbm),
        scratch_shapes=scratch,
        compiler_params=pltpu.CompilerParams(
            collective_id=0, has_side_effects=True, vmem_limit_bytes=56 * 1024 * 1024
        ),
    )(*operands)


def solution(mesh):
    nz = mesh.shape["ep"] // 2
    groups = mesh.shape["grp"]
    share = 4 if groups % 4 == 0 else 2 if groups % 2 == 0 else 1
    owned, split, copied = P(("grp", "ep"), None), P("ep", None), P()
    in_specs = (
        owned,
        P(("grp", "ep"), None, None, None),
        split,
        split,
        split,
        *([copied] * 12),
        split,
        *([copied] * 4),
        owned,
        owned,
        P("ep", None, None),
        P("ep", None, None),
        P("ep", None, None),
    )
    out_specs = (owned, P(("grp", "ep"), None, None, None))
    return jax.shard_map(
        functools.partial(step, nz, share),
        mesh=mesh,
        in_specs=in_specs,
        out_specs=out_specs,
        check_vma=False,
    )
```

```python
import functools

import jax
import jax.numpy as jnp
from jax import lax
from jax.experimental import pallas as pl
from jax.experimental.pallas import tpu as pltpu
from jax.sharding import PartitionSpec as P

MESH = pl.DeviceIdType.MESH
F32 = jnp.float32
BF16 = jnp.bfloat16
SMALL = 18
ROWS = 4
HEAD = 64
STRIDE = 4


def dot(a, b):
    return jnp.dot(a, b, preferred_element_type=F32)


def lane_ids(shape):
    return lax.broadcasted_iota(jnp.int32, shape, len(shape) - 1)


def row_ids(shape):
    return lax.broadcasted_iota(jnp.int32, shape, len(shape) - 2)


def kernel(
    nz,
    share,
    tok_hbm,
    state_hbm,
    wr_hbm,
    wk_hbm,
    wv_hbm,
    wo_hbm,
    *rest,
):
    small_hbm, rest = rest[:SMALL], rest[SMALL:]
    run(nz, share, tok_hbm, state_hbm, (wr_hbm, wk_hbm, wv_hbm, wo_hbm), small_hbm, *rest)


def run(
    nz,
    share,
    tok_hbm,
    state_hbm,
    w_hbm,
    small_hbm,
    eg_hbm,
    eu_hbm,
    ed_hbm,
    out_ref,
    next_hbm,
    tok_ref,
    *rest,
):
    small, rest = rest[:SMALL], rest[SMALL:]
    work(nz, share, tok_hbm, state_hbm, w_hbm, small_hbm, eg_hbm, eu_hbm, ed_hbm,
         out_ref, next_hbm, tok_ref, small, *rest)


def work(
    nz,
    share,
    tok_hbm,
    state_hbm,
    w_hbm,
    small_hbm,
    eg_hbm,
    eu_hbm,
    ed_hbm,
    out_ref,
    next_hbm,
    tok_ref,
    small,
    st,
    sn,
    wstage,
    wsend,
    wb,
    em,
    xt,
    xm,
    xg,
    x2,
    hid,
    ysend,
    yrecv,
    cb,
    csend,
    tok8,
    tokp,
    hidp,
    dh,
    ah,
    gh,
    ro,
    sv,
    bh,
    eg,
    eu,
    ed,
    zown,
    zoth,
    zsib,
    tsum,
    r1,
    u2,
    r2,
    ld_sem,
    w_send,
    w_recv,
    q_send,
    q_recv,
    s_send,
    s_recv,
    l1_send,
    l1_recv,
    l2_send,
    l2_recv,
    a_send,
    a_recv,
    x_send,
    x_recv,
    f1_send,
    f1_recv,
    f2_send,
    f2_recv,
    small_sem,
):
    (
        dl1, dl2, doff, cl1, cl2, coff, gl1, gl2, blend,
        sscale, hgain, hbias, mgain, mbias, egain, ebias, routes, rweight,
    ) = small
    nk = nz // STRIDE
    dim = HEAD * nz
    half = dim // 2
    nm = 4 // share
    quarter = nz // 4
    ep = lax.axis_index("ep")
    grp = lax.axis_index("grp")
    z = ep // 2
    c = ep % 2
    gq = grp % share
    gbase = grp - gq
    res = z % STRIDE
    own_k = z // STRIDE
    sib = {"ep": z * 2 + 1 - c}

    def chip(zt):
        return {"ep": (zt % nz) * 2 + c}

    def slot_of(zt):
        return (zt % STRIDE) * nk + zt // STRIDE

    def far_first(j):
        d = nz // 2 - (j + 1) // 2
        return (z + nz + d * (1 - 2 * (j % 2))) % nz

    bar = pltpu.get_barrier_semaphore()

    @pl.loop(1, nz)
    def _(j):
        pl.semaphore_signal(bar, inc=1, device_id=chip(z + j), device_id_type=MESH)

    pl.semaphore_signal(bar, inc=1, device_id=sib, device_id_type=MESH)
    for i in range(1, share):
        pl.semaphore_signal(
            bar, inc=1, device_id={"grp": gbase + (gq + i) % share}, device_id_type=MESH
        )

    tok_load = pltpu.make_async_copy(tok_hbm, tok_ref, ld_sem.at[8])
    tok_load.start()
    for i in range(nm):
        for m in range(4):
            if m % nm == i:

                @pl.when(gq == m // nm)
                def _(i=i, m=m):
                    pltpu.make_async_copy(w_hbm[m], wstage.at[i], ld_sem.at[i]).start()

    st_load = pltpu.make_async_copy(state_hbm, st, ld_sem.at[4])
    eg_load = pltpu.make_async_copy(eg_hbm.at[0], eg, ld_sem.at[5])
    eu_load = pltpu.make_async_copy(eu_hbm.at[0], eu, ld_sem.at[6])
    ed_load = pltpu.make_async_copy(ed_hbm.at[0], ed, ld_sem.at[7])
    small_loads = [
        pltpu.make_async_copy(a, b, small_sem.at[i])
        for i, (a, b) in enumerate(zip(small_hbm, small))
    ]
    for cp in small_loads:
        cp.start()
    st_load.start()
    eg_load.start()
    eu_load.start()
    ed_load.start()

    lane128 = lane_ids((8, 128))
    left = lane128 < HEAD
    top = row_ids((8, 128)) < ROWS
    lane16 = lane_ids((16, 128))
    left16 = lane16 < HEAD

    tok_load.wait()
    tok = tok_ref[...].astype(F32)
    tok8[0:ROWS, :] = tok
    tok8[ROWS : 2 * ROWS, :] = tok
    tokp[0:ROWS, :] = tok[:, :half]
    tokp[ROWS : 2 * ROWS, :] = tok[:, half:]
    xt[res, own_k] = tokp[...].astype(BF16)

    for i in range(nm):
        pltpu.make_async_copy(w_hbm[0], wstage.at[i], ld_sem.at[i]).wait()

        @pl.loop(0, nz // 2)
        def _(t, i=i):
            at = pl.multiple_of(t * 128, 128)
            a = wstage[i, 0:16, pl.ds(at, 128)].astype(F32)
            b = wstage[i, 16:32, pl.ds(at, 128)].astype(F32)
            wsend[i, 2 * t] = jnp.where(left16, a, pltpu.roll(b, HEAD, 1)).astype(BF16)
            wsend[i, 2 * t + 1] = jnp.where(left16, pltpu.roll(a, HEAD, 1), b).astype(BF16)

        wb[gq * nm + i, c, z] = wsend[i, z]

    for cp in small_loads:
        cp.wait()
    weight = rweight[...]
    part = weight / jnp.sum(weight, -1, keepdims=True)
    ids = routes[...]
    lanes4 = lane_ids((ROWS, 128))
    by_expert = jnp.zeros((ROWS, 128), F32)
    for k in range(ids.shape[1]):
        by_expert += jnp.where(ids[:, k : k + 1] == lanes4, part[:, k : k + 1], 0.0)
    high = by_expert.astype(BF16).astype(F32)
    low = by_expert - high
    both = jnp.where(lanes4 < HEAD, high, pltpu.roll(low, HEAD, 1))
    sv[0, 0:ROWS, :] = both
    sv[0, ROWS : 2 * ROWS, :] = both
    csend[...] = sv[0].astype(BF16)
    my_slot = slot_of(z)
    cb[c, my_slot] = csend[...]

    side = 1 - 2 * (own_k % 2)
    hk = nk // 2

    def step_copy(buf, n, slot, sem, kt):
        at = buf.at[res, slot % nk]
        return pltpu.make_async_remote_copy(
            src_ref=at,
            dst_ref=at,
            send_sem=l1_send.at[n, sem],
            recv_sem=l1_recv.at[n, sem],
            device_id=chip((kt % nk) * STRIDE + res),
            device_id_type=MESH,
        )

    def near_copies(buf, n, slot):
        k = slot % nk
        at = buf.at[res, k]
        part = k // hk
        for i, to, sem in ((0, z + 1, 0), (1, z + nz - 1, 1), (2, z + nz + 2 - 4 * part, 2 + part)):
            pltpu.make_async_remote_copy(
                src_ref=at,
                dst_ref=at,
                send_sem=l2_send.at[n, i],
                recv_sem=l2_recv.at[n, sem],
                device_id=chip(to),
                device_id_type=MESH,
            ).start()

    direct = [(0, -1), (1, 1)] + ([(2, -2), (3, 2)] if nk > 4 else []) if nk > 2 else []
    direct += [(6, nk // 2)] if nk in (2, 4) else []
    onward = [(4, -3), (5, 3), (6, 4)] if nk == 8 else []

    def gather_start(buf, n):
        for sem, o in reversed(direct):
            step_copy(buf, n, own_k, sem, own_k + nk - o).start()
        near_copies(buf, n, own_k)

    def gather_direct(buf, n):
        for sem, o in direct:
            step_copy(buf, n, own_k + nk + o, sem, own_k).wait_recv()
            if sem == 2 and onward:
                step_copy(buf, n, own_k + nk - 2, 4, own_k + 1).start()
            if sem == 3 and onward:
                step_copy(buf, n, own_k + nk + 2, 5, own_k + nk - 1).start()
                step_copy(buf, n, own_k + nk - 2 * side, 6, own_k + nk + 2 * side).start()
            if sem < 2 or not onward:
                near_copies(buf, n, own_k + nk + o)
        if onward:
            near_copies(buf, n, own_k + nk - 2)
            near_copies(buf, n, own_k + nk + 2)

    def gather_onward(buf, n):
        for sem, o in onward:
            step_copy(buf, n, own_k + nk + o, sem, own_k).wait_recv()
            near_copies(buf, n, own_k + nk + o)

    def near_all(buf, n, i, sem, r, k0, count):
        at = buf.at[r, pl.ds(k0, count)]
        return pltpu.make_async_remote_copy(
            src_ref=at,
            dst_ref=at,
            send_sem=l2_send.at[n, i],
            recv_sem=l2_recv.at[n, sem],
            device_id=chip(z + 1),
            device_id_type=MESH,
        )

    def gather_wait(buf, n):
        near_all(buf, n, 0, 0, (res + STRIDE - 1) % STRIDE, 0, nk).wait_recv()
        near_all(buf, n, 1, 1, (res + 1) % STRIDE, 0, nk).wait_recv()
        near_all(buf, n, 2, 2, (res + 2) % STRIDE, 0, hk).wait_recv()
        near_all(buf, n, 2, 3, (res + 2) % STRIDE, hk, hk).wait_recv()

    def gather_drain(buf, n):
        for sem, _ in direct + onward:
            step_copy(buf, n, own_k, sem, own_k).wait_send()
        for i in range(3):
            near_all(buf, n, i, i, res, 0, nk).wait_send()

    def scatter(src_of, dst, send_sem, recv_sem):
        @pl.loop(0, nz - 1)
        def _(j):
            zt = far_first(j)
            pltpu.make_async_remote_copy(
                src_ref=src_of(zt),
                dst_ref=dst,
                send_sem=send_sem,
                recv_sem=recv_sem,
                device_id=chip(zt),
                device_id_type=MESH,
            ).start()

    def scatter_all(block, send_sem, recv_sem):
        return pltpu.make_async_remote_copy(
            src_ref=block.at[pl.ds(0, nz - 1)],
            dst_ref=block.at[pl.ds(0, nz - 1)],
            send_sem=send_sem,
            recv_sem=recv_sem,
            device_id=chip(z),
            device_id_type=MESH,
        )

    tokb = tok8[...].astype(BF16)

    def dot_t(a, b):
        return lax.dot_general(a, b, (((1,), (1,)), ((), ())), preferred_element_type=F32)

    squash = jnp.tanh(dot_t(tokb, dl1[...])).astype(BF16)
    lowl = dot_t(tokb, cl1[...]).astype(BF16)
    opened = jax.nn.sigmoid(dot(tokb, gl1[...])).astype(BF16)

    for j in range(nz // 2):
        cols = slice(128 * j, 128 * j + 128)

        def two_heads(ref, tile, j=j):
            ref[2 * j] = tile
            ref[2 * j + 1] = pltpu.roll(tile, HEAD, 1)

        pre = doff[:, cols] + dot(squash, dl2[:, cols])
        two_heads(dh, jnp.exp(-(jnp.exp(jnp.full((8, 128), -0.5, F32)) * jax.nn.sigmoid(pre))))
        two_heads(ah, jax.nn.sigmoid(coff[:, cols] + dot(lowl, cl2[:, cols])))
        two_heads(gh, dot(opened, gl2[:, cols]))

    pl.semaphore_wait(bar, nz - 1 + 1 + share - 1)

    for i in range(nm):
        m = gq * nm + i
        scatter(
            lambda zt, i=i: wsend.at[i, zt],
            wb.at[m, c, z],
            w_send.at[i],
            w_recv.at[i, z // quarter],
        )
    gather_start(xt, 0)

    gather_direct(xt, 0)

    def piece(m, core, n, to, send_sem, recv_sem):
        at = wb.at[m, core, pl.ds(n * quarter, quarter)]
        return pltpu.make_async_remote_copy(
            src_ref=at,
            dst_ref=at,
            send_sem=send_sem,
            recv_sem=recv_sem,
            device_id=to,
            device_id_type=MESH,
        )

    def sib_piece(m, core, n):
        return piece(m, core, n, sib, s_send.at[m, n], s_recv.at[m, n])

    def group_piece(m, n, g):
        to = {"grp": gbase + (gq + g) % share} if share > 1 else sib
        return piece(m, c, n, to, q_send.at[g, m % nm, n], q_recv.at[m, n])

    def hand_out(i, m):
        for d in range(4):
            n = (z // quarter + d) % 4
            count = quarter - 1 if d == 0 else quarter
            at = wb.at[m, c, pl.ds(0, count)]
            pltpu.make_async_remote_copy(
                src_ref=at,
                dst_ref=at,
                send_sem=w_send.at[i],
                recv_sem=w_recv.at[i, n],
                device_id=chip(z),
                device_id_type=MESH,
            ).wait_recv()
            for g in range(1, share):
                group_piece(m, n, g).start()
            sib_piece(m, c, n).start()

    def pass_on(m):
        for n in range(4):
            group_piece(m, n, 0).wait_recv()
            sib_piece(m, c, n).start()

    def mine(m):
        return gq == m // nm

    for m in range(3):
        pl.when(mine(m))(functools.partial(hand_out, m % nm, m))
    gather_onward(xt, 0)
    if share > 1:
        for m in range(3):
            pl.when(jnp.logical_not(mine(m)))(functools.partial(pass_on, m))

    def widen(m, at):
        keep = left16.astype(F32).astype(BF16)
        drop = (1.0 - left16.astype(F32)).astype(BF16)
        for hk in range(2):

            @pl.loop(0, nz // 2)
            def _(zz, hk=hk):
                for core in range(2):
                    tile = wb[m, core, hk * (nz // 2) + zz]
                    base = pl.multiple_of(zz * 64 + core * 32, 32)
                    cols = slice(at + hk * 128, at + hk * 128 + 128)
                    em[pl.ds(base, 16), cols] = tile * keep
                    em[pl.ds(pl.multiple_of(base + 16, 16), 16), cols] = tile * drop

    def rows_of(value):
        return value.astype(F32).reshape(8 * nz, half).astype(BF16)

    top3 = row_ids((nz, 8, 128)) < ROWS
    left3 = lane_ids((nz, 8, 128)) < HEAD
    topw = (row_ids((8 * nz, 128)) % 8) < ROWS

    def fold(r):
        a = jnp.where(topw, r[:, 0:128], r[:, 128:256])
        a = (a + pltpu.roll(a, HEAD, 1)).reshape(nz, 8, 128)
        return a + pltpu.roll(a, ROWS, 1)

    for m in range(3):
        for n in range(4):
            sib_piece(m, 1 - c, n).wait_recv()
        widen(m, m * 256)

    gather_wait(xt, 0)
    xv = rows_of(xt[...])
    cr = fold(dot(xv, em[:, 0:256]))
    ck = fold(dot(xv, em[:, 256:512]))
    cv = fold(dot(xv, em[:, 512:768]))
    ysend[...] = jnp.where(top3, jnp.where(left3, cr, ck), cv).astype(BF16)
    scatter(lambda zt: ysend.at[slot_of(zt)], yrecv.at[z], a_send.at[0], a_recv.at[0])
    yrecv[z] = ysend[my_slot]
    scatter(lambda zt: csend, cb.at[c, my_slot], a_send.at[2], a_recv.at[2])
    topk = row_ids((nk, 8, 128)) < ROWS
    leftk = lane_ids((nk, 8, 128)) < HEAD
    for s in range(2):
        for m in range(half // 128):
            one = xt[2 * s, :, :, 128 * m : 128 * m + 128].astype(F32)
            two = xt[2 * s + 1, :, :, 128 * m : 128 * m + 128].astype(F32)
            x2[s, :, :, 128 * m : 128 * m + 128] = jnp.where(topk, one, pltpu.roll(two, ROWS, 1))
            x2[s, :, :, half + 128 * m : half + 128 * m + 128] = jnp.where(
                topk, pltpu.roll(one, ROWS, 1), two
            )
    pl.when(mine(3))(functools.partial(hand_out, 3 % nm, 3))
    st_load.wait()
    scatter_all(yrecv, a_send.at[0], a_recv.at[0]).wait_recv()

    eye = (
        lax.broadcasted_iota(jnp.int32, (HEAD, HEAD), 0)
        == lax.broadcasted_iota(jnp.int32, (HEAD, HEAD), 1)
    ).astype(F32)

    def pick(ref, j):
        tile = jnp.broadcast_to(ref[:, 128 * j : 128 * j + 128], (8, 128))
        return tile, pltpu.roll(tile, HEAD, 1)

    blends = []
    for j in range(nz // 2):
        blends += pick(blend, j)
    for h in range(nz):
        bh[h] = blends[h]

    @pl.loop(0, nz // 2)
    def _(pair):
        for h in (2 * pair, 2 * pair + 1):
            y = yrecv[h].astype(F32)
            turned = pltpu.roll(y, ROWS, 0)
            rk = jnp.where(top, y, turned)
            v = jnp.where(top, turned, y)
            r = jnp.where(left, rk, 0.0)
            k = jnp.where(left, pltpu.roll(rk, HEAD, 1), 0.0)
            a = ah[h]
            unit = k * lax.rsqrt(jnp.sum(k * k, -1, keepdims=True) + 1e-06)
            written = k * (1.0 + (a - 1.0) * bh[h])
            ua = unit * a
            scale = sscale[pl.ds(h, 1), :]
            own = jnp.sum((r * written)[:, 0:HEAD] * scale, -1, keepdims=True)
            d = dh[h]
            sv[h] = own * v
            for t in range(ROWS):
                one = slice(t, t + 1)
                s = st[t, h]
                removed = jnp.sum(s * unit[one, 0:HEAD], -1, keepdims=True)
                vcol = jnp.sum(eye * v[one, 0:HEAD], -1, keepdims=True)
                n = s * d[one, 0:HEAD] - removed * ua[one, 0:HEAD] + vcol * written[one, 0:HEAD]
                sn[t, h] = n
                read = jnp.sum(n * r[one, 0:HEAD], -1, keepdims=True)
                row = jnp.sum(eye * read, 0, keepdims=True)
                ro[h, t : t + 1, 0:HEAD] = row
                ro[h, ROWS + t : ROWS + t + 1, 0:HEAD] = row

    st_store = pltpu.make_async_copy(sn, next_hbm, ld_sem.at[4])
    st_store.start()

    def mixer_head(h, gain, bias):
        x = jnp.where(left, ro[h], 0.0)
        mean = jnp.sum(x, -1, keepdims=True) * (1.0 / HEAD)
        dev = jnp.where(left, x - mean, 0.0)
        var = jnp.sum(dev * dev, -1, keepdims=True) * (1.0 / HEAD)
        normed = dev * lax.rsqrt(var + 0.00064) * gain + bias
        return (normed + sv[h]) * gh[h]

    def mixer_pair(j):
        g0, g1 = pick(hgain, j)
        b0, b1 = pick(hbias, j)
        one, two = mixer_head(2 * j, g0, b0), mixer_head(2 * j + 1, g1, b1)
        return jnp.where(left, one, pltpu.roll(two, HEAD, 1))

    for j in range(nz // 4):
        tile = jnp.where(top, mixer_pair(j), mixer_pair(nz // 4 + j))
        xm[res, own_k, :, 128 * j : 128 * j + 128] = tile.astype(BF16)

    gather_start(xm, 1)
    if share > 1:
        pl.when(jnp.logical_not(mine(3)))(functools.partial(pass_on, 3))
    gather_direct(xm, 1)
    gather_onward(xm, 1)
    for n in range(4):
        sib_piece(3, 1 - c, n).wait_recv()
    widen(3, 768)
    gather_wait(xm, 1)
    co = fold(dot(rows_of(xm[...]), em[:, 768:1024]))
    xg[res, own_k] = jnp.where(
        leftk,
        jnp.where(topk, co[0:nk], co[nk : 2 * nk]),
        jnp.where(topk, co[2 * nk : 3 * nk], co[3 * nk :]),
    ).astype(BF16)
    gather_start(xg, 2)

    scatter_all(cb.at[c], a_send.at[2], a_recv.at[2]).wait_recv()

    def to_sib(src, dst, n):
        return pltpu.make_async_remote_copy(
            src_ref=src,
            dst_ref=dst,
            send_sem=x_send.at[n],
            recv_sem=x_recv.at[n],
            device_id=sib,
            device_id_type=MESH,
        )

    to_sib(cb.at[c], cb.at[c], 0).start()

    gather_direct(xg, 2)
    gather_onward(xg, 2)
    gather_wait(xg, 2)
    for j in range(nz // 2):
        cols = slice(128 * j, 128 * j + 128)
        one = xg[2 * j % STRIDE, 2 * j // STRIDE].astype(F32)
        two = xg[(2 * j + 1) % STRIDE, (2 * j + 1) // STRIDE].astype(F32)
        x2[0, :, :, cols] += jnp.where(leftk, one, pltpu.roll(two, HEAD, 2))
        x2[1, :, :, cols] += jnp.where(leftk, pltpu.roll(one, HEAD, 2), two)

    some = max(1, nk // 2)
    for s in range(2):
        for k in range(0, nk, some):
            x = x2[s, k : k + some]
            dev = x - jnp.mean(x, -1, keepdims=True)
            var = jnp.mean(dev * dev, -1, keepdims=True)
            y = dev * lax.rsqrt(var + 1e-05) * mgain[...] + mbias[...]
            x2[s, k : k + some] = y
            base = 8 * (s * nk + k)
            hid[c, base : base + 8 * some, :] = y.reshape(8 * some, dim).astype(BF16)

    to_sib(hid.at[c], hid.at[c], 1).start()

    topp = row_ids((8, half)) < ROWS

    def packed(ref):
        return jnp.where(topp, ref[:, 0:half], ref[:, half:dim])

    def row_total(x):
        s = jnp.broadcast_to(jnp.sum(x, -1, keepdims=True), (8, 128))
        s = s + pltpu.roll(s, ROWS, 0)
        return s[:, 0:1] * (1.0 / dim)

    def layer_norm(x, gain, bias):
        dev = x - row_total(x)
        var = row_total(dev * dev)
        return dev * lax.rsqrt(var + 1e-05) * packed(gain) + packed(bias)

    two_rows = x2[res // 2, own_k].astype(BF16).astype(F32)
    mine = row_ids((8, dim)) // ROWS == res % 2
    doubled = jnp.where(mine, two_rows, pltpu.roll(two_rows, ROWS, 0))
    hidp[...] = jnp.where(topp, doubled[:, 0:half], doubled[:, half:dim])

    eg_load.wait()
    eu_load.wait()
    ed_load.wait()
    to_sib(cb.at[1 - c], cb.at[1 - c], 0).wait_recv()

    def expert(core):
        xv = hid[core]
        lane3 = lane_ids((nz, 8, 128))
        hit = (lane3 == ep) | (lane3 == ep + HEAD)
        coef = jnp.sum(jnp.where(hit, cb[core].astype(F32), 0.0), -1, keepdims=True)
        top1 = row_ids((nk, 8, 1)) < ROWS
        coef = jnp.concatenate(
            [
                jnp.where(top1, coef[0:nk], coef[nk : 2 * nk]),
                jnp.where(top1, coef[2 * nk : 3 * nk], coef[3 * nk :]),
            ],
            0,
        ).reshape(ROWS * nz, 1)
        gate = dot(xv, eg[...])
        up = dot(xv, eu[...])
        inner = (gate * jax.nn.sigmoid(gate) * up).astype(BF16)
        return inner, coef

    def down(inner, coef, z, j, width):
        cols = slice(j * width, (j + 1) * width)
        low = dot(inner, ed[:, cols]) * coef
        high = dot(inner, ed[:, half + j * width : half + (j + 1) * width]) * coef
        low, high = low.reshape(2, nk, 8, width), high.reshape(2, nk, 8, width)
        keep = row_ids((nk, 8, width)) < ROWS
        for s in range(2):
            one = jnp.where(keep, low[s], pltpu.roll(high[s], ROWS, 1))
            two = jnp.where(keep, pltpu.roll(low[s], ROWS, 1), high[s])
            z[2 * s, :, :, cols] = one.astype(BF16)
            z[2 * s + 1, :, :, cols] = two.astype(BF16)

    width = min(256, half)
    inner, coef = expert(c)
    for j in range(half // width):
        down(inner, coef, zown, j, width)
    to_sib(hid.at[1 - c], hid.at[1 - c], 1).wait_recv()
    inner, coef = expert(1 - c)
    for j in range(half // width):
        down(inner, coef, zoth, j, width)
    to_sib(zoth, zsib, 2).start()
    to_sib(zoth, zsib, 2).wait_recv()
    tsum[...] = (zown[...].astype(F32) + zsib[...].astype(F32)).astype(BF16)

    def near_sum(slot):
        k = slot % nk
        part = k // hk
        up, down_, far = (res + 1) % STRIDE, (res + STRIDE - 1) % STRIDE, (res + 2) % STRIDE
        return [
            pltpu.make_async_remote_copy(
                src_ref=tsum.at[r, k],
                dst_ref=r1.at[i, k],
                send_sem=f1_send.at[i],
                recv_sem=f1_recv.at[i, k],
                device_id=chip(to),
                device_id_type=MESH,
            )
            for i, (to, r) in enumerate(
                ((z + 1, up), (z + nz - 1, down_), (z + nz + 2 - 4 * part, far))
            )
        ]

    def step_sum(kt, src, sem):
        return pltpu.make_async_remote_copy(
            src_ref=u2.at[src],
            dst_ref=r2.at[sem],
            send_sem=f2_send.at[sem],
            recv_sem=f2_recv.at[sem],
            device_id=chip((kt % nk) * STRIDE + res),
            device_id_type=MESH,
        )

    def near_total(slot):
        k = slot % nk
        for cp in near_sum(k):
            cp.wait_recv()
        return (
            tsum[res, k].astype(F32)
            + r1[0, k].astype(F32)
            + r1[1, k].astype(F32)
            + r1[2, k].astype(F32)
        )

    def arrived(sem):
        step_sum(own_k, 0, sem).wait_recv()
        return r2[sem].astype(F32)

    if nk == 8:
        order = [nk + 4, nk - 3, nk + 3, nk - 2 * side, nk + 2 * side, nk - 1, nk + 1, nk]
    else:
        order = [nk // 2] + ([1, nk - 1] if nk == 4 else []) + [nk]
    for o in order:
        for cp in near_sum(own_k + o):
            cp.start()
    if nk == 8:
        u2[0] = near_total(own_k + 4).astype(BF16)
        step_sum(own_k + nk + 2 * side * -1, 0, 0).start()
        u2[1] = near_total(own_k + nk - 3 * side).astype(BF16)
        step_sum(own_k + nk - side, 1, 1).start()
        u2[2] = near_total(own_k + nk + 3 * side).astype(BF16)
        step_sum(own_k + nk + side, 2, 2).start()
        u2[3] = near_total(own_k + nk - side).astype(BF16)
        step_sum(own_k + nk - side, 3, 3).start()
        u2[4] = near_total(own_k + nk + side).astype(BF16)
        step_sum(own_k + nk + side, 4, 4).start()
        part_b = near_total(own_k + nk + 2 * side)
        part_a = near_total(own_k + nk - 2 * side)
        u2[6] = (part_b + arrived(1)).astype(BF16)
        step_sum(own_k + nk + 2 * side, 6, 6).start()
        u2[5] = (part_a + arrived(2) + arrived(0)).astype(BF16)
        step_sum(own_k + nk - 2 * side, 5, 5).start()
        total = near_total(own_k)
        used = range(7)
    else:
        for i, o in enumerate(order[:-1]):
            u2[i] = near_total(own_k + o).astype(BF16)
            step_sum(own_k + o, i, i).start()
        total = near_total(own_k)
        used = range(len(order) - 1)
    total = total + hidp[...]
    for sem in used:
        if nk != 8 or sem >= 3:
            total = total + arrived(sem)
    y = layer_norm(total, egain, ebias)
    out_ref[:, 0:half] = y[0:ROWS, :].astype(BF16)
    out_ref[:, half:dim] = y[ROWS : 2 * ROWS, :].astype(BF16)

    gather_drain(xt, 0)
    gather_drain(xm, 1)
    gather_drain(xg, 2)
    for i in range(nm):
        scatter_all(wb.at[gq * nm + i, c], w_send.at[i], w_recv.at[i, 0]).wait_send()
        for g in range(1, share):
            for n in range(4):
                group_piece(gq * nm + i, n, g).wait_send()
    for m in range(4):
        for n in range(4):
            sib_piece(m, c, n).wait_send()
    scatter_all(yrecv, a_send.at[0], a_recv.at[0]).wait_send()
    scatter_all(cb.at[c], a_send.at[2], a_recv.at[2]).wait_send()
    to_sib(cb.at[c], cb.at[c], 0).wait_send()
    to_sib(hid.at[c], hid.at[c], 1).wait_send()
    to_sib(zoth, zsib, 2).wait_send()
    for i in range(3):
        pltpu.make_async_remote_copy(
            src_ref=tsum.at[res],
            dst_ref=r1.at[i],
            send_sem=f1_send.at[i],
            recv_sem=f1_recv.at[i, 0],
            device_id=chip(z + 1),
            device_id_type=MESH,
        ).wait_send()
    for sem in used:
        step_sum(own_k, sem, sem).wait_send()
    st_store.wait()


def step(nz, share, *args):
    tokens, state = args[0], args[1]
    dim = tokens.shape[1]
    half = dim // 2
    nk = nz // STRIDE
    nm = 4 // share
    ff = args[24].shape[2]
    args = list(args)
    args[5], args[8] = args[5].T, args[8].T
    for i in (7, 10, 13, 15, 16, 18, 19, 20, 21):
        args[i] = args[i].reshape(1, dim)
    small = [5, 6, 7, 8, 9, 10, 11, 12, 13, 14, 15, 16, 18, 19, 20, 21, 22, 23]
    operands = [args[i] for i in [0, 1, 2, 3, 4, 17] + small + [24, 25, 26]]
    vmem = pl.BlockSpec(memory_space=pltpu.VMEM)
    hbm = pl.BlockSpec(memory_space=pl.ANY)
    dma = pltpu.SemaphoreType.DMA
    heads = (nz, 8, 128)
    rows = (STRIDE, nk, 8, half)
    scratch = [
        pltpu.VMEM(tokens.shape, BF16),
        *[pltpu.VMEM(args[i].shape, args[i].dtype) for i in small],
        pltpu.VMEM(state.shape, F32),
        pltpu.VMEM(state.shape, F32),
        pltpu.VMEM((nm, 32, dim), BF16),
        pltpu.VMEM((nm, nz, 16, 128), BF16),
        pltpu.VMEM((4, 2, nz, 16, 128), BF16),
        pltpu.VMEM((half, 1024), BF16),
        pltpu.VMEM(rows, BF16),
        pltpu.VMEM(rows, BF16),
        pltpu.VMEM((STRIDE, nk, nk, 8, 128), BF16),
        pltpu.VMEM((2, nk, 8, dim), F32),
        pltpu.VMEM((2, ROWS * nz, dim), BF16),
        pltpu.VMEM(heads, BF16),
        pltpu.VMEM(heads, BF16),
        pltpu.VMEM((2,) + heads, BF16),
        pltpu.VMEM((8, 128), BF16),
        pltpu.VMEM((8, dim), F32),
        pltpu.VMEM((8, half), F32),
        pltpu.VMEM((8, half), F32),
        pltpu.VMEM(heads, F32),
        pltpu.VMEM(heads, F32),
        pltpu.VMEM(heads, F32),
        pltpu.VMEM(heads, F32),
        pltpu.VMEM(heads, F32),
        pltpu.VMEM(heads, F32),
        pltpu.VMEM((dim, ff), BF16),
        pltpu.VMEM((dim, ff), BF16),
        pltpu.VMEM((ff, dim), BF16),
        pltpu.VMEM(rows, BF16),
        pltpu.VMEM(rows, BF16),
        pltpu.VMEM(rows, BF16),
        pltpu.VMEM(rows, BF16),
        pltpu.VMEM((3, nk, 8, half), BF16),
        pltpu.VMEM((nk, 8, half), BF16),
        pltpu.VMEM((nk, 8, half), BF16),
        dma((9,)),
        dma((nm,)),
        dma((nm, 4)),
        dma((share, nm, 4)),
        dma((4, 4)),
        dma((4, 4)),
        dma((4, 4)),
        dma((3, 7)),
        dma((3, 7)),
        dma((3, 3)),
        dma((3, 4)),
        dma((3,)),
        dma((3,)),
        dma((3,)),
        dma((3,)),
        dma((3,)),
        dma((3, nk)),
        dma((7,)),
        dma((7,)),
        dma((SMALL,)),
    ]
    return pl.pallas_call(
        functools.partial(kernel, nz, share),
        out_shape=(
            jax.ShapeDtypeStruct(tokens.shape, BF16),
            jax.ShapeDtypeStruct(state.shape, F32),
        ),
        in_specs=[hbm] * len(operands),
        out_specs=(vmem, hbm),
        scratch_shapes=scratch,
        compiler_params=pltpu.CompilerParams(
            collective_id=0, has_side_effects=True, vmem_limit_bytes=56 * 1024 * 1024
        ),
    )(*operands)


def solution(mesh):
    nz = mesh.shape["ep"] // 2
    groups = mesh.shape["grp"]
    share = 4 if groups % 4 == 0 else 2 if groups % 2 == 0 else 1
    owned, split, copied = P(("grp", "ep"), None), P("ep", None), P()
    in_specs = (
        owned,
        P(("grp", "ep"), None, None, None),
        split,
        split,
        split,
        *([copied] * 12),
        split,
        *([copied] * 4),
        owned,
        owned,
        P("ep", None, None),
        P("ep", None, None),
        P("ep", None, None),
    )
    out_specs = (owned, P(("grp", "ep"), None, None, None))
    return jax.shard_map(
        functools.partial(step, nz, share),
        mesh=mesh,
        in_specs=in_specs,
        out_specs=out_specs,
        check_vma=False,
    )
```

```python
import functools

import jax
import jax.numpy as jnp
from jax import lax
from jax.experimental import pallas as pl
from jax.experimental.pallas import tpu as pltpu
from jax.sharding import PartitionSpec as P

MESH = pl.DeviceIdType.MESH
F32 = jnp.float32
BF16 = jnp.bfloat16
SMALL = 18
ROWS = 4
HEAD = 64
STRIDE = 4


def dot(a, b):
    return jnp.dot(a, b, preferred_element_type=F32)


def lane_ids(shape):
    return lax.broadcasted_iota(jnp.int32, shape, len(shape) - 1)


def row_ids(shape):
    return lax.broadcasted_iota(jnp.int32, shape, len(shape) - 2)


def kernel(
    nz,
    share,
    tok_hbm,
    state_hbm,
    wr_hbm,
    wk_hbm,
    wv_hbm,
    wo_hbm,
    *rest,
):
    small_hbm, rest = rest[:SMALL], rest[SMALL:]
    run(nz, share, tok_hbm, state_hbm, (wr_hbm, wk_hbm, wv_hbm, wo_hbm), small_hbm, *rest)


def run(
    nz,
    share,
    tok_hbm,
    state_hbm,
    w_hbm,
    small_hbm,
    eg_hbm,
    eu_hbm,
    ed_hbm,
    out_ref,
    next_hbm,
    tok_ref,
    *rest,
):
    small, rest = rest[:SMALL], rest[SMALL:]
    work(nz, share, tok_hbm, state_hbm, w_hbm, small_hbm, eg_hbm, eu_hbm, ed_hbm,
         out_ref, next_hbm, tok_ref, small, *rest)


def work(
    nz,
    share,
    tok_hbm,
    state_hbm,
    w_hbm,
    small_hbm,
    eg_hbm,
    eu_hbm,
    ed_hbm,
    out_ref,
    next_hbm,
    tok_ref,
    small,
    st,
    sn,
    wstage,
    wsend,
    wb,
    em,
    xt,
    xm,
    xg,
    x2,
    hid,
    ysend,
    yrecv,
    cb,
    csend,
    tok8,
    tokp,
    hidp,
    dh,
    ah,
    gh,
    ro,
    sv,
    bh,
    eg,
    eu,
    ed,
    zown,
    zoth,
    zsib,
    tsum,
    r1,
    u2,
    r2,
    ld_sem,
    w_send,
    w_recv,
    q_send,
    q_recv,
    s_send,
    s_recv,
    l1_send,
    l1_recv,
    l2_send,
    l2_recv,
    a_send,
    a_recv,
    x_send,
    x_recv,
    f1_send,
    f1_recv,
    f2_send,
    f2_recv,
    small_sem,
):
    (
        dl1, dl2, doff, cl1, cl2, coff, gl1, gl2, blend,
        sscale, hgain, hbias, mgain, mbias, egain, ebias, routes, rweight,
    ) = small
    nk = nz // STRIDE
    dim = HEAD * nz
    half = dim // 2
    nm = 4 // share
    quarter = nz // 4
    ep = lax.axis_index("ep")
    grp = lax.axis_index("grp")
    z = ep // 2
    c = ep % 2
    gq = grp % share
    gbase = grp - gq
    res = z % STRIDE
    own_k = z // STRIDE
    sib = {"ep": z * 2 + 1 - c}

    def chip(zt):
        return {"ep": (zt % nz) * 2 + c}

    def slot_of(zt):
        return (zt % STRIDE) * nk + zt // STRIDE

    def far_first(j):
        d = nz // 2 - (j + 1) // 2
        return (z + nz + d * (1 - 2 * (j % 2))) % nz

    bar = pltpu.get_barrier_semaphore()

    @pl.loop(0, nz - 1)
    def _(j):
        pl.semaphore_signal(bar, inc=1, device_id=chip(far_first(j)), device_id_type=MESH)

    pl.semaphore_signal(bar, inc=1, device_id=sib, device_id_type=MESH)
    for i in range(1, share):
        pl.semaphore_signal(
            bar, inc=1, device_id={"grp": gbase + (gq + i) % share}, device_id_type=MESH
        )

    tok_load = pltpu.make_async_copy(tok_hbm, tok_ref, ld_sem.at[8])
    tok_load.start()
    for i in range(nm):
        for m in range(4):
            if m % nm == i:

                @pl.when(gq == m // nm)
                def _(i=i, m=m):
                    pltpu.make_async_copy(w_hbm[m], wstage.at[i], ld_sem.at[i]).start()

    st_load = pltpu.make_async_copy(state_hbm, st, ld_sem.at[4])
    eg_load = pltpu.make_async_copy(eg_hbm.at[0], eg, ld_sem.at[5])
    eu_load = pltpu.make_async_copy(eu_hbm.at[0], eu, ld_sem.at[6])
    ed_load = pltpu.make_async_copy(ed_hbm.at[0], ed, ld_sem.at[7])
    small_loads = [
        pltpu.make_async_copy(a, b, small_sem.at[i])
        for i, (a, b) in enumerate(zip(small_hbm, small))
    ]
    for cp in small_loads:
        cp.start()
    st_load.start()
    eg_load.start()
    eu_load.start()
    ed_load.start()

    lane128 = lane_ids((8, 128))
    left = lane128 < HEAD
    top = row_ids((8, 128)) < ROWS
    lane16 = lane_ids((16, 128))
    left16 = lane16 < HEAD

    tok_load.wait()
    tok = tok_ref[...].astype(F32)
    tok8[0:ROWS, :] = tok
    tok8[ROWS : 2 * ROWS, :] = tok
    tokp[0:ROWS, :] = tok[:, :half]
    tokp[ROWS : 2 * ROWS, :] = tok[:, half:]
    xt[res, own_k] = tokp[...].astype(BF16)

    for i in range(nm):
        pltpu.make_async_copy(w_hbm[0], wstage.at[i], ld_sem.at[i]).wait()

        @pl.loop(0, nz // 2)
        def _(t, i=i):
            at = pl.multiple_of(t * 128, 128)
            a = wstage[i, 0:16, pl.ds(at, 128)].astype(F32)
            b = wstage[i, 16:32, pl.ds(at, 128)].astype(F32)
            wsend[i, 2 * t] = jnp.where(left16, a, pltpu.roll(b, HEAD, 1)).astype(BF16)
            wsend[i, 2 * t + 1] = jnp.where(left16, pltpu.roll(a, HEAD, 1), b).astype(BF16)

        wb[gq * nm + i, c, z] = wsend[i, z]

    for cp in small_loads:
        cp.wait()
    weight = rweight[...]
    part = weight / jnp.sum(weight, -1, keepdims=True)
    ids = routes[...]
    lanes4 = lane_ids((ROWS, 128))
    by_expert = jnp.zeros((ROWS, 128), F32)
    for k in range(ids.shape[1]):
        by_expert += jnp.where(ids[:, k : k + 1] == lanes4, part[:, k : k + 1], 0.0)
    high = by_expert.astype(BF16).astype(F32)
    low = by_expert - high
    both = jnp.where(lanes4 < HEAD, high, pltpu.roll(low, HEAD, 1))
    sv[0, 0:ROWS, :] = both
    sv[0, ROWS : 2 * ROWS, :] = both
    csend[...] = sv[0].astype(BF16)
    my_slot = slot_of(z)
    cb[c, my_slot] = csend[...]

    side = 1 - 2 * (own_k % 2)
    hk = nk // 2

    def step_copy(buf, n, slot, sem, kt):
        at = buf.at[res, slot % nk]
        return pltpu.make_async_remote_copy(
            src_ref=at,
            dst_ref=at,
            send_sem=l1_send.at[n, sem],
            recv_sem=l1_recv.at[n, sem],
            device_id=chip((kt % nk) * STRIDE + res),
            device_id_type=MESH,
        )

    def near_copies(buf, n, slot):
        k = slot % nk
        at = buf.at[res, k]
        part = k // hk
        for i, to, sem in ((0, z + 1, 0), (1, z + nz - 1, 1), (2, z + nz + 2 - 4 * part, 2 + part)):
            pltpu.make_async_remote_copy(
                src_ref=at,
                dst_ref=at,
                send_sem=l2_send.at[n, i],
                recv_sem=l2_recv.at[n, sem],
                device_id=chip(to),
                device_id_type=MESH,
            ).start()

    direct = [(0, -1), (1, 1)] + ([(2, -2), (3, 2)] if nk > 4 else []) if nk > 2 else []
    direct += [(6, nk // 2)] if nk in (2, 4) else []
    onward = [(4, -3), (5, 3), (6, 4)] if nk == 8 else []

    def gather_start(buf, n):
        for sem, o in reversed(direct):
            step_copy(buf, n, own_k, sem, own_k + nk - o).start()
        near_copies(buf, n, own_k)

    def gather_direct(buf, n):
        for sem, o in direct:
            step_copy(buf, n, own_k + nk + o, sem, own_k).wait_recv()
            if sem == 2 and onward:
                step_copy(buf, n, own_k + nk - 2, 4, own_k + 1).start()
            if sem == 3 and onward:
                step_copy(buf, n, own_k + nk + 2, 5, own_k + nk - 1).start()
                step_copy(buf, n, own_k + nk - 2 * side, 6, own_k + nk + 2 * side).start()
            if sem < 2 or not onward:
                near_copies(buf, n, own_k + nk + o)
        if onward:
            near_copies(buf, n, own_k + nk - 2)
            near_copies(buf, n, own_k + nk + 2)

    def gather_onward(buf, n):
        for sem, o in onward:
            step_copy(buf, n, own_k + nk + o, sem, own_k).wait_recv()
            near_copies(buf, n, own_k + nk + o)

    def near_all(buf, n, i, sem, r, k0, count):
        at = buf.at[r, pl.ds(k0, count)]
        return pltpu.make_async_remote_copy(
            src_ref=at,
            dst_ref=at,
            send_sem=l2_send.at[n, i],
            recv_sem=l2_recv.at[n, sem],
            device_id=chip(z + 1),
            device_id_type=MESH,
        )

    def gather_wait(buf, n):
        near_all(buf, n, 0, 0, (res + STRIDE - 1) % STRIDE, 0, nk).wait_recv()
        near_all(buf, n, 1, 1, (res + 1) % STRIDE, 0, nk).wait_recv()
        near_all(buf, n, 2, 2, (res + 2) % STRIDE, 0, hk).wait_recv()
        near_all(buf, n, 2, 3, (res + 2) % STRIDE, hk, hk).wait_recv()

    def gather_drain(buf, n):
        for sem, _ in direct + onward:
            step_copy(buf, n, own_k, sem, own_k).wait_send()
        for i in range(3):
            near_all(buf, n, i, i, res, 0, nk).wait_send()

    def scatter(src_of, dst, send_sem, recv_sem):
        @pl.loop(0, nz - 1)
        def _(j):
            zt = far_first(j)
            pltpu.make_async_remote_copy(
                src_ref=src_of(zt),
                dst_ref=dst,
                send_sem=send_sem,
                recv_sem=recv_sem,
                device_id=chip(zt),
                device_id_type=MESH,
            ).start()

    def scatter_all(block, send_sem, recv_sem):
        return pltpu.make_async_remote_copy(
            src_ref=block.at[pl.ds(0, nz - 1)],
            dst_ref=block.at[pl.ds(0, nz - 1)],
            send_sem=send_sem,
            recv_sem=recv_sem,
            device_id=chip(z),
            device_id_type=MESH,
        )

    tokb = tok8[...].astype(BF16)

    def dot_t(a, b):
        return lax.dot_general(a, b, (((1,), (1,)), ((), ())), preferred_element_type=F32)

    squash = jnp.tanh(dot_t(tokb, dl1[...])).astype(BF16)
    lowl = dot_t(tokb, cl1[...]).astype(BF16)
    opened = jax.nn.sigmoid(dot(tokb, gl1[...])).astype(BF16)

    for j in range(nz // 2):
        cols = slice(128 * j, 128 * j + 128)

        def two_heads(ref, tile, j=j):
            ref[2 * j] = tile
            ref[2 * j + 1] = pltpu.roll(tile, HEAD, 1)

        pre = doff[:, cols] + dot(squash, dl2[:, cols])
        two_heads(dh, jnp.exp(-(jnp.exp(jnp.full((8, 128), -0.5, F32)) * jax.nn.sigmoid(pre))))
        two_heads(ah, jax.nn.sigmoid(coff[:, cols] + dot(lowl, cl2[:, cols])))
        two_heads(gh, dot(opened, gl2[:, cols]))

    pl.semaphore_wait(bar, nz - 1 + 1 + share - 1)

    gather_start(xt, 0)
    for i in range(nm):
        m = gq * nm + i
        scatter(
            lambda zt, i=i: wsend.at[i, zt],
            wb.at[m, c, z],
            w_send.at[i],
            w_recv.at[i, z // quarter],
        )

    gather_direct(xt, 0)

    def piece(m, core, n, to, send_sem, recv_sem):
        at = wb.at[m, core, pl.ds(n * quarter, quarter)]
        return pltpu.make_async_remote_copy(
            src_ref=at,
            dst_ref=at,
            send_sem=send_sem,
            recv_sem=recv_sem,
            device_id=to,
            device_id_type=MESH,
        )

    def sib_piece(m, core, n):
        return piece(m, core, n, sib, s_send.at[m, n], s_recv.at[m, n])

    def group_piece(m, n, g):
        to = {"grp": gbase + (gq + g) % share} if share > 1 else sib
        return piece(m, c, n, to, q_send.at[g, m % nm, n], q_recv.at[m, n])

    def hand_out(i, m):
        for d in range(4):
            n = (z // quarter + d) % 4
            count = quarter - 1 if d == 0 else quarter
            at = wb.at[m, c, pl.ds(0, count)]
            pltpu.make_async_remote_copy(
                src_ref=at,
                dst_ref=at,
                send_sem=w_send.at[i],
                recv_sem=w_recv.at[i, n],
                device_id=chip(z),
                device_id_type=MESH,
            ).wait_recv()
            for g in range(1, share):
                group_piece(m, n, g).start()
            sib_piece(m, c, n).start()

    def pass_on(m):
        for n in range(4):
            group_piece(m, n, 0).wait_recv()
            sib_piece(m, c, n).start()

    def mine(m):
        return gq == m // nm

    for m in range(3):
        pl.when(mine(m))(functools.partial(hand_out, m % nm, m))
    gather_onward(xt, 0)
    if share > 1:
        for m in range(3):
            pl.when(jnp.logical_not(mine(m)))(functools.partial(pass_on, m))

    def widen(m, at):
        keep = left16.astype(F32).astype(BF16)
        drop = (1.0 - left16.astype(F32)).astype(BF16)
        for hk in range(2):

            @pl.loop(0, nz // 2)
            def _(zz, hk=hk):
                for core in range(2):
                    tile = wb[m, core, hk * (nz // 2) + zz]
                    base = pl.multiple_of(zz * 64 + core * 32, 32)
                    cols = slice(at + hk * 128, at + hk * 128 + 128)
                    em[pl.ds(base, 16), cols] = tile * keep
                    em[pl.ds(pl.multiple_of(base + 16, 16), 16), cols] = tile * drop

    def rows_of(value):
        return value.astype(F32).reshape(8 * nz, half).astype(BF16)

    top3 = row_ids((nz, 8, 128)) < ROWS
    left3 = lane_ids((nz, 8, 128)) < HEAD
    topw = (row_ids((8 * nz, 128)) % 8) < ROWS

    def fold(r):
        a = jnp.where(topw, r[:, 0:128], r[:, 128:256])
        a = (a + pltpu.roll(a, HEAD, 1)).reshape(nz, 8, 128)
        return a + pltpu.roll(a, ROWS, 1)

    for m in range(3):
        for n in range(4):
            sib_piece(m, 1 - c, n).wait_recv()
        widen(m, m * 256)

    gather_wait(xt, 0)
    xv = rows_of(xt[...])
    cr = fold(dot(xv, em[:, 0:256]))
    ck = fold(dot(xv, em[:, 256:512]))
    cv = fold(dot(xv, em[:, 512:768]))
    ysend[...] = jnp.where(top3, jnp.where(left3, cr, ck), cv).astype(BF16)
    scatter(lambda zt: ysend.at[slot_of(zt)], yrecv.at[z], a_send.at[0], a_recv.at[0])
    yrecv[z] = ysend[my_slot]
    scatter(lambda zt: csend, cb.at[c, my_slot], a_send.at[2], a_recv.at[2])
    topk = row_ids((nk, 8, 128)) < ROWS
    leftk = lane_ids((nk, 8, 128)) < HEAD
    for s in range(2):
        for m in range(half // 128):
            one = xt[2 * s, :, :, 128 * m : 128 * m + 128].astype(F32)
            two = xt[2 * s + 1, :, :, 128 * m : 128 * m + 128].astype(F32)
            x2[s, :, :, 128 * m : 128 * m + 128] = jnp.where(topk, one, pltpu.roll(two, ROWS, 1))
            x2[s, :, :, half + 128 * m : half + 128 * m + 128] = jnp.where(
                topk, pltpu.roll(one, ROWS, 1), two
            )
    pl.when(mine(3))(functools.partial(hand_out, 3 % nm, 3))
    st_load.wait()
    scatter_all(yrecv, a_send.at[0], a_recv.at[0]).wait_recv()

    eye = (
        lax.broadcasted_iota(jnp.int32, (HEAD, HEAD), 0)
        == lax.broadcasted_iota(jnp.int32, (HEAD, HEAD), 1)
    ).astype(F32)

    def pick(ref, j):
        tile = jnp.broadcast_to(ref[:, 128 * j : 128 * j + 128], (8, 128))
        return tile, pltpu.roll(tile, HEAD, 1)

    blends = []
    for j in range(nz // 2):
        blends += pick(blend, j)
    for h in range(nz):
        bh[h] = blends[h]

    @pl.loop(0, nz // 2)
    def _(pair):
        for h in (2 * pair, 2 * pair + 1):
            y = yrecv[h].astype(F32)
            turned = pltpu.roll(y, ROWS, 0)
            rk = jnp.where(top, y, turned)
            v = jnp.where(top, turned, y)
            r = jnp.where(left, rk, 0.0)
            k = jnp.where(left, pltpu.roll(rk, HEAD, 1), 0.0)
            a = ah[h]
            unit = k * lax.rsqrt(jnp.sum(k * k, -1, keepdims=True) + 1e-06)
            written = k * (1.0 + (a - 1.0) * bh[h])
            ua = unit * a
            scale = sscale[pl.ds(h, 1), :]
            own = jnp.sum((r * written)[:, 0:HEAD] * scale, -1, keepdims=True)
            d = dh[h]
            sv[h] = own * v
            for t in range(ROWS):
                one = slice(t, t + 1)
                s = st[t, h]
                removed = jnp.sum(s * unit[one, 0:HEAD], -1, keepdims=True)
                vcol = jnp.sum(eye * v[one, 0:HEAD], -1, keepdims=True)
                n = s * d[one, 0:HEAD] - removed * ua[one, 0:HEAD] + vcol * written[one, 0:HEAD]
                sn[t, h] = n
                read = jnp.sum(n * r[one, 0:HEAD], -1, keepdims=True)
                row = jnp.sum(eye * read, 0, keepdims=True)
                ro[h, t : t + 1, 0:HEAD] = row
                ro[h, ROWS + t : ROWS + t + 1, 0:HEAD] = row

    st_store = pltpu.make_async_copy(sn, next_hbm, ld_sem.at[4])
    st_store.start()

    def mixer_head(h, gain, bias):
        x = jnp.where(left, ro[h], 0.0)
        mean = jnp.sum(x, -1, keepdims=True) * (1.0 / HEAD)
        dev = jnp.where(left, x - mean, 0.0)
        var = jnp.sum(dev * dev, -1, keepdims=True) * (1.0 / HEAD)
        normed = dev * lax.rsqrt(var + 0.00064) * gain + bias
        return (normed + sv[h]) * gh[h]

    def mixer_pair(j):
        g0, g1 = pick(hgain, j)
        b0, b1 = pick(hbias, j)
        one, two = mixer_head(2 * j, g0, b0), mixer_head(2 * j + 1, g1, b1)
        return jnp.where(left, one, pltpu.roll(two, HEAD, 1))

    for j in range(nz // 4):
        tile = jnp.where(top, mixer_pair(j), mixer_pair(nz // 4 + j))
        xm[res, own_k, :, 128 * j : 128 * j + 128] = tile.astype(BF16)

    gather_start(xm, 1)
    if share > 1:
        pl.when(jnp.logical_not(mine(3)))(functools.partial(pass_on, 3))
    gather_direct(xm, 1)
    gather_onward(xm, 1)
    for n in range(4):
        sib_piece(3, 1 - c, n).wait_recv()
    widen(3, 768)
    gather_wait(xm, 1)
    co = fold(dot(rows_of(xm[...]), em[:, 768:1024]))
    xg[res, own_k] = jnp.where(
        leftk,
        jnp.where(topk, co[0:nk], co[nk : 2 * nk]),
        jnp.where(topk, co[2 * nk : 3 * nk], co[3 * nk :]),
    ).astype(BF16)
    gather_start(xg, 2)

    scatter_all(cb.at[c], a_send.at[2], a_recv.at[2]).wait_recv()

    def to_sib(src, dst, n):
        return pltpu.make_async_remote_copy(
            src_ref=src,
            dst_ref=dst,
            send_sem=x_send.at[n],
            recv_sem=x_recv.at[n],
            device_id=sib,
            device_id_type=MESH,
        )

    to_sib(cb.at[c], cb.at[c], 0).start()

    gather_direct(xg, 2)
    gather_onward(xg, 2)
    gather_wait(xg, 2)
    for j in range(nz // 2):
        cols = slice(128 * j, 128 * j + 128)
        one = xg[2 * j % STRIDE, 2 * j // STRIDE].astype(F32)
        two = xg[(2 * j + 1) % STRIDE, (2 * j + 1) // STRIDE].astype(F32)
        x2[0, :, :, cols] += jnp.where(leftk, one, pltpu.roll(two, HEAD, 2))
        x2[1, :, :, cols] += jnp.where(leftk, pltpu.roll(one, HEAD, 2), two)

    some = max(1, nk // 2)
    for s in range(2):
        for k in range(0, nk, some):
            x = x2[s, k : k + some]
            dev = x - jnp.mean(x, -1, keepdims=True)
            var = jnp.mean(dev * dev, -1, keepdims=True)
            y = dev * lax.rsqrt(var + 1e-05) * mgain[...] + mbias[...]
            x2[s, k : k + some] = y
            base = 8 * (s * nk + k)
            hid[c, base : base + 8 * some, :] = y.reshape(8 * some, dim).astype(BF16)

    to_sib(hid.at[c], hid.at[c], 1).start()

    topp = row_ids((8, half)) < ROWS

    def packed(ref):
        return jnp.where(topp, ref[:, 0:half], ref[:, half:dim])

    def row_total(x):
        s = jnp.broadcast_to(jnp.sum(x, -1, keepdims=True), (8, 128))
        s = s + pltpu.roll(s, ROWS, 0)
        return s[:, 0:1] * (1.0 / dim)

    def layer_norm(x, gain, bias):
        dev = x - row_total(x)
        var = row_total(dev * dev)
        return dev * lax.rsqrt(var + 1e-05) * packed(gain) + packed(bias)

    two_rows = x2[res // 2, own_k].astype(BF16).astype(F32)
    mine = row_ids((8, dim)) // ROWS == res % 2
    doubled = jnp.where(mine, two_rows, pltpu.roll(two_rows, ROWS, 0))
    hidp[...] = jnp.where(topp, doubled[:, 0:half], doubled[:, half:dim])

    eg_load.wait()
    eu_load.wait()
    ed_load.wait()
    to_sib(cb.at[1 - c], cb.at[1 - c], 0).wait_recv()

    def expert(core):
        xv = hid[core]
        lane3 = lane_ids((nz, 8, 128))
        hit = (lane3 == ep) | (lane3 == ep + HEAD)
        coef = jnp.sum(jnp.where(hit, cb[core].astype(F32), 0.0), -1, keepdims=True)
        top1 = row_ids((nk, 8, 1)) < ROWS
        coef = jnp.concatenate(
            [
                jnp.where(top1, coef[0:nk], coef[nk : 2 * nk]),
                jnp.where(top1, coef[2 * nk : 3 * nk], coef[3 * nk :]),
            ],
            0,
        ).reshape(ROWS * nz, 1)
        gate = dot(xv, eg[...])
        up = dot(xv, eu[...])
        inner = (gate * jax.nn.sigmoid(gate) * up).astype(BF16)
        return inner, coef

    def down(inner, coef, z, j, width):
        cols = slice(j * width, (j + 1) * width)
        low = dot(inner, ed[:, cols]) * coef
        high = dot(inner, ed[:, half + j * width : half + (j + 1) * width]) * coef
        low, high = low.reshape(2, nk, 8, width), high.reshape(2, nk, 8, width)
        keep = row_ids((nk, 8, width)) < ROWS
        for s in range(2):
            one = jnp.where(keep, low[s], pltpu.roll(high[s], ROWS, 1))
            two = jnp.where(keep, pltpu.roll(low[s], ROWS, 1), high[s])
            z[2 * s, :, :, cols] = one.astype(BF16)
            z[2 * s + 1, :, :, cols] = two.astype(BF16)

    width = min(256, half)
    inner, coef = expert(c)
    for j in range(half // width):
        down(inner, coef, zown, j, width)
    to_sib(hid.at[1 - c], hid.at[1 - c], 1).wait_recv()
    inner, coef = expert(1 - c)
    for j in range(half // width):
        down(inner, coef, zoth, j, width)
    to_sib(zoth, zsib, 2).start()
    to_sib(zoth, zsib, 2).wait_recv()
    tsum[...] = (zown[...].astype(F32) + zsib[...].astype(F32)).astype(BF16)

    def near_sum(slot):
        k = slot % nk
        part = k // hk
        up, down_, far = (res + 1) % STRIDE, (res + STRIDE - 1) % STRIDE, (res + 2) % STRIDE
        return [
            pltpu.make_async_remote_copy(
                src_ref=tsum.at[r, k],
                dst_ref=r1.at[i, k],
                send_sem=f1_send.at[i],
                recv_sem=f1_recv.at[i, k],
                device_id=chip(to),
                device_id_type=MESH,
            )
            for i, (to, r) in enumerate(
                ((z + 1, up), (z + nz - 1, down_), (z + nz + 2 - 4 * part, far))
            )
        ]

    def step_sum(kt, src, sem):
        return pltpu.make_async_remote_copy(
            src_ref=u2.at[src],
            dst_ref=r2.at[sem],
            send_sem=f2_send.at[sem],
            recv_sem=f2_recv.at[sem],
            device_id=chip((kt % nk) * STRIDE + res),
            device_id_type=MESH,
        )

    def near_total(slot):
        k = slot % nk
        for cp in near_sum(k):
            cp.wait_recv()
        return (
            tsum[res, k].astype(F32)
            + r1[0, k].astype(F32)
            + r1[1, k].astype(F32)
            + r1[2, k].astype(F32)
        )

    def arrived(sem):
        step_sum(own_k, 0, sem).wait_recv()
        return r2[sem].astype(F32)

    if nk == 8:
        order = [nk + 4, nk - 3, nk + 3, nk - 2 * side, nk + 2 * side, nk - 1, nk + 1, nk]
    else:
        order = [nk // 2] + ([1, nk - 1] if nk == 4 else []) + [nk]
    for o in order:
        for cp in near_sum(own_k + o):
            cp.start()
    if nk == 8:
        u2[0] = near_total(own_k + 4).astype(BF16)
        step_sum(own_k + nk + 2 * side * -1, 0, 0).start()
        u2[1] = near_total(own_k + nk - 3 * side).astype(BF16)
        step_sum(own_k + nk - side, 1, 1).start()
        u2[2] = near_total(own_k + nk + 3 * side).astype(BF16)
        step_sum(own_k + nk + side, 2, 2).start()
        u2[3] = near_total(own_k + nk - side).astype(BF16)
        step_sum(own_k + nk - side, 3, 3).start()
        u2[4] = near_total(own_k + nk + side).astype(BF16)
        step_sum(own_k + nk + side, 4, 4).start()
        part_b = near_total(own_k + nk + 2 * side)
        part_a = near_total(own_k + nk - 2 * side)
        u2[6] = (part_b + arrived(1)).astype(BF16)
        step_sum(own_k + nk + 2 * side, 6, 6).start()
        u2[5] = (part_a + arrived(2) + arrived(0)).astype(BF16)
        step_sum(own_k + nk - 2 * side, 5, 5).start()
        total = near_total(own_k)
        used = range(7)
    else:
        for i, o in enumerate(order[:-1]):
            u2[i] = near_total(own_k + o).astype(BF16)
            step_sum(own_k + o, i, i).start()
        total = near_total(own_k)
        used = range(len(order) - 1)
    total = total + hidp[...]
    for sem in used:
        if nk != 8 or sem >= 3:
            total = total + arrived(sem)
    y = layer_norm(total, egain, ebias)
    out_ref[:, 0:half] = y[0:ROWS, :].astype(BF16)
    out_ref[:, half:dim] = y[ROWS : 2 * ROWS, :].astype(BF16)

    gather_drain(xt, 0)
    gather_drain(xm, 1)
    gather_drain(xg, 2)
    for i in range(nm):
        scatter_all(wb.at[gq * nm + i, c], w_send.at[i], w_recv.at[i, 0]).wait_send()
        for g in range(1, share):
            for n in range(4):
                group_piece(gq * nm + i, n, g).wait_send()
    for m in range(4):
        for n in range(4):
            sib_piece(m, c, n).wait_send()
    scatter_all(yrecv, a_send.at[0], a_recv.at[0]).wait_send()
    scatter_all(cb.at[c], a_send.at[2], a_recv.at[2]).wait_send()
    to_sib(cb.at[c], cb.at[c], 0).wait_send()
    to_sib(hid.at[c], hid.at[c], 1).wait_send()
    to_sib(zoth, zsib, 2).wait_send()
    for i in range(3):
        pltpu.make_async_remote_copy(
            src_ref=tsum.at[res],
            dst_ref=r1.at[i],
            send_sem=f1_send.at[i],
            recv_sem=f1_recv.at[i, 0],
            device_id=chip(z + 1),
            device_id_type=MESH,
        ).wait_send()
    for sem in used:
        step_sum(own_k, sem, sem).wait_send()
    st_store.wait()


def hand_back(small, state, small_out, state_out, small_buf, buf, in_sem, out_sem):
    pieces = [(small, small_buf, small_out)]
    half = state.shape[1] // 2
    for i in range(state.shape[0]):
        for part in (pl.ds(0, half), pl.ds(half, half)):
            pieces.append((state.at[i, part], buf.at[i, part], state_out.at[i, part]))
    reads = [pltpu.make_async_copy(a, b, in_sem.at[i]) for i, (a, b, _) in enumerate(pieces)]
    writes = [pltpu.make_async_copy(b, o, out_sem.at[i]) for i, (_, b, o) in enumerate(pieces)]
    for cp in reads:
        cp.start()
    for read, write in zip(reads, writes):
        read.wait()
        write.start()
    for cp in writes:
        cp.wait()


def step(nz, share, *args):
    tokens, state = args[0], args[1]
    dim = tokens.shape[1]
    half = dim // 2
    nk = nz // STRIDE
    nm = 4 // share
    ff = args[24].shape[2]
    args = list(args)
    args[5], args[8] = args[5].T, args[8].T
    for i in (7, 10, 13, 15, 16, 18, 19, 20, 21):
        args[i] = args[i].reshape(1, dim)
    small = [5, 6, 7, 8, 9, 10, 11, 12, 13, 14, 15, 16, 18, 19, 20, 21, 22, 23]
    operands = [args[i] for i in [0, 1, 2, 3, 4, 17] + small + [24, 25, 26]]
    vmem = pl.BlockSpec(memory_space=pltpu.VMEM)
    hbm = pl.BlockSpec(memory_space=pl.ANY)
    dma = pltpu.SemaphoreType.DMA
    heads = (nz, 8, 128)
    rows = (STRIDE, nk, 8, half)
    scratch = [
        pltpu.VMEM(tokens.shape, BF16),
        *[pltpu.VMEM(args[i].shape, args[i].dtype) for i in small],
        pltpu.VMEM(state.shape, F32),
        pltpu.VMEM(state.shape, F32),
        pltpu.VMEM((nm, 32, dim), BF16),
        pltpu.VMEM((nm, nz, 16, 128), BF16),
        pltpu.VMEM((4, 2, nz, 16, 128), BF16),
        pltpu.VMEM((half, 1024), BF16),
        pltpu.VMEM(rows, BF16),
        pltpu.VMEM(rows, BF16),
        pltpu.VMEM((STRIDE, nk, nk, 8, 128), BF16),
        pltpu.VMEM((2, nk, 8, dim), F32),
        pltpu.VMEM((2, ROWS * nz, dim), BF16),
        pltpu.VMEM(heads, BF16),
        pltpu.VMEM(heads, BF16),
        pltpu.VMEM((2,) + heads, BF16),
        pltpu.VMEM((8, 128), BF16),
        pltpu.VMEM((8, dim), F32),
        pltpu.VMEM((8, half), F32),
        pltpu.VMEM((8, half), F32),
        pltpu.VMEM(heads, F32),
        pltpu.VMEM(heads, F32),
        pltpu.VMEM(heads, F32),
        pltpu.VMEM(heads, F32),
        pltpu.VMEM(heads, F32),
        pltpu.VMEM(heads, F32),
        pltpu.VMEM((dim, ff), BF16),
        pltpu.VMEM((dim, ff), BF16),
        pltpu.VMEM((ff, dim), BF16),
        pltpu.VMEM(rows, BF16),
        pltpu.VMEM(rows, BF16),
        pltpu.VMEM(rows, BF16),
        pltpu.VMEM(rows, BF16),
        pltpu.VMEM((3, nk, 8, half), BF16),
        pltpu.VMEM((nk, 8, half), BF16),
        pltpu.VMEM((nk, 8, half), BF16),
        dma((9,)),
        dma((nm,)),
        dma((nm, 4)),
        dma((share, nm, 4)),
        dma((4, 4)),
        dma((4, 4)),
        dma((4, 4)),
        dma((3, 7)),
        dma((3, 7)),
        dma((3, 3)),
        dma((3, 4)),
        dma((3,)),
        dma((3,)),
        dma((3,)),
        dma((3,)),
        dma((3,)),
        dma((3, nk)),
        dma((7,)),
        dma((7,)),
        dma((SMALL,)),
    ]
    result, state_new = pl.pallas_call(
        functools.partial(kernel, nz, share),
        out_shape=(
            jax.ShapeDtypeStruct(tokens.shape, BF16),
            jax.ShapeDtypeStruct(state.shape, F32),
        ),
        in_specs=[hbm] * len(operands),
        out_specs=(vmem, hbm),
        scratch_shapes=scratch,
        compiler_params=pltpu.CompilerParams(
            collective_id=0, has_side_effects=True, vmem_limit_bytes=56 * 1024 * 1024
        ),
    )(*operands)
    return pl.pallas_call(
        hand_back,
        out_shape=(
            jax.ShapeDtypeStruct(tokens.shape, BF16),
            jax.ShapeDtypeStruct(state.shape, F32),
        ),
        in_specs=[hbm, hbm],
        out_specs=(hbm, hbm),
        scratch_shapes=[
            pltpu.VMEM(tokens.shape, BF16),
            pltpu.VMEM(state.shape, F32),
            dma((1 + 2 * state.shape[0],)),
            dma((1 + 2 * state.shape[0],)),
        ],
        compiler_params=pltpu.CompilerParams(vmem_limit_bytes=62 * 1024 * 1024),
    )(result, state_new)


def solution(mesh):
    nz = mesh.shape["ep"] // 2
    groups = mesh.shape["grp"]
    share = 4 if groups % 4 == 0 else 2 if groups % 2 == 0 else 1
    owned, split, copied = P(("grp", "ep"), None), P("ep", None), P()
    in_specs = (
        owned,
        P(("grp", "ep"), None, None, None),
        split,
        split,
        split,
        *([copied] * 12),
        split,
        *([copied] * 4),
        owned,
        owned,
        P("ep", None, None),
        P("ep", None, None),
        P("ep", None, None),
    )
    out_specs = (owned, P(("grp", "ep"), None, None, None))
    return jax.shard_map(
        functools.partial(step, nz, share),
        mesh=mesh,
        in_specs=in_specs,
        out_specs=out_specs,
        check_vma=False,
    )
```

```python
import functools

import jax
import jax.numpy as jnp
from jax import lax
from jax.experimental import pallas as pl
from jax.experimental.pallas import tpu as pltpu
from jax.sharding import PartitionSpec as P

MESH = pl.DeviceIdType.MESH
F32 = jnp.float32
BF16 = jnp.bfloat16
SMALL = 18
ROWS = 4
HEAD = 64
STRIDE = 4


def dot(a, b):
    return jnp.dot(a, b, preferred_element_type=F32)


def lane_ids(shape):
    return lax.broadcasted_iota(jnp.int32, shape, len(shape) - 1)


def row_ids(shape):
    return lax.broadcasted_iota(jnp.int32, shape, len(shape) - 2)


def kernel(
    nz,
    share,
    tok_hbm,
    state_hbm,
    wr_hbm,
    wk_hbm,
    wv_hbm,
    wo_hbm,
    *rest,
):
    small_hbm, rest = rest[:SMALL], rest[SMALL:]
    run(nz, share, tok_hbm, state_hbm, (wr_hbm, wk_hbm, wv_hbm, wo_hbm), small_hbm, *rest)


def run(
    nz,
    share,
    tok_hbm,
    state_hbm,
    w_hbm,
    small_hbm,
    eg_hbm,
    eu_hbm,
    ed_hbm,
    out_ref,
    next_hbm,
    tok_ref,
    *rest,
):
    small, rest = rest[:SMALL], rest[SMALL:]
    work(nz, share, tok_hbm, state_hbm, w_hbm, small_hbm, eg_hbm, eu_hbm, ed_hbm,
         out_ref, next_hbm, tok_ref, small, *rest)


def work(
    nz,
    share,
    tok_hbm,
    state_hbm,
    w_hbm,
    small_hbm,
    eg_hbm,
    eu_hbm,
    ed_hbm,
    out_ref,
    next_hbm,
    tok_ref,
    small,
    st,
    sn,
    wstage,
    wsend,
    wb,
    em,
    xt,
    xm,
    xg,
    x2,
    hid,
    ysend,
    yrecv,
    cb,
    csend,
    tok8,
    tokp,
    hidp,
    dh,
    ah,
    gh,
    ro,
    sv,
    bh,
    eg,
    eu,
    ed,
    zown,
    zoth,
    zsib,
    tsum,
    r1,
    u2,
    r2,
    ld_sem,
    w_send,
    w_recv,
    q_send,
    q_recv,
    s_send,
    s_recv,
    l1_send,
    l1_recv,
    l2_send,
    l2_recv,
    a_send,
    a_recv,
    x_send,
    x_recv,
    f1_send,
    f1_recv,
    f2_send,
    f2_recv,
    small_sem,
):
    (
        dl1, dl2, doff, cl1, cl2, coff, gl1, gl2, blend,
        sscale, hgain, hbias, mgain, mbias, egain, ebias, routes, rweight,
    ) = small
    nk = nz // STRIDE
    dim = HEAD * nz
    half = dim // 2
    nm = 4 // share
    quarter = nz // 4
    ep = lax.axis_index("ep")
    grp = lax.axis_index("grp")
    z = ep // 2
    c = ep % 2
    gq = grp % share
    gbase = grp - gq
    res = z % STRIDE
    own_k = z // STRIDE
    sib = {"ep": z * 2 + 1 - c}

    def chip(zt):
        return {"ep": (zt % nz) * 2 + c}

    def slot_of(zt):
        return (zt % STRIDE) * nk + zt // STRIDE

    def far_first(j):
        d = nz // 2 - (j + 1) // 2
        return (z + nz + d * (1 - 2 * (j % 2))) % nz

    bar = pltpu.get_barrier_semaphore()

    @pl.loop(0, nz - 1)
    def _(j):
        pl.semaphore_signal(bar, inc=1, device_id=chip(far_first(j)), device_id_type=MESH)

    pl.semaphore_signal(bar, inc=1, device_id=sib, device_id_type=MESH)
    for i in range(1, share):
        pl.semaphore_signal(
            bar, inc=1, device_id={"grp": gbase + (gq + i) % share}, device_id_type=MESH
        )

    tok_load = pltpu.make_async_copy(tok_hbm, tok_ref, ld_sem.at[8])
    tok_load.start()
    for i in range(nm):
        for m in range(4):
            if m % nm == i:

                @pl.when(gq == m // nm)
                def _(i=i, m=m):
                    pltpu.make_async_copy(w_hbm[m], wstage.at[i], ld_sem.at[i]).start()

    st_load = pltpu.make_async_copy(state_hbm, st, ld_sem.at[4])
    eg_load = pltpu.make_async_copy(eg_hbm.at[0], eg, ld_sem.at[5])
    eu_load = pltpu.make_async_copy(eu_hbm.at[0], eu, ld_sem.at[6])
    ed_load = pltpu.make_async_copy(ed_hbm.at[0], ed, ld_sem.at[7])
    small_loads = [
        pltpu.make_async_copy(a, b, small_sem.at[i])
        for i, (a, b) in enumerate(zip(small_hbm, small))
    ]
    for cp in small_loads:
        cp.start()
    st_load.start()
    eg_load.start()
    eu_load.start()
    ed_load.start()

    lane128 = lane_ids((8, 128))
    left = lane128 < HEAD
    top = row_ids((8, 128)) < ROWS
    lane16 = lane_ids((16, 128))
    left16 = lane16 < HEAD

    tok_load.wait()
    tok = tok_ref[...].astype(F32)
    tok8[0:ROWS, :] = tok
    tok8[ROWS : 2 * ROWS, :] = tok
    tokp[0:ROWS, :] = tok[:, :half]
    tokp[ROWS : 2 * ROWS, :] = tok[:, half:]
    xt[res, own_k] = tokp[...].astype(BF16)

    for i in range(nm):
        pltpu.make_async_copy(w_hbm[0], wstage.at[i], ld_sem.at[i]).wait()

        @pl.loop(0, nz // 2)
        def _(t, i=i):
            at = pl.multiple_of(t * 128, 128)
            a = wstage[i, 0:16, pl.ds(at, 128)].astype(F32)
            b = wstage[i, 16:32, pl.ds(at, 128)].astype(F32)
            wsend[i, 2 * t] = jnp.where(left16, a, pltpu.roll(b, HEAD, 1)).astype(BF16)
            wsend[i, 2 * t + 1] = jnp.where(left16, pltpu.roll(a, HEAD, 1), b).astype(BF16)

        wb[gq * nm + i, c, z] = wsend[i, z]

    for cp in small_loads:
        cp.wait()
    weight = rweight[...]
    part = weight / jnp.sum(weight, -1, keepdims=True)
    ids = routes[...]
    lanes4 = lane_ids((ROWS, 128))
    by_expert = jnp.zeros((ROWS, 128), F32)
    for k in range(ids.shape[1]):
        by_expert += jnp.where(ids[:, k : k + 1] == lanes4, part[:, k : k + 1], 0.0)
    high = by_expert.astype(BF16).astype(F32)
    low = by_expert - high
    both = jnp.where(lanes4 < HEAD, high, pltpu.roll(low, HEAD, 1))
    sv[0, 0:ROWS, :] = both
    sv[0, ROWS : 2 * ROWS, :] = both
    csend[...] = sv[0].astype(BF16)
    my_slot = slot_of(z)
    cb[c, my_slot] = csend[...]

    side = 1 - 2 * (own_k % 2)
    hk = nk // 2

    def step_copy(buf, n, slot, sem, kt):
        at = buf.at[res, slot % nk]
        return pltpu.make_async_remote_copy(
            src_ref=at,
            dst_ref=at,
            send_sem=l1_send.at[n, sem],
            recv_sem=l1_recv.at[n, sem],
            device_id=chip((kt % nk) * STRIDE + res),
            device_id_type=MESH,
        )

    def near_copies(buf, n, slot):
        k = slot % nk
        at = buf.at[res, k]
        part = k // hk
        for i, to, sem in ((0, z + 1, 0), (1, z + nz - 1, 1), (2, z + nz + 2 - 4 * part, 2 + part)):
            pltpu.make_async_remote_copy(
                src_ref=at,
                dst_ref=at,
                send_sem=l2_send.at[n, i],
                recv_sem=l2_recv.at[n, sem],
                device_id=chip(to),
                device_id_type=MESH,
            ).start()

    direct = [(0, -1), (1, 1)] + ([(2, -2), (3, 2)] if nk > 4 else []) if nk > 2 else []
    direct += [(6, nk // 2)] if nk in (2, 4) else []
    onward = [(4, -3), (5, 3), (6, 4)] if nk == 8 else []

    def gather_start(buf, n):
        for sem, o in reversed(direct):
            step_copy(buf, n, own_k, sem, own_k + nk - o).start()
        near_copies(buf, n, own_k)

    def gather_direct(buf, n):
        for sem, o in direct:
            step_copy(buf, n, own_k + nk + o, sem, own_k).wait_recv()
            if sem == 2 and onward:
                step_copy(buf, n, own_k + nk - 2, 4, own_k + 1).start()
            if sem == 3 and onward:
                step_copy(buf, n, own_k + nk + 2, 5, own_k + nk - 1).start()
                step_copy(buf, n, own_k + nk - 2 * side, 6, own_k + nk + 2 * side).start()
            if sem < 2 or not onward:
                near_copies(buf, n, own_k + nk + o)
        if onward:
            near_copies(buf, n, own_k + nk - 2)
            near_copies(buf, n, own_k + nk + 2)

    def gather_onward(buf, n):
        for sem, o in onward:
            step_copy(buf, n, own_k + nk + o, sem, own_k).wait_recv()
            near_copies(buf, n, own_k + nk + o)

    def near_all(buf, n, i, sem, r, k0, count):
        at = buf.at[r, pl.ds(k0, count)]
        return pltpu.make_async_remote_copy(
            src_ref=at,
            dst_ref=at,
            send_sem=l2_send.at[n, i],
            recv_sem=l2_recv.at[n, sem],
            device_id=chip(z + 1),
            device_id_type=MESH,
        )

    def gather_wait(buf, n):
        near_all(buf, n, 0, 0, (res + STRIDE - 1) % STRIDE, 0, nk).wait_recv()
        near_all(buf, n, 1, 1, (res + 1) % STRIDE, 0, nk).wait_recv()
        near_all(buf, n, 2, 2, (res + 2) % STRIDE, 0, hk).wait_recv()
        near_all(buf, n, 2, 3, (res + 2) % STRIDE, hk, hk).wait_recv()

    def gather_drain(buf, n):
        for sem, _ in direct + onward:
            step_copy(buf, n, own_k, sem, own_k).wait_send()
        for i in range(3):
            near_all(buf, n, i, i, res, 0, nk).wait_send()

    def scatter(src_of, dst, send_sem, recv_sem):
        @pl.loop(0, nz - 1)
        def _(j):
            zt = far_first(j)
            pltpu.make_async_remote_copy(
                src_ref=src_of(zt),
                dst_ref=dst,
                send_sem=send_sem,
                recv_sem=recv_sem,
                device_id=chip(zt),
                device_id_type=MESH,
            ).start()

    def scatter_all(block, send_sem, recv_sem):
        return pltpu.make_async_remote_copy(
            src_ref=block.at[pl.ds(0, nz - 1)],
            dst_ref=block.at[pl.ds(0, nz - 1)],
            send_sem=send_sem,
            recv_sem=recv_sem,
            device_id=chip(z),
            device_id_type=MESH,
        )

    tokb = tok8[...].astype(BF16)

    def dot_t(a, b):
        return lax.dot_general(a, b, (((1,), (1,)), ((), ())), preferred_element_type=F32)

    squash = jnp.tanh(dot_t(tokb, dl1[...])).astype(BF16)
    lowl = dot_t(tokb, cl1[...]).astype(BF16)
    opened = jax.nn.sigmoid(dot(tokb, gl1[...])).astype(BF16)

    for j in range(nz // 2):
        cols = slice(128 * j, 128 * j + 128)

        def two_heads(ref, tile, j=j):
            ref[2 * j] = tile
            ref[2 * j + 1] = pltpu.roll(tile, HEAD, 1)

        pre = doff[:, cols] + dot(squash, dl2[:, cols])
        two_heads(dh, jnp.exp(-(jnp.exp(jnp.full((8, 128), -0.5, F32)) * jax.nn.sigmoid(pre))))
        two_heads(ah, jax.nn.sigmoid(coff[:, cols] + dot(lowl, cl2[:, cols])))
        two_heads(gh, dot(opened, gl2[:, cols]))

    pl.semaphore_wait(bar, nz - 1 + 1 + share - 1)

    gather_start(xt, 0)
    for i in range(nm):
        m = gq * nm + i
        scatter(
            lambda zt, i=i: wsend.at[i, zt],
            wb.at[m, c, z],
            w_send.at[i],
            w_recv.at[i, z // quarter],
        )

    gather_direct(xt, 0)

    def piece(m, core, n, to, send_sem, recv_sem):
        at = wb.at[m, core, pl.ds(n * quarter, quarter)]
        return pltpu.make_async_remote_copy(
            src_ref=at,
            dst_ref=at,
            send_sem=send_sem,
            recv_sem=recv_sem,
            device_id=to,
            device_id_type=MESH,
        )

    def sib_piece(m, core, n):
        return piece(m, core, n, sib, s_send.at[m, n], s_recv.at[m, n])

    def group_piece(m, n, g):
        to = {"grp": gbase + (gq + g) % share} if share > 1 else sib
        return piece(m, c, n, to, q_send.at[g, m % nm, n], q_recv.at[m, n])

    def hand_out(i, m):
        for d in range(4):
            n = (z // quarter + d) % 4
            count = quarter - 1 if d == 0 else quarter
            at = wb.at[m, c, pl.ds(0, count)]
            pltpu.make_async_remote_copy(
                src_ref=at,
                dst_ref=at,
                send_sem=w_send.at[i],
                recv_sem=w_recv.at[i, n],
                device_id=chip(z),
                device_id_type=MESH,
            ).wait_recv()
            for g in range(1, share):
                group_piece(m, n, g).start()
            sib_piece(m, c, n).start()

    def pass_on(m):
        for n in range(4):
            group_piece(m, n, 0).wait_recv()
            sib_piece(m, c, n).start()

    def mine(m):
        return gq == m // nm

    for m in range(3):
        pl.when(mine(m))(functools.partial(hand_out, m % nm, m))
    if share > 1:
        for m in range(3):
            pl.when(jnp.logical_not(mine(m)))(functools.partial(pass_on, m))
    gather_onward(xt, 0)

    def widen(m, at):
        keep = left16.astype(F32).astype(BF16)
        drop = (1.0 - left16.astype(F32)).astype(BF16)
        for hk in range(2):

            @pl.loop(0, nz // 2)
            def _(zz, hk=hk):
                for core in range(2):
                    tile = wb[m, core, hk * (nz // 2) + zz]
                    base = pl.multiple_of(zz * 64 + core * 32, 32)
                    cols = slice(at + hk * 128, at + hk * 128 + 128)
                    em[pl.ds(base, 16), cols] = tile * keep
                    em[pl.ds(pl.multiple_of(base + 16, 16), 16), cols] = tile * drop

    def rows_of(value):
        return value.astype(F32).reshape(8 * nz, half).astype(BF16)

    top3 = row_ids((nz, 8, 128)) < ROWS
    left3 = lane_ids((nz, 8, 128)) < HEAD
    topw = (row_ids((8 * nz, 128)) % 8) < ROWS

    def fold(r):
        a = jnp.where(topw, r[:, 0:128], r[:, 128:256])
        a = (a + pltpu.roll(a, HEAD, 1)).reshape(nz, 8, 128)
        return a + pltpu.roll(a, ROWS, 1)

    for m in range(3):
        for n in range(4):
            sib_piece(m, 1 - c, n).wait_recv()
        widen(m, m * 256)

    gather_wait(xt, 0)
    xv = rows_of(xt[...])
    cr = fold(dot(xv, em[:, 0:256]))
    ck = fold(dot(xv, em[:, 256:512]))
    cv = fold(dot(xv, em[:, 512:768]))
    ysend[...] = jnp.where(top3, jnp.where(left3, cr, ck), cv).astype(BF16)
    scatter(lambda zt: ysend.at[slot_of(zt)], yrecv.at[z], a_send.at[0], a_recv.at[0])
    yrecv[z] = ysend[my_slot]
    scatter(lambda zt: csend, cb.at[c, my_slot], a_send.at[2], a_recv.at[2])
    topk = row_ids((nk, 8, 128)) < ROWS
    leftk = lane_ids((nk, 8, 128)) < HEAD
    for s in range(2):
        for m in range(half // 128):
            one = xt[2 * s, :, :, 128 * m : 128 * m + 128].astype(F32)
            two = xt[2 * s + 1, :, :, 128 * m : 128 * m + 128].astype(F32)
            x2[s, :, :, 128 * m : 128 * m + 128] = jnp.where(topk, one, pltpu.roll(two, ROWS, 1))
            x2[s, :, :, half + 128 * m : half + 128 * m + 128] = jnp.where(
                topk, pltpu.roll(one, ROWS, 1), two
            )
    pl.when(mine(3))(functools.partial(hand_out, 3 % nm, 3))
    st_load.wait()
    scatter_all(yrecv, a_send.at[0], a_recv.at[0]).wait_recv()

    eye = (
        lax.broadcasted_iota(jnp.int32, (HEAD, HEAD), 0)
        == lax.broadcasted_iota(jnp.int32, (HEAD, HEAD), 1)
    ).astype(F32)

    def pick(ref, j):
        tile = jnp.broadcast_to(ref[:, 128 * j : 128 * j + 128], (8, 128))
        return tile, pltpu.roll(tile, HEAD, 1)

    blends = []
    for j in range(nz // 2):
        blends += pick(blend, j)
    for h in range(nz):
        bh[h] = blends[h]

    @pl.loop(0, nz // 2)
    def _(pair):
        for h in (2 * pair, 2 * pair + 1):
            y = yrecv[h].astype(F32)
            turned = pltpu.roll(y, ROWS, 0)
            rk = jnp.where(top, y, turned)
            v = jnp.where(top, turned, y)
            r = jnp.where(left, rk, 0.0)
            k = jnp.where(left, pltpu.roll(rk, HEAD, 1), 0.0)
            a = ah[h]
            unit = k * lax.rsqrt(jnp.sum(k * k, -1, keepdims=True) + 1e-06)
            written = k * (1.0 + (a - 1.0) * bh[h])
            ua = unit * a
            scale = sscale[pl.ds(h, 1), :]
            own = jnp.sum((r * written)[:, 0:HEAD] * scale, -1, keepdims=True)
            d = dh[h]
            sv[h] = own * v
            for t in range(ROWS):
                one = slice(t, t + 1)
                s = st[t, h]
                removed = jnp.sum(s * unit[one, 0:HEAD], -1, keepdims=True)
                vcol = jnp.sum(eye * v[one, 0:HEAD], -1, keepdims=True)
                n = s * d[one, 0:HEAD] - removed * ua[one, 0:HEAD] + vcol * written[one, 0:HEAD]
                sn[t, h] = n
                read = jnp.sum(n * r[one, 0:HEAD], -1, keepdims=True)
                row = jnp.sum(eye * read, 0, keepdims=True)
                ro[h, t : t + 1, 0:HEAD] = row
                ro[h, ROWS + t : ROWS + t + 1, 0:HEAD] = row

    st_store = pltpu.make_async_copy(sn, next_hbm, ld_sem.at[4])
    st_store.start()

    def mixer_head(h, gain, bias):
        x = jnp.where(left, ro[h], 0.0)
        mean = jnp.sum(x, -1, keepdims=True) * (1.0 / HEAD)
        dev = jnp.where(left, x - mean, 0.0)
        var = jnp.sum(dev * dev, -1, keepdims=True) * (1.0 / HEAD)
        normed = dev * lax.rsqrt(var + 0.00064) * gain + bias
        return (normed + sv[h]) * gh[h]

    def mixer_pair(j):
        g0, g1 = pick(hgain, j)
        b0, b1 = pick(hbias, j)
        one, two = mixer_head(2 * j, g0, b0), mixer_head(2 * j + 1, g1, b1)
        return jnp.where(left, one, pltpu.roll(two, HEAD, 1))

    for j in range(nz // 4):
        tile = jnp.where(top, mixer_pair(j), mixer_pair(nz // 4 + j))
        xm[res, own_k, :, 128 * j : 128 * j + 128] = tile.astype(BF16)

    gather_start(xm, 1)
    if share > 1:
        pl.when(jnp.logical_not(mine(3)))(functools.partial(pass_on, 3))
    gather_direct(xm, 1)
    gather_onward(xm, 1)
    for n in range(4):
        sib_piece(3, 1 - c, n).wait_recv()
    widen(3, 768)
    gather_wait(xm, 1)
    co = fold(dot(rows_of(xm[...]), em[:, 768:1024]))
    xg[res, own_k] = jnp.where(
        leftk,
        jnp.where(topk, co[0:nk], co[nk : 2 * nk]),
        jnp.where(topk, co[2 * nk : 3 * nk], co[3 * nk :]),
    ).astype(BF16)
    gather_start(xg, 2)

    scatter_all(cb.at[c], a_send.at[2], a_recv.at[2]).wait_recv()

    def to_sib(src, dst, n):
        return pltpu.make_async_remote_copy(
            src_ref=src,
            dst_ref=dst,
            send_sem=x_send.at[n],
            recv_sem=x_recv.at[n],
            device_id=sib,
            device_id_type=MESH,
        )

    to_sib(cb.at[c], cb.at[c], 0).start()

    gather_direct(xg, 2)
    gather_onward(xg, 2)
    gather_wait(xg, 2)
    for j in range(nz // 2):
        cols = slice(128 * j, 128 * j + 128)
        one = xg[2 * j % STRIDE, 2 * j // STRIDE].astype(F32)
        two = xg[(2 * j + 1) % STRIDE, (2 * j + 1) // STRIDE].astype(F32)
        x2[0, :, :, cols] += jnp.where(leftk, one, pltpu.roll(two, HEAD, 2))
        x2[1, :, :, cols] += jnp.where(leftk, pltpu.roll(one, HEAD, 2), two)

    some = max(1, nk // 2)
    for s in range(2):
        for k in range(0, nk, some):
            x = x2[s, k : k + some]
            dev = x - jnp.mean(x, -1, keepdims=True)
            var = jnp.mean(dev * dev, -1, keepdims=True)
            y = dev * lax.rsqrt(var + 1e-05) * mgain[...] + mbias[...]
            x2[s, k : k + some] = y
            base = 8 * (s * nk + k)
            hid[c, base : base + 8 * some, :] = y.reshape(8 * some, dim).astype(BF16)

    to_sib(hid.at[c], hid.at[c], 1).start()

    topp = row_ids((8, half)) < ROWS

    def packed(ref):
        return jnp.where(topp, ref[:, 0:half], ref[:, half:dim])

    def row_total(x):
        s = jnp.broadcast_to(jnp.sum(x, -1, keepdims=True), (8, 128))
        s = s + pltpu.roll(s, ROWS, 0)
        return s[:, 0:1] * (1.0 / dim)

    def layer_norm(x, gain, bias):
        dev = x - row_total(x)
        var = row_total(dev * dev)
        return dev * lax.rsqrt(var + 1e-05) * packed(gain) + packed(bias)

    two_rows = x2[res // 2, own_k].astype(BF16).astype(F32)
    mine = row_ids((8, dim)) // ROWS == res % 2
    doubled = jnp.where(mine, two_rows, pltpu.roll(two_rows, ROWS, 0))
    hidp[...] = jnp.where(topp, doubled[:, 0:half], doubled[:, half:dim])

    eg_load.wait()
    eu_load.wait()
    ed_load.wait()
    to_sib(cb.at[1 - c], cb.at[1 - c], 0).wait_recv()

    def expert(core):
        xv = hid[core]
        lane3 = lane_ids((nz, 8, 128))
        hit = (lane3 == ep) | (lane3 == ep + HEAD)
        coef = jnp.sum(jnp.where(hit, cb[core].astype(F32), 0.0), -1, keepdims=True)
        top1 = row_ids((nk, 8, 1)) < ROWS
        coef = jnp.concatenate(
            [
                jnp.where(top1, coef[0:nk], coef[nk : 2 * nk]),
                jnp.where(top1, coef[2 * nk : 3 * nk], coef[3 * nk :]),
            ],
            0,
        ).reshape(ROWS * nz, 1)
        gate = dot(xv, eg[...])
        up = dot(xv, eu[...])
        inner = (gate * jax.nn.sigmoid(gate) * up).astype(BF16)
        return inner, coef

    def down(inner, coef, z, j, width):
        cols = slice(j * width, (j + 1) * width)
        low = dot(inner, ed[:, cols]) * coef
        high = dot(inner, ed[:, half + j * width : half + (j + 1) * width]) * coef
        low, high = low.reshape(2, nk, 8, width), high.reshape(2, nk, 8, width)
        keep = row_ids((nk, 8, width)) < ROWS
        for s in range(2):
            one = jnp.where(keep, low[s], pltpu.roll(high[s], ROWS, 1))
            two = jnp.where(keep, pltpu.roll(low[s], ROWS, 1), high[s])
            z[2 * s, :, :, cols] = one.astype(BF16)
            z[2 * s + 1, :, :, cols] = two.astype(BF16)

    width = min(256, half)
    inner, coef = expert(c)
    for j in range(half // width):
        down(inner, coef, zown, j, width)
    to_sib(hid.at[1 - c], hid.at[1 - c], 1).wait_recv()
    inner, coef = expert(1 - c)
    for j in range(half // width):
        down(inner, coef, zoth, j, width)
    to_sib(zoth, zsib, 2).start()
    to_sib(zoth, zsib, 2).wait_recv()
    tsum[...] = (zown[...].astype(F32) + zsib[...].astype(F32)).astype(BF16)

    def near_sum(slot):
        k = slot % nk
        part = k // hk
        up, down_, far = (res + 1) % STRIDE, (res + STRIDE - 1) % STRIDE, (res + 2) % STRIDE
        return [
            pltpu.make_async_remote_copy(
                src_ref=tsum.at[r, k],
                dst_ref=r1.at[i, k],
                send_sem=f1_send.at[i],
                recv_sem=f1_recv.at[i, k],
                device_id=chip(to),
                device_id_type=MESH,
            )
            for i, (to, r) in enumerate(
                ((z + 1, up), (z + nz - 1, down_), (z + nz + 2 - 4 * part, far))
            )
        ]

    def step_sum(kt, src, sem):
        return pltpu.make_async_remote_copy(
            src_ref=u2.at[src],
            dst_ref=r2.at[sem],
            send_sem=f2_send.at[sem],
            recv_sem=f2_recv.at[sem],
            device_id=chip((kt % nk) * STRIDE + res),
            device_id_type=MESH,
        )

    def near_total(slot):
        k = slot % nk
        for cp in near_sum(k):
            cp.wait_recv()
        return (
            tsum[res, k].astype(F32)
            + r1[0, k].astype(F32)
            + r1[1, k].astype(F32)
            + r1[2, k].astype(F32)
        )

    def arrived(sem):
        step_sum(own_k, 0, sem).wait_recv()
        return r2[sem].astype(F32)

    if nk == 8:
        order = [nk + 4, nk - 3, nk + 3, nk - 2 * side, nk + 2 * side, nk - 1, nk + 1, nk]
    else:
        order = [nk // 2] + ([1, nk - 1] if nk == 4 else []) + [nk]
    for o in order:
        for cp in near_sum(own_k + o):
            cp.start()
    if nk == 8:
        u2[0] = near_total(own_k + 4).astype(BF16)
        step_sum(own_k + nk + 2 * side * -1, 0, 0).start()
        u2[1] = near_total(own_k + nk - 3 * side).astype(BF16)
        step_sum(own_k + nk - side, 1, 1).start()
        u2[2] = near_total(own_k + nk + 3 * side).astype(BF16)
        step_sum(own_k + nk + side, 2, 2).start()
        u2[3] = near_total(own_k + nk - side).astype(BF16)
        step_sum(own_k + nk - side, 3, 3).start()
        u2[4] = near_total(own_k + nk + side).astype(BF16)
        step_sum(own_k + nk + side, 4, 4).start()
        part_b = near_total(own_k + nk + 2 * side)
        part_a = near_total(own_k + nk - 2 * side)
        u2[6] = (part_b + arrived(1)).astype(BF16)
        step_sum(own_k + nk + 2 * side, 6, 6).start()
        u2[5] = (part_a + arrived(2) + arrived(0)).astype(BF16)
        step_sum(own_k + nk - 2 * side, 5, 5).start()
        total = near_total(own_k)
        used = range(7)
    else:
        for i, o in enumerate(order[:-1]):
            u2[i] = near_total(own_k + o).astype(BF16)
            step_sum(own_k + o, i, i).start()
        total = near_total(own_k)
        used = range(len(order) - 1)
    total = total + hidp[...]
    for sem in used:
        if nk != 8 or sem >= 3:
            total = total + arrived(sem)
    y = layer_norm(total, egain, ebias)
    out_ref[:, 0:half] = y[0:ROWS, :].astype(BF16)
    out_ref[:, half:dim] = y[ROWS : 2 * ROWS, :].astype(BF16)

    gather_drain(xt, 0)
    gather_drain(xm, 1)
    gather_drain(xg, 2)
    for i in range(nm):
        scatter_all(wb.at[gq * nm + i, c], w_send.at[i], w_recv.at[i, 0]).wait_send()
        for g in range(1, share):
            for n in range(4):
                group_piece(gq * nm + i, n, g).wait_send()
    for m in range(4):
        for n in range(4):
            sib_piece(m, c, n).wait_send()
    scatter_all(yrecv, a_send.at[0], a_recv.at[0]).wait_send()
    scatter_all(cb.at[c], a_send.at[2], a_recv.at[2]).wait_send()
    to_sib(cb.at[c], cb.at[c], 0).wait_send()
    to_sib(hid.at[c], hid.at[c], 1).wait_send()
    to_sib(zoth, zsib, 2).wait_send()
    for i in range(3):
        pltpu.make_async_remote_copy(
            src_ref=tsum.at[res],
            dst_ref=r1.at[i],
            send_sem=f1_send.at[i],
            recv_sem=f1_recv.at[i, 0],
            device_id=chip(z + 1),
            device_id_type=MESH,
        ).wait_send()
    for sem in used:
        step_sum(own_k, sem, sem).wait_send()
    st_store.wait()


def hand_back(small, state, small_out, state_out, small_buf, buf, in_sem, out_sem):
    pieces = [(small, small_buf, small_out)]
    half = state.shape[1] // 2
    for i in range(state.shape[0]):
        for part in (pl.ds(0, half), pl.ds(half, half)):
            pieces.append((state.at[i, part], buf.at[i, part], state_out.at[i, part]))
    reads = [pltpu.make_async_copy(a, b, in_sem.at[i]) for i, (a, b, _) in enumerate(pieces)]
    writes = [pltpu.make_async_copy(b, o, out_sem.at[i]) for i, (_, b, o) in enumerate(pieces)]
    for cp in reads:
        cp.start()
    for read, write in zip(reads, writes):
        read.wait()
        write.start()
    for cp in writes:
        cp.wait()


def step(nz, share, *args):
    tokens, state = args[0], args[1]
    dim = tokens.shape[1]
    half = dim // 2
    nk = nz // STRIDE
    nm = 4 // share
    ff = args[24].shape[2]
    args = list(args)
    args[5], args[8] = args[5].T, args[8].T
    for i in (7, 10, 13, 15, 16, 18, 19, 20, 21):
        args[i] = args[i].reshape(1, dim)
    small = [5, 6, 7, 8, 9, 10, 11, 12, 13, 14, 15, 16, 18, 19, 20, 21, 22, 23]
    operands = [args[i] for i in [0, 1, 2, 3, 4, 17] + small + [24, 25, 26]]
    vmem = pl.BlockSpec(memory_space=pltpu.VMEM)
    hbm = pl.BlockSpec(memory_space=pl.ANY)
    dma = pltpu.SemaphoreType.DMA
    heads = (nz, 8, 128)
    rows = (STRIDE, nk, 8, half)
    scratch = [
        pltpu.VMEM(tokens.shape, BF16),
        *[pltpu.VMEM(args[i].shape, args[i].dtype) for i in small],
        pltpu.VMEM(state.shape, F32),
        pltpu.VMEM(state.shape, F32),
        pltpu.VMEM((nm, 32, dim), BF16),
        pltpu.VMEM((nm, nz, 16, 128), BF16),
        pltpu.VMEM((4, 2, nz, 16, 128), BF16),
        pltpu.VMEM((half, 1024), BF16),
        pltpu.VMEM(rows, BF16),
        pltpu.VMEM(rows, BF16),
        pltpu.VMEM((STRIDE, nk, nk, 8, 128), BF16),
        pltpu.VMEM((2, nk, 8, dim), F32),
        pltpu.VMEM((2, ROWS * nz, dim), BF16),
        pltpu.VMEM(heads, BF16),
        pltpu.VMEM(heads, BF16),
        pltpu.VMEM((2,) + heads, BF16),
        pltpu.VMEM((8, 128), BF16),
        pltpu.VMEM((8, dim), F32),
        pltpu.VMEM((8, half), F32),
        pltpu.VMEM((8, half), F32),
        pltpu.VMEM(heads, F32),
        pltpu.VMEM(heads, F32),
        pltpu.VMEM(heads, F32),
        pltpu.VMEM(heads, F32),
        pltpu.VMEM(heads, F32),
        pltpu.VMEM(heads, F32),
        pltpu.VMEM((dim, ff), BF16),
        pltpu.VMEM((dim, ff), BF16),
        pltpu.VMEM((ff, dim), BF16),
        pltpu.VMEM(rows, BF16),
        pltpu.VMEM(rows, BF16),
        pltpu.VMEM(rows, BF16),
        pltpu.VMEM(rows, BF16),
        pltpu.VMEM((3, nk, 8, half), BF16),
        pltpu.VMEM((nk, 8, half), BF16),
        pltpu.VMEM((nk, 8, half), BF16),
        dma((9,)),
        dma((nm,)),
        dma((nm, 4)),
        dma((share, nm, 4)),
        dma((4, 4)),
        dma((4, 4)),
        dma((4, 4)),
        dma((3, 7)),
        dma((3, 7)),
        dma((3, 3)),
        dma((3, 4)),
        dma((3,)),
        dma((3,)),
        dma((3,)),
        dma((3,)),
        dma((3,)),
        dma((3, nk)),
        dma((7,)),
        dma((7,)),
        dma((SMALL,)),
    ]
    result, state_new = pl.pallas_call(
        functools.partial(kernel, nz, share),
        out_shape=(
            jax.ShapeDtypeStruct(tokens.shape, BF16),
            jax.ShapeDtypeStruct(state.shape, F32),
        ),
        in_specs=[hbm] * len(operands),
        out_specs=(vmem, hbm),
        scratch_shapes=scratch,
        compiler_params=pltpu.CompilerParams(
            collective_id=0, has_side_effects=True, vmem_limit_bytes=56 * 1024 * 1024
        ),
    )(*operands)
    return pl.pallas_call(
        hand_back,
        out_shape=(
            jax.ShapeDtypeStruct(tokens.shape, BF16),
            jax.ShapeDtypeStruct(state.shape, F32),
        ),
        in_specs=[hbm, hbm],
        out_specs=(hbm, hbm),
        scratch_shapes=[
            pltpu.VMEM(tokens.shape, BF16),
            pltpu.VMEM(state.shape, F32),
            dma((1 + 2 * state.shape[0],)),
            dma((1 + 2 * state.shape[0],)),
        ],
        compiler_params=pltpu.CompilerParams(vmem_limit_bytes=62 * 1024 * 1024),
    )(result, state_new)


def solution(mesh):
    nz = mesh.shape["ep"] // 2
    groups = mesh.shape["grp"]
    share = 4 if groups % 4 == 0 else 2 if groups % 2 == 0 else 1
    owned, split, copied = P(("grp", "ep"), None), P("ep", None), P()
    in_specs = (
        owned,
        P(("grp", "ep"), None, None, None),
        split,
        split,
        split,
        *([copied] * 12),
        split,
        *([copied] * 4),
        owned,
        owned,
        P("ep", None, None),
        P("ep", None, None),
        P("ep", None, None),
    )
    out_specs = (owned, P(("grp", "ep"), None, None, None))
    return jax.shard_map(
        functools.partial(step, nz, share),
        mesh=mesh,
        in_specs=in_specs,
        out_specs=out_specs,
        check_vma=False,
    )
```
